128 devices in a mesh: dp: 4 (over x), kv: 16 (over z, y), tp: 2 (over core).
Axes of the slice: x: 4, y: 4, z: 4, core: 2. Of those that a mesh axis runs over, the one named last changes fastest.
Arguments:
- tokens: bfloat16 [1024, 4096], P('dp', ('kv', 'tp')), may hold values from -53 to 53
- carried_state: float32 [1024, 16, 128, 128], P(('dp', 'kv', 'tp')), may hold values from -9 to 9
- first_gain: float32 [4096], replicated, may hold values from 0.1 to 1.9
- first_gate: bfloat16 [4096, 11264], P(None, ('kv', 'tp')), may hold values from -0.09375 to 0.09375
- first_up: bfloat16 [4096, 11264], P(None, ('kv', 'tp')), may hold values from -0.09375 to 0.09375
- first_down: bfloat16 [11264, 4096], P(('kv', 'tp')), may hold values from -0.109375 to 0.109375
- mix_gain: float32 [4096], replicated, may hold values from 0.1 to 1.9
- query_weight: bfloat16 [4096, 2048], P(('kv', 'tp')), may hold values from -0.09375 to 0.09375
- forget_weight: bfloat16 [4096, 2048], P(('kv', 'tp')), may hold values from -0.09375 to 0.09375
- input_weight: bfloat16 [4096, 2048], P(('kv', 'tp')), may hold values from -0.09375 to 0.09375
- outgate_weight: bfloat16 [4096, 2048], P(('kv', 'tp')), may hold values from -0.09375 to 0.09375
- forget_floor: float32 [2048], replicated, may hold values from 0.05 to 0.9
- head_gain: float32 [128], replicated, may hold values from 0.1 to 1.9
- output_weight: bfloat16 [2048, 4096], P(None, ('kv', 'tp')), may hold values from -0.125 to 0.125
- second_gain: float32 [4096], replicated, may hold values from 0.1 to 1.9
- second_gate: bfloat16 [4096, 11264], P(None, ('kv', 'tp')), may hold values from -0.09375 to 0.09375
- second_up: bfloat16 [4096, 11264], P(None, ('kv', 'tp')), may hold values from -0.09375 to 0.09375
- second_down: bfloat16 [11264, 4096], P(('kv', 'tp')), may hold values from -0.109375 to 0.109375
Outputs:
- layer_out: bfloat16 [1024, 4096], P('dp', ('kv', 'tp'))
- next_state: float32 [1024, 16, 128, 128], P(('dp', 'kv', 'tp'))
The draws below stay inside these ranges and needn't reach their ends.
All inputs are finite; a program needn't handle non-finite values.
Results may differ from the reference program's by a relative error of at most 0.018.
Values may be sent and summed in bfloat16 or wider, within the bound.
A program may use at most 128 MiB of HBM per device.

```python
import jax
import jax.numpy as jnp
from jax import lax

D = 4096
FF = 11264
HEADS = 16
KEY = 128
VAL = 128
SEQS = 1024
KW = 2048
VW = 2048


def draw_tokens(key, part):
    keys = jax.random.split(jax.random.fold_in(key, 11), 3)
    row_scale = jnp.exp(jax.random.uniform(keys[0], (SEQS, 1), jnp.float32, jnp.log(0.3), jnp.log(3.0)))
    col_trend = jnp.exp(jnp.linspace(jnp.log(0.4), jnp.log(2.5), D)).astype(jnp.float32).reshape(1, D)
    rough = jax.random.uniform(keys[1], (1, D), jnp.float32, 0.6, 1.4)
    base = jnp.clip(jax.random.normal(keys[2], (SEQS, D), jnp.float32), -5.0, 5.0)
    return (base * rough * col_trend * row_scale).astype(jnp.bfloat16)


def strengthened(result, rng, source, target, shards_of, factor):
    owner, partner = [(jnp.arange(result.shape[axis_at]) // (result.shape[axis_at] // shards_of)).reshape([-1 if axis == axis_at else 1 for axis in range(result.ndim)]) for axis_at in (source, target)]
    chosen = jax.random.permutation(rng, shards_of)[partner]
    strong = (owner == chosen) | (owner == (partner + shards_of // 2) % shards_of)
    return jnp.where(strong, factor * result, result)


def block_scale(stream_key, shape, cuts, least, top_value):
    loudness = 1.0
    for dim, parts in cuts:
        heights = jax.random.uniform(jax.random.fold_in(jax.random.fold_in(stream_key, 6), dim), (parts,), jnp.float32, least / len(cuts), top_value / len(cuts))
        loudness = loudness * jnp.repeat(jnp.exp(heights), shape[dim] // parts).reshape((-1,) + (1,) * (len(shape) - 1 - dim))
    return loudness


def scatter_about(rng, shape, width, limit, cuts=(), dtype=jnp.bfloat16):
    values = width * jax.random.normal(rng, shape, jnp.float32)
    if cuts:
        values = values * block_scale(rng, shape, cuts, -0.22, 0.18)
    return jnp.clip(values, -limit, limit).astype(dtype)


def noise_with(rng, extent, spread, most, cuts, heavy, kind=jnp.bfloat16):
    values = spread * jax.random.normal(rng, extent, jnp.float32)
    if cuts:
        values = values * block_scale(rng, extent, cuts, -0.22, 0.18)
    return jnp.clip(strengthened(values, jax.random.fold_in(rng, 3), *heavy), -most, most).astype(kind)


def setup_inputs(seed: int = 0) -> dict:
    arg_keys = jax.random.split(jax.random.key(seed), 19)
    tokens = draw_tokens(jax.random.fold_in(arg_keys[18], 71), 0)
    carried_state = scatter_about(arg_keys[1], (SEQS, HEADS, KEY, VAL), 1.5, 9.0, ((0, 128),), jnp.float32)
    first_gain = jnp.clip(1.0 + 0.18 * jax.random.normal(arg_keys[2], (D,), jnp.float32), 0.1, 1.9)
    first_gate = scatter_about(arg_keys[3], (D, FF), D ** -0.5, 0.09375, ((1, 32),))
    first_up = scatter_about(arg_keys[4], (D, FF), D ** -0.5, 0.09375, ((1, 32),))
    first_down = noise_with(arg_keys[5], (FF, D), FF ** -0.5, 0.109375, ((0, 32),), (0, 1, 32, 2.75))
    mix_gain = jnp.clip(1.0 + 0.18 * jax.random.normal(arg_keys[6], (D,), jnp.float32), 0.1, 1.9)
    query_weight = scatter_about(arg_keys[7], (D, KW), D ** -0.5, 0.09375, ((0, 32),))
    forget_weight = scatter_about(arg_keys[8], (D, KW), D ** -0.5, 0.09375, ((0, 32),))
    input_weight = scatter_about(arg_keys[9], (D, VW), D ** -0.5, 0.09375, ((0, 32),))
    outgate_weight = scatter_about(arg_keys[10], (D, VW), D ** -0.5, 0.09375, ((0, 32),))
    forget_floor = jnp.clip(jax.random.uniform(arg_keys[11], (KW,), jnp.float32, 0.05, 0.9), 0.05, 0.9)
    head_gain = jnp.clip(1.0 + 0.18 * jax.random.normal(arg_keys[12], (VAL,), jnp.float32), 0.1, 1.9)
    output_weight = scatter_about(arg_keys[13], (VW, D), VW ** -0.5, 0.125, ((1, 32),))
    second_gain = jnp.clip(1.0 + 0.18 * jax.random.normal(arg_keys[14], (D,), jnp.float32), 0.1, 1.9)
    second_gate = scatter_about(arg_keys[15], (D, FF), D ** -0.5, 0.09375, ((1, 32),))
    second_up = scatter_about(arg_keys[16], (D, FF), D ** -0.5, 0.09375, ((1, 32),))
    second_down = noise_with(arg_keys[17], (FF, D), FF ** -0.5, 0.109375, ((0, 32),), (0, 1, 32, 2.75))
    return {"tokens": tokens, "carried_state": carried_state, "first_gain": first_gain, "first_gate": first_gate, "first_up": first_up, "first_down": first_down, "mix_gain": mix_gain, "query_weight": query_weight, "forget_weight": forget_weight, "input_weight": input_weight, "outgate_weight": outgate_weight, "forget_floor": forget_floor, "head_gain": head_gain, "output_weight": output_weight, "second_gain": second_gain, "second_gate": second_gate, "second_up": second_up, "second_down": second_down}


epsilon = 1e-06

def inverse_rms(entries):
    return lax.rsqrt(lax.optimization_barrier(jnp.mean(entries * entries, axis=-1, keepdims=True)) + epsilon)

def half_channel(inputs, gain_vec, gate_weight, up_weight, down_weight):
    widened = inputs.astype(jnp.float32)
    row_scale = inverse_rms(widened)
    scaled = (widened * gain_vec).astype(jnp.bfloat16)
    gate_acc = row_scale * jnp.dot(scaled, gate_weight, preferred_element_type=jnp.float32)
    up_acc = row_scale * jnp.dot(scaled, up_weight, preferred_element_type=jnp.float32)
    hidden = (jax.nn.silu(gate_acc) * up_acc).astype(jnp.bfloat16)
    return (widened + 0.5 * jnp.dot(hidden, down_weight, preferred_element_type=jnp.float32)).astype(jnp.bfloat16)

def reference(tokens, carried_state, first_gain, first_gate, first_up, first_down, mix_gain, query_weight, forget_weight, input_weight, outgate_weight, forget_floor, head_gain, output_weight, second_gain, second_gate, second_up, second_down):
    mixer_in = half_channel(tokens, first_gain, first_gate, first_up, first_down)
    widened = mixer_in.astype(jnp.float32)
    row_scale = inverse_rms(widened)
    scaled = (widened * mix_gain).astype(jnp.bfloat16)
    seq_count = tokens.shape[0]
    query_act = (row_scale * jnp.dot(scaled, query_weight, preferred_element_type=jnp.float32)).reshape(seq_count, HEADS, KEY)
    forget_pre = (row_scale * jnp.dot(scaled, forget_weight, preferred_element_type=jnp.float32)).reshape(seq_count, HEADS, KEY)
    input_val = (row_scale * jnp.dot(scaled, input_weight, preferred_element_type=jnp.float32)).reshape(seq_count, HEADS, VAL)
    gate_pre = (row_scale * jnp.dot(scaled, outgate_weight, preferred_element_type=jnp.float32)).reshape(seq_count, HEADS, VAL)
    floor_grid = forget_floor.reshape(HEADS, KEY)
    forget = floor_grid + (1.0 - floor_grid) * jax.nn.sigmoid(forget_pre)
    next_state = forget[..., None] * carried_state + (1.0 - forget)[..., None] * input_val[:, :, None, :]
    readout = lax.optimization_barrier(jnp.sum(next_state * jax.nn.silu(query_act)[..., None], axis=2))
    normed = readout * inverse_rms(readout) * head_gain
    mixer_out = (normed * jax.nn.silu(gate_pre)).reshape(seq_count, VW).astype(jnp.bfloat16)
    middle = (widened + jnp.dot(mixer_out, output_weight, preferred_element_type=jnp.float32)).astype(jnp.bfloat16)
    layer_out = half_channel(middle, second_gain, second_gate, second_up, second_down)
    return (layer_out, next_state)
```

```python
import jax
import jax.numpy as jnp
from jax import lax
from jax.experimental import pallas as pl
from jax.experimental.pallas import tpu as pltpu
from jax.sharding import Mesh
from jax.sharding import PartitionSpec as P

KV_TP = ("kv_0", "kv_1", "tp")
DP_KV_TP = ("dp", "kv_0", "kv_1", "tp")
MESH = pl.DeviceIdType.MESH
HBM = pltpu.MemorySpace.HBM
VMEM = pltpu.MemorySpace.VMEM
F32 = jnp.float32
BF16 = jnp.bfloat16

epsilon = 1e-06
RING = 4
LANES = 128
CHIPS = RING * RING
BLOCKS = 2 * CHIPS
NEAR = (("kv_0", 1), ("kv_0", 3), ("kv_1", 1), ("kv_1", 3), ("tp", 1))
HALF_AXES = (("kv_1", "kv_0"), ("kv_0", "kv_1"))
FAR_FIRST = (2, 1, 3, 0)
CHIP_ORDER = tuple((a, b) for a in FAR_FIRST for b in FAR_FIRST if a == 2 or b == 2) + tuple(
    (a, b) for a in FAR_FIRST for b in FAR_FIRST if a != 2 and b != 2
)
POSITION = {chip: place for place, chip in enumerate(CHIP_ORDER)}


def own_place():
    return (lax.axis_index("kv_0"), lax.axis_index("kv_1"), lax.axis_index("tp"))


def block_of(place, along_0, along_1, other_core):
    at_0, at_1, core = place
    return (
        lax.rem(at_0 + along_0, RING) * (2 * RING)
        + lax.rem(at_1 + along_1, RING) * 2
        + lax.rem(core + other_core, 2)
    )


class Wire:
    def __init__(self, place, send_sems, recv_sems):
        at_0, at_1, core = place
        self.place = {"kv_0": (at_0, RING), "kv_1": (at_1, RING), "tp": (core, 2)}
        self.send_sems, self.recv_sems = send_sems, recv_sems
        self.used = 0
        self.sent = []

    def near(self, axis, step):
        at, size = self.place[axis]
        return {axis: lax.rem(at + step, size)}

    def greet(self):
        barrier = pltpu.get_barrier_semaphore()
        for axis, step in NEAR:
            pl.semaphore_signal(
                barrier, inc=1, device_id=self.near(axis, step), device_id_type=MESH
            )
        pl.semaphore_wait(barrier, len(NEAR))

    def take(self, count):
        first = self.used
        self.used += count
        return first

    def make(self, source, target, axis, step, slot):
        return pltpu.make_async_remote_copy(
            src_ref=source,
            dst_ref=target,
            send_sem=self.send_sems.at[slot],
            recv_sem=self.recv_sems.at[slot],
            device_id=self.near(axis, step),
            device_id_type=MESH,
        )

    def send(self, source, target, axis, step):
        copy = self.make(source, target, axis, step, self.take(1))
        copy.start()
        self.sent.append(copy)
        return copy

    def finish(self):
        for copy in self.sent:
            copy.wait_send()
        self.sent = []


def halves_of(rows):
    tiles = rows // 16
    first = (tiles - tiles // 2) * 16
    second = rows - first
    return ((0, first, first // 32 * 16), (first, second, second // 32 * 16))


def gather(wire, held):
    halves = halves_of(held.shape[3])
    copies = {}

    def view(half, first, second, part, slot=0):
        start, rows, cut = halves[half]
        start, rows = ((start, rows), (start, cut), (start + cut, rows - cut))[part]
        along = (second, first) if HALF_AXES[half][0] == "kv_1" else (first, second)
        return held.at[along[0], along[1], slot, pl.ds(start, rows), :]

    def spread(half, stage, first):
        for step, there in ((1, 3), (3, 1)):
            if stage == 0:
                source, target = view(half, 0, 0, 0), view(half, there, 0, 0)
            else:
                source, target = view(half, first, 0, 0), view(half, first, there, 0)
            copies[half, stage, first, there] = wire.send(
                source, target, HALF_AXES[half][stage], step
            )

    def relay(half, stage, first, came):
        copies[half, stage, first, came].wait_recv()
        step, part = (1, 1) if came == 3 else (3, 2)
        if stage == 0:
            source, target = view(half, came, 0, part), view(half, 2, 0, part)
        else:
            source, target = view(half, first, came, part), view(half, first, 2, part)
        copies[half, stage, first, 2, part] = wire.send(
            source, target, HALF_AXES[half][stage], step
        )

    def across(half, first, second):
        copies[half, "across", first, second] = wire.send(
            view(half, first, second, 0), view(half, first, second, 0, 1), "tp", 1
        )

    def far(half, stage, first):
        for part in (1, 2):
            copies[half, stage, first, 2, part].wait_recv()

    both = (0, 1)
    for half in both:
        spread(half, 0, 0)
    for half in both:
        spread(half, 1, 0)
    for half in both:
        across(half, 0, 0)
    for came in (3, 1):
        for half in both:
            relay(half, 0, 0, came)
            spread(half, 1, came)
            across(half, came, 0)
    for came in (3, 1):
        for half in both:
            relay(half, 1, 0, came)
            across(half, 0, came)
    for half in both:
        far(half, 0, 0)
        spread(half, 1, 2)
        across(half, 2, 0)
    for first in (3, 1):
        for came in (3, 1):
            for half in both:
                relay(half, 1, first, came)
                across(half, first, came)
    for half in both:
        far(half, 1, 0)
        across(half, 0, 2)
    for came in (3, 1):
        for half in both:
            relay(half, 1, 2, came)
            across(half, 2, came)
    for first in (3, 1, 2):
        for half in both:
            far(half, 1, first)
            across(half, first, 2)
    for key, copy in copies.items():
        if key[1] == "across":
            copy.wait_recv()


def scatter_sum(wire, rows, term, buffers):
    halves = halves_of(rows)
    early_out, early_in, late_out, late_in, last_out, last_in = buffers
    copies = {}

    def chip(half, first, second):
        return (second, first) if HALF_AXES[half][0] == "kv_1" else (first, second)

    def parts(half):
        start, count, cut = halves[half]
        return ((0, cut, 1), (cut, count - cut, 3))

    for turn, second in enumerate(FAR_FIRST):
        for half in (0, 1):
            start, count, _ = halves[half]
            early_out[half, turn, pl.ds(0, count), :] = term(
                chip(half, 2, second), start, count
            ).astype(BF16)
            for at, length, step in parts(half):
                copies["early", half, turn, step] = wire.send(
                    early_out.at[half, turn, pl.ds(at, length), :],
                    early_in.at[half, turn, pl.ds(at, length), :],
                    HALF_AXES[half][0],
                    step,
                )
    for turn, second in enumerate(FAR_FIRST):
        for half in (0, 1):
            start, count, _ = halves[half]
            for way, (at, length, step) in enumerate(parts(half)):
                near = chip(half, step, second)
                copies["early", half, turn, step].wait_recv()
                rest_at, rest = (length, count - length) if at == 0 else (0, at)
                late_out[half, turn, way, pl.ds(at, length), :] = (
                    term(near, start + at, length)
                    + early_in[half, turn, pl.ds(at, length), :].astype(F32)
                ).astype(BF16)
                late_out[half, turn, way, pl.ds(rest_at, rest), :] = term(
                    near, start + rest_at, rest
                ).astype(BF16)
                copies["late", half, turn, step] = wire.send(
                    late_out.at[half, turn, way, pl.ds(0, count), :],
                    late_in.at[half, turn, way, pl.ds(0, count), :],
                    HALF_AXES[half][0],
                    step,
                )
    sums = [None, None]
    for turn, second in enumerate(FAR_FIRST):
        for half in (0, 1):
            start, count, cut = halves[half]
            value = term(chip(half, 0, second), start, count)
            for way, (_, _, step) in enumerate(parts(half)):
                copies["late", half, turn, step].wait_recv()
                value += late_in[half, turn, way, pl.ds(0, count), :].astype(F32)
            axis = HALF_AXES[half][1]
            if second == 2:
                last_out[half, 0, pl.ds(0, count), :] = value.astype(BF16)
                for at, length, step in parts(half):
                    copies["last", half, step] = wire.send(
                        last_out.at[half, 0, pl.ds(at, length), :],
                        last_in.at[half, 0, pl.ds(at, length), :],
                        axis,
                        step,
                    )
            elif second == 0:
                sums[half] = value
            else:
                way = 1 if second == 1 else 2
                at, length, step = parts(half)[way - 1]
                rest_at, rest = (length, count - length) if at == 0 else (0, at)
                copies["last", half, step].wait_recv()
                last_out[half, way, pl.ds(at, length), :] = (
                    value[at : at + length]
                    + last_in[half, 0, pl.ds(at, length), :].astype(F32)
                ).astype(BF16)
                last_out[half, way, pl.ds(rest_at, rest), :] = value[
                    rest_at : rest_at + rest
                ].astype(BF16)
                copies["final", half, step] = wire.send(
                    last_out.at[half, way, pl.ds(0, count), :],
                    last_in.at[half, way, pl.ds(0, count), :],
                    axis,
                    step,
                )
    for half in (0, 1):
        count = halves[half][1]
        for way, step in ((1, 1), (2, 3)):
            copies["final", half, step].wait_recv()
            sums[half] += last_in[half, way, pl.ds(0, count), :].astype(F32)
    return sums


def scatter_buffers(rows):
    half = halves_of(rows)[0][1]
    return [
        pltpu.VMEM((2, RING, half, LANES), BF16),
        pltpu.VMEM((2, RING, half, LANES), BF16),
        pltpu.VMEM((2, RING, 2, half, LANES), BF16),
        pltpu.VMEM((2, RING, 2, half, LANES), BF16),
        pltpu.VMEM((2, 3, half, LANES), BF16),
        pltpu.VMEM((2, 3, half, LANES), BF16),
    ]


def load_feed_forward(place, gate_hbm, up_hbm, down_hbm, wide, down, sems):
    hidden = gate_hbm.shape[0]
    half = wide.shape[0] // 2
    for block in range(BLOCKS):
        along_0, along_1, other = block // (2 * RING), block // 2 % RING, block % 2
        columns = pl.ds(
            pl.multiple_of(block_of(place, along_0, along_1, other) * LANES, LANES), LANES
        )
        here = pl.ds(block * LANES, LANES)
        pltpu.make_async_copy(
            gate_hbm.at[:, columns], wide.at[pl.ds(0, hidden), here], sems.at[0]
        ).start()
        pltpu.make_async_copy(
            up_hbm.at[:, columns], wide.at[pl.ds(half, hidden), here], sems.at[1]
        ).start()
    for at, (along_0, along_1) in enumerate(CHIP_ORDER):
        for other in (0, 1):
            columns = pl.ds(
                pl.multiple_of(block_of(place, along_0, along_1, other) * LANES, LANES), LANES
            )
            pltpu.make_async_copy(
                down_hbm.at[:, columns], down.at[at, :, pl.ds(other * LANES, LANES)], sems.at[2]
            ).start()
    return hidden, half


def feed_forward(
    place, wire, held, gain, gate_hbm, up_hbm, down_hbm, wide, down, sems, scratch, buffers
):
    scaled, squares, acc, own, pair_out, pair_in = scratch
    hidden, half = (gate_hbm.shape[0], wide.shape[0] // 2)
    rows = scaled.shape[0]
    width = scaled.shape[1]
    squares[...] = jnp.zeros_like(squares)

    def scale(block, carry):
        entry = held[block // (2 * RING), block // 2 % RING, block % 2].astype(F32)
        index = block_of(place, block // (2 * RING), block // 2 % RING, block % 2)
        squares[...] += entry * entry
        scaled[:, pl.ds(pl.multiple_of(block * LANES, LANES), LANES)] = (
            entry * gain[pl.ds(index, 1), :]
        ).astype(BF16)
        return carry

    lax.fori_loop(0, BLOCKS, scale, 0)
    pltpu.make_async_copy(gate_hbm, wide.at[pl.ds(0, hidden), :], sems.at[0]).wait()
    pltpu.make_async_copy(up_hbm, wide.at[pl.ds(half, hidden), :], sems.at[1]).wait()
    acc[...] = jnp.zeros_like(acc)
    depth = width // 4

    def product(step, carry):
        chunk = pl.ds(pl.multiple_of(step * depth, depth), depth)
        acc[...] += lax.dot_general(
            scaled[:, chunk],
            wide[:, chunk],
            (((1,), (1,)), ((), ())),
            preferred_element_type=F32,
        )
        return carry

    lax.fori_loop(0, 4, product, 0)
    row_scale = lax.rsqrt(jnp.sum(squares[...], axis=1, keepdims=True) / width + epsilon)
    gate = row_scale * acc[:, :hidden]
    up = row_scale * acc[:, half : half + hidden]
    units = (gate / (1.0 + jnp.exp(-gate)) * up).astype(BF16)
    pltpu.make_async_copy(down, down, sems.at[2]).wait()
    first = wire.take(CHIPS)

    def pair_copy(at):
        return wire.make(pair_out.at[at], pair_in.at[at], "tp", 1, first + at)

    def project(at, carry):
        result = jnp.dot(units, down[at], preferred_element_type=F32)
        own[at] = result[:, :LANES]
        pair_out[at] = result[:, LANES:].astype(BF16)
        pair_copy(at).start()
        return carry

    lax.fori_loop(0, CHIPS, project, 0)
    arrived = set()

    def term(chip, start, count):
        at = POSITION[chip]
        if at not in arrived:
            arrived.add(at)
            pair_copy(at).wait_recv()
        return own[at, pl.ds(start, count), :] + pair_in[at, pl.ds(start, count), :].astype(F32)

    sums = scatter_sum(wire, rows, term, buffers)
    wire.sent += [pair_copy(at) for at in range(CHIPS)]
    return sums


def feed_forward_scratch(rows, width, hidden):
    half = -(-hidden // LANES) * LANES
    return [
        pltpu.VMEM((RING, RING, 2, rows, LANES), BF16),
        pltpu.VMEM((2 * half, width), BF16),
        pltpu.VMEM((CHIPS, hidden, 2 * LANES), BF16),
        pltpu.SemaphoreType.DMA((8,)),
        pltpu.VMEM((rows, width), BF16),
        pltpu.VMEM((rows, LANES), F32),
        pltpu.VMEM((rows, 2 * half), F32),
        pltpu.VMEM((CHIPS, rows, LANES), F32),
        pltpu.VMEM((CHIPS, rows, LANES), BF16),
        pltpu.VMEM((CHIPS, rows, LANES), BF16),
        *scatter_buffers(rows),
    ]


def clear_padding(wide, hidden):
    half = wide.shape[0] // 2
    for start in (hidden, half + hidden):
        wide[pl.ds(start, half - hidden), :] = jnp.zeros((half - hidden, wide.shape[1]), BF16)


def first_kernel(
    tokens,
    gate_hbm,
    up_hbm,
    down_hbm,
    first_gain,
    mix_gain,
    query_hbm,
    forget_hbm,
    input_hbm,
    outgate_hbm,
    projected,
    mixer_share,
    send_sems,
    recv_sems,
    held,
    wide,
    down,
    sems,
    scaled,
    squares,
    acc,
    own,
    pair_out,
    pair_in,
    *rest,
):
    buffers, (low, high, share, ordered, wide_own, wide_out, wide_in), wide_buffers = (
        rest[:6],
        rest[6:13],
        rest[13:],
    )
    place = own_place()
    wire = Wire(place, send_sems, recv_sems)
    own_tokens = pltpu.make_async_copy(tokens, held.at[0, 0, 0], sems.at[3])
    own_tokens.start()
    wire.greet()
    own_tokens.wait()
    load_feed_forward(place, gate_hbm, up_hbm, down_hbm, wide, down, sems)
    width = query_hbm.shape[1]
    loads = [
        pltpu.make_async_copy(source, target.at[:, pl.ds(at, width)], sems.at[4 + index])
        for index, (source, target, at) in enumerate(
            (
                (query_hbm, low, 0),
                (forget_hbm, low, width),
                (input_hbm, high, 0),
                (outgate_hbm, high, width),
            )
        )
    ]
    for load in loads:
        load.start()
    clear_padding(wide, gate_hbm.shape[0])
    gather(wire, held)
    sums = feed_forward(
        place,
        wire,
        held,
        first_gain,
        gate_hbm,
        up_hbm,
        down_hbm,
        wide,
        down,
        sems,
        (scaled, squares, acc, own, pair_out, pair_in),
        buffers,
    )
    rows = share.shape[0]
    for (start, count, _), value in zip(halves_of(rows), sums):
        part = pl.ds(start, count)
        mixed = (held[0, 0, 0, part, :].astype(F32) + 0.5 * value).astype(BF16)
        mixer_share[part, :] = mixed
        share[part, :] = mixed.astype(F32)
    seqs = rows // BLOCKS
    for block in range(BLOCKS):
        index = block_of(place, block // (2 * RING), block // 2 % RING, block % 2)
        ordered[pl.ds(block * seqs, seqs), :] = share[
            pl.ds(pl.multiple_of(index * seqs, seqs), seqs), :
        ]
    entry = ordered[...]
    index = block_of(place, 0, 0, 0)
    mix_scaled = (entry * mix_gain[pl.ds(index, 1), :]).astype(BF16)
    square_sum = jnp.broadcast_to(jnp.sum(entry * entry, axis=1, keepdims=True), entry.shape)
    for load in loads:
        load.wait()

    def keep(at, lower, upper):
        pair = jnp.concatenate(
            [lower.reshape(BLOCKS, seqs, LANES), upper.reshape(BLOCKS, seqs, LANES)], axis=1
        ).reshape(CHIPS, 2, 2 * seqs, LANES)
        wide_own[:, pl.ds(at, 2 * seqs), :] = pair[:, 0]
        wide_out[:, pl.ds(at, 2 * seqs), :] = pair[:, 1].astype(BF16)

    columns = low.shape[1]
    tile = 2 * seqs

    def project(step, carry):
        chunk = pl.ds(pl.multiple_of(step * (2 * LANES), 2 * LANES), 2 * LANES)
        lower = jnp.dot(mix_scaled, low[:, chunk], preferred_element_type=F32)
        upper = jnp.dot(mix_scaled, high[:, chunk], preferred_element_type=F32)
        for which in (0, 1):
            at = pl.multiple_of(step * (2 * tile) + which * tile, tile)
            lanes = slice(which * LANES, (which + 1) * LANES)
            keep(at, lower[:, lanes], upper[:, lanes])
        return carry

    lax.fori_loop(0, columns // (2 * LANES), project, 0)
    keep(columns // LANES * tile, square_sum, jnp.zeros_like(square_sum))
    across = []
    wide_rows = wide_own.shape[1]
    for start, count, _ in halves_of(wide_rows):
        part = pl.ds(start, count)
        across.append(wire.send(wide_out.at[:, part, :], wide_in.at[:, part, :], "tp", 1))
    for copy in across:
        copy.wait_recv()

    def term(chip, start, count):
        at = chip[0] * RING + chip[1]
        part = pl.ds(start, count)
        return wide_own[at, part, :] + wide_in[at, part, :].astype(F32)

    sums = scatter_sum(wire, wide_rows, term, wide_buffers)
    for (start, count, _), value in zip(halves_of(wide_rows), sums):
        projected[pl.ds(start, count), :] = value
    wire.finish()


def state_kernel(
    full_width, projected, squares, floor_grid, head_gain, state, next_state, mixer_out
):
    head = pl.program_id(0)
    heads = pl.num_programs(0)
    seqs, _, keys, values = state.shape
    tile = 2 * seqs
    scale = lax.rsqrt(squares[...] / full_width + epsilon)

    def channels(block, second):
        return scale * projected[
            pl.ds(pl.multiple_of(block * tile + second * seqs, seqs), seqs), :
        ]

    query = channels(head, 0)
    entering = channels(head, 1)
    forget_pre = channels(heads + head, 0)
    gate = channels(heads + head, 1)
    floor = floor_grid[pl.ds(head, 1), :]
    forget = floor + (1.0 - floor) / (1.0 + jnp.exp(-forget_pre))
    query = query / (1.0 + jnp.exp(-query))
    forget_columns = forget.T
    query_columns = query.T
    readouts = []
    for seq in range(seqs):
        kept = jnp.broadcast_to(forget_columns[:, seq : seq + 1], (keys, values))
        asked = jnp.broadcast_to(query_columns[:, seq : seq + 1], (keys, values))
        after = kept * state[seq, 0] + (1.0 - kept) * entering[seq : seq + 1, :]
        next_state[seq, 0] = after
        readouts.append(jnp.sum(after * asked, axis=0, keepdims=True))
    readout = jnp.concatenate(readouts, axis=0)
    normed = (
        readout
        * lax.rsqrt(jnp.mean(readout * readout, axis=-1, keepdims=True) + epsilon)
        * head_gain[...]
    )
    half = heads // 2
    row = lax.rem(head, half) * tile + (head // half) * seqs
    mixer_out[pl.ds(pl.multiple_of(row, seqs), seqs), :] = normed * (gate / (1.0 + jnp.exp(-gate)))


def second_kernel(
    mixer_out,
    mixer_share,
    output_hbm,
    gate_hbm,
    up_hbm,
    down_hbm,
    second_gain,
    layer_out,
    send_sems,
    recv_sems,
    held,
    wide,
    down,
    sems,
    scaled,
    squares,
    acc,
    own,
    pair_out,
    pair_in,
    *rest,
):
    buffers, (mixed, output, update) = rest[:6], rest[6:]
    place = own_place()
    wire = Wire(place, send_sems, recv_sems)
    depth = output.shape[0]
    loads = [
        pltpu.make_async_copy(
            output_hbm.at[pl.ds(which * depth, depth), :],
            output.at[:, pl.ds(which * LANES, LANES)],
            sems.at[3 + which],
        )
        for which in (0, 1)
    ]
    for load in loads:
        load.start()
    mixed[0, 0, 0] = mixer_out[...].astype(BF16)
    wire.greet()
    load_feed_forward(place, gate_hbm, up_hbm, down_hbm, wide, down, sems)
    clear_padding(wide, gate_hbm.shape[0])
    gather(wire, mixed)
    for load in loads:
        load.wait()
    rows = update.shape[0]
    seqs = rows // BLOCKS
    tile = 2 * seqs
    total = None
    for step in range(depth // (2 * LANES)):
        pieces = [
            mixed[:, :, :, pl.ds((2 * step + which) * tile, tile), :].reshape(
                BLOCKS * tile, LANES
            )
            for which in (0, 1)
        ]
        product = jnp.dot(
            jnp.concatenate(pieces, axis=1),
            output[pl.ds(step * 2 * LANES, 2 * LANES), :],
            preferred_element_type=F32,
        )
        total = product if total is None else total + product
    total = total.reshape(BLOCKS, tile, 2 * LANES)
    total = total[:, :seqs, :LANES] + total[:, seqs:, LANES:]
    for block in range(BLOCKS):
        index = block_of(place, block // (2 * RING), block // 2 % RING, block % 2)
        update[pl.ds(pl.multiple_of(index * seqs, seqs), seqs), :] = total[block]
    held[0, 0, 0] = (mixer_share[...].astype(F32) + update[...]).astype(BF16)
    gather(wire, held)
    sums = feed_forward(
        place,
        wire,
        held,
        second_gain,
        gate_hbm,
        up_hbm,
        down_hbm,
        wide,
        down,
        sems,
        (scaled, squares, acc, own, pair_out, pair_in),
        buffers,
    )
    for (start, count, _), value in zip(halves_of(rows), sums):
        part = pl.ds(start, count)
        layer_out[part, :] = (held[0, 0, 0, part, :].astype(F32) + 0.5 * value).astype(BF16)
    wire.finish()


def in_space(*spaces):
    return [pl.BlockSpec(memory_space=space) for space in spaces]


def kernel_params(identity):
    return pltpu.CompilerParams(
        collective_id=identity, has_side_effects=True, vmem_limit_bytes=62 << 20
    )


def per_device(
    tokens,
    carried_state,
    first_gain,
    first_gate,
    first_up,
    first_down,
    mix_gain,
    query_weight,
    forget_weight,
    input_weight,
    outgate_weight,
    forget_floor,
    head_gain,
    output_weight,
    second_gain,
    second_gate,
    second_up,
    second_down,
):
    rows, share = tokens.shape
    full_width, hidden = first_gate.shape
    seqs, heads, keys, values = carried_state.shape
    tile = 2 * seqs
    wide_rows = (2 * heads + 1) * tile
    by_block = (full_width // LANES, LANES)
    projected, mixer_share = pl.pallas_call(
        first_kernel,
        name="first_block",
        out_shape=(
            jax.ShapeDtypeStruct((wide_rows, LANES), F32),
            jax.ShapeDtypeStruct((rows, share), BF16),
        ),
        in_specs=in_space(HBM, HBM, HBM, HBM, VMEM, VMEM, HBM, HBM, HBM, HBM),
        out_specs=in_space(VMEM, VMEM),
        scratch_shapes=[
            pltpu.SemaphoreType.DMA((192,)),
            pltpu.SemaphoreType.DMA((192,)),
            *feed_forward_scratch(rows, full_width, hidden),
            pltpu.VMEM((share, 2 * heads * keys), BF16),
            pltpu.VMEM((share, 2 * heads * values), BF16),
            pltpu.VMEM((rows, LANES), F32),
            pltpu.VMEM((rows, LANES), F32),
            pltpu.VMEM((CHIPS, wide_rows, LANES), F32),
            pltpu.VMEM((CHIPS, wide_rows, LANES), BF16),
            pltpu.VMEM((CHIPS, wide_rows, LANES), BF16),
            *scatter_buffers(wide_rows),
        ],
        compiler_params=kernel_params(0),
    )(
        tokens,
        first_gate.T,
        first_up.T,
        first_down,
        first_gain.reshape(by_block),
        mix_gain.reshape(by_block),
        query_weight,
        forget_weight,
        input_weight,
        outgate_weight,
    )
    whole = lambda *shape: pl.BlockSpec(shape, lambda head: (0,) * len(shape))
    one_head = pl.BlockSpec((seqs, 1, keys, values), lambda head: (0, head, 0, 0))
    next_state, mixer_out = pl.pallas_call(
        lambda *refs: state_kernel(full_width, *refs),
        name="state_update",
        grid=(heads,),
        out_shape=(
            jax.ShapeDtypeStruct(carried_state.shape, F32),
            jax.ShapeDtypeStruct((heads * seqs, values), F32),
        ),
        in_specs=[
            whole(wide_rows, LANES),
            pl.BlockSpec((seqs, LANES), lambda head: (2 * (wide_rows // tile - 1), 0)),
            whole(heads, keys),
            whole(1, values),
            one_head,
        ],
        out_specs=(one_head, whole(heads * seqs, values)),
        compiler_params=pltpu.CompilerParams(dimension_semantics=("arbitrary",)),
    )(
        projected,
        projected,
        forget_floor.reshape(heads, keys),
        head_gain.reshape(1, values),
        carried_state,
    )
    layer_out = pl.pallas_call(
        second_kernel,
        name="second_block",
        out_shape=jax.ShapeDtypeStruct((rows, share), BF16),
        in_specs=in_space(VMEM, VMEM, HBM, HBM, HBM, HBM, VMEM),
        out_specs=pl.BlockSpec(memory_space=VMEM),
        scratch_shapes=[
            pltpu.SemaphoreType.DMA((224,)),
            pltpu.SemaphoreType.DMA((224,)),
            *feed_forward_scratch(rows, full_width, hidden),
            pltpu.VMEM((RING, RING, 2, heads * seqs, LANES), BF16),
            pltpu.VMEM((heads * values // 2, 2 * LANES), BF16),
            pltpu.VMEM((rows, LANES), F32),
        ],
        compiler_params=kernel_params(1),
    )(
        mixer_out,
        mixer_share,
        output_weight,
        second_gate.T,
        second_up.T,
        second_down,
        second_gain.reshape(by_block),
    )
    return (layer_out, next_state)


def solution(mesh):
    split = Mesh(
        mesh.devices.reshape(mesh.shape["dp"], RING, RING, mesh.shape["tp"]), DP_KV_TP
    )
    return jax.shard_map(
        per_device,
        mesh=split,
        in_specs=(
            P("dp", KV_TP),
            P(DP_KV_TP, None, None, None),
            P(),
            P(None, KV_TP),
            P(None, KV_TP),
            P(KV_TP, None),
            P(),
            P(KV_TP, None),
            P(KV_TP, None),
            P(KV_TP, None),
            P(KV_TP, None),
            P(),
            P(),
            P(None, KV_TP),
            P(),
            P(None, KV_TP),
            P(None, KV_TP),
            P(KV_TP, None),
        ),
        out_specs=(P("dp", KV_TP), P(DP_KV_TP, None, None, None)),
        check_vma=False,
    )
```

```python
import jax
import jax.numpy as jnp
from jax import lax
from jax.experimental import pallas as pl
from jax.experimental.pallas import tpu as pltpu
from jax.sharding import Mesh
from jax.sharding import PartitionSpec as P

KV_TP = ("kv_0", "kv_1", "tp")
DP_KV_TP = ("dp", "kv_0", "kv_1", "tp")
MESH = pl.DeviceIdType.MESH
HBM = pltpu.MemorySpace.HBM
VMEM = pltpu.MemorySpace.VMEM
F32 = jnp.float32
BF16 = jnp.bfloat16

epsilon = 1e-06
RING = 4
LANES = 128
CHIPS = RING * RING
BLOCKS = 2 * CHIPS
NEAR = tuple((axis, step) for axis in ("kv_0", "kv_1") for step in (2, 1, 3)) + (("tp", 1),)
HALF_AXES = (("kv_1", "kv_0"), ("kv_0", "kv_1"))
FAR_FIRST = (2, 1, 3, 0)
NEAR_FIRST = (1, 3, 2)
STEPS = (2, 1, 3)
IN_LINE = ((0, 0),) + tuple((0, a) for a in NEAR_FIRST) + tuple((a, 0) for a in NEAR_FIRST)
ASIDE = tuple((a, b) for a in NEAR_FIRST for b in NEAR_FIRST)
GROUPS = (
    tuple((*chip, core) for core in (0, 1) for chip in IN_LINE),
    tuple((*chip, 0) for chip in ASIDE),
    tuple((*chip, 1) for chip in ASIDE),
)
ORDER = GROUPS[0] + GROUPS[1] + GROUPS[2]
KEPT_AT = {block: at for at, block in enumerate(ORDER)}
FIRST_CHIPS = tuple(
    chip
    for turn in FAR_FIRST
    for step in STEPS
    for chip in ((step, turn), (turn, step))
)
CHIP_ORDER = tuple(dict.fromkeys(FIRST_CHIPS)) + ((0, 0),)
POSITION = {chip: place for place, chip in enumerate(CHIP_ORDER)}


def own_place():
    return (lax.axis_index("kv_0"), lax.axis_index("kv_1"), lax.axis_index("tp"))


def block_of(place, along_0, along_1, other_core):
    at_0, at_1, core = place
    return (
        lax.rem(at_0 + along_0, RING) * (2 * RING)
        + lax.rem(at_1 + along_1, RING) * 2
        + lax.rem(core + other_core, 2)
    )


class Wire:
    def __init__(self, place, send_sems, recv_sems):
        at_0, at_1, core = place
        self.place = {"kv_0": (at_0, RING), "kv_1": (at_1, RING), "tp": (core, 2)}
        self.send_sems, self.recv_sems = send_sems, recv_sems
        self.used = 0
        self.sent = []

    def near(self, axis, step):
        at, size = self.place[axis]
        return {axis: lax.rem(at + step, size)}

    def greet(self):
        barrier = pltpu.get_barrier_semaphore()
        for axis, step in NEAR:
            pl.semaphore_signal(
                barrier, inc=1, device_id=self.near(axis, step), device_id_type=MESH
            )
        pl.semaphore_wait(barrier, len(NEAR))

    def take(self, count):
        first = self.used
        self.used += count
        return first

    def make(self, source, target, axis, step, slot):
        return pltpu.make_async_remote_copy(
            src_ref=source,
            dst_ref=target,
            send_sem=self.send_sems.at[slot],
            recv_sem=self.recv_sems.at[slot],
            device_id=self.near(axis, step),
            device_id_type=MESH,
        )

    def send(self, source, target, axis, step):
        copy = self.make(source, target, axis, step, self.take(1))
        copy.start()
        self.sent.append(copy)
        return copy

    def finish(self):
        for copy in self.sent:
            copy.wait_send()
        self.sent = []


def halves_of(rows):
    tiles = rows // 16
    first = (tiles - tiles // 2) * 16
    second = rows - first
    return ((0, first, first // 32 * 16), (first, second, second // 32 * 16))


def gather(wire, held, ready=None):
    halves = halves_of(held.shape[1])
    copies = {}

    def view(half, first, second, core=0):
        start, rows, _ = halves[half]
        along = (second, first) if HALF_AXES[half][0] == "kv_1" else (first, second)
        return held.at[KEPT_AT[(*along, core)], pl.ds(start, rows), :]

    def spread(half, stage, first, steps=STEPS):
        for step in steps:
            there = RING - step
            target = view(half, there, 0) if stage == 0 else view(half, first, there)
            copies[half, stage, first, there] = wire.send(
                view(half, first, 0), target, HALF_AXES[half][stage], step
            )

    def across(half, first, second):
        copies[half, "across", first, second] = wire.send(
            view(half, first, second), view(half, first, second, 1), "tp", 1
        )

    def arrive(half, stage, first, there):
        copies[half, stage, first, there].wait_recv()

    both = (0, 1)
    for half in both:
        spread(half, 0, 0, NEAR_FIRST)
    for half in both:
        spread(half, 1, 0)
    for half in both:
        across(half, 0, 0)
    for there in NEAR_FIRST:
        for half in both:
            arrive(half, 0, 0, there)
            spread(half, 1, there)
            across(half, there, 0)
    for there in NEAR_FIRST:
        for half in both:
            arrive(half, 1, 0, there)
            across(half, 0, there)

    def settle(chips):
        for half in both:
            for chip in chips:
                first, second = chip[::-1] if HALF_AXES[half][0] == "kv_1" else chip
                arrive(half, "across", first, second)

    settle(IN_LINE)
    if ready:
        ready(0)
    for first in NEAR_FIRST:
        for there in NEAR_FIRST:
            for half in both:
                arrive(half, 1, first, there)
                across(half, first, there)
    if ready:
        ready(1)
    settle(ASIDE)
    if ready:
        ready(2)


def axes_chip(half, first, second):
    return (second, first) if HALF_AXES[half][0] == "kv_1" else (first, second)


def add_up(wire, halves, value, last_out, last_in):
    copies = {}
    sums = [None, None]
    for turn, second in enumerate(FAR_FIRST):
        for half in (0, 1):
            count = halves[half][1]
            result = value(turn, half)
            if second == 0:
                sums[half] = result
                continue
            last_out[half, turn, pl.ds(0, count), :] = result.astype(BF16)
            copies[half, turn] = wire.send(
                last_out.at[half, turn, pl.ds(0, count), :],
                last_in.at[half, turn, pl.ds(0, count), :],
                HALF_AXES[half][1],
                second,
            )
    for turn in (1, 2, 0):
        for half in (0, 1):
            copies[half, turn].wait_recv()
            sums[half] += last_in[half, turn, pl.ds(0, halves[half][1]), :].astype(F32)
    return sums


def scatter_direct(wire, rows, term, between, buffers):
    halves = halves_of(rows)
    early_out, early_in, last_out, last_in = buffers
    copies = {}
    for turn, second in enumerate(FAR_FIRST):
        for way, step in enumerate(STEPS):
            for half in (0, 1):
                start, count, _ = halves[half]
                early_out[half, turn, way, pl.ds(0, count), :] = term(
                    axes_chip(half, step, second), start, count
                ).astype(BF16)
                copies[half, turn, way] = wire.send(
                    early_out.at[half, turn, way, pl.ds(0, count), :],
                    early_in.at[half, turn, way, pl.ds(0, count), :],
                    HALF_AXES[half][0],
                    step,
                )
        between(turn)

    def value(turn, half):
        start, count, _ = halves[half]
        result = term(axes_chip(half, 0, FAR_FIRST[turn]), start, count)
        for way in range(len(STEPS)):
            copies[half, turn, way].wait_recv()
            result += early_in[half, turn, way, pl.ds(0, count), :].astype(F32)
        return result

    return add_up(wire, halves, value, last_out, last_in)


def scatter_relayed(wire, rows, term, before, buffers):
    halves = halves_of(rows)
    early_out, early_in, late_out, late_in, last_out, last_in = buffers
    copies = {}

    def parts(half):
        _, count, cut = halves[half]
        return ((0, cut, 1), (cut, count - cut, 3))

    for half in (0, 1):
        before(half)
        for turn, second in enumerate(FAR_FIRST):
            start, count, _ = halves[half]
            early_out[half, turn, pl.ds(0, count), :] = term(
                axes_chip(half, 2, second), start, count
            ).astype(BF16)
            for at, length, step in parts(half):
                copies["early", half, turn, step] = wire.send(
                    early_out.at[half, turn, pl.ds(at, length), :],
                    early_in.at[half, turn, pl.ds(at, length), :],
                    HALF_AXES[half][0],
                    step,
                )
    for turn, second in enumerate(FAR_FIRST):
        for half in (0, 1):
            start, count, _ = halves[half]
            for way, (at, length, step) in enumerate(parts(half)):
                near = axes_chip(half, step, second)
                rest_at, rest = (length, count - length) if at == 0 else (0, at)
                late_out[half, turn, way, pl.ds(rest_at, rest), :] = term(
                    near, start + rest_at, rest
                ).astype(BF16)
                copies["early", half, turn, step].wait_recv()
                late_out[half, turn, way, pl.ds(at, length), :] = (
                    term(near, start + at, length)
                    + early_in[half, turn, pl.ds(at, length), :].astype(F32)
                ).astype(BF16)
                copies["late", half, turn, way] = wire.send(
                    late_out.at[half, turn, way, pl.ds(0, count), :],
                    late_in.at[half, turn, way, pl.ds(0, count), :],
                    HALF_AXES[half][0],
                    step,
                )

    def value(turn, half):
        start, count, _ = halves[half]
        result = term(axes_chip(half, 0, FAR_FIRST[turn]), start, count)
        for way in (0, 1):
            copies["late", half, turn, way].wait_recv()
            result += late_in[half, turn, way, pl.ds(0, count), :].astype(F32)
        return result

    return add_up(wire, halves, value, last_out, last_in)


def scatter_buffers(rows, relayed):
    half = halves_of(rows)[0][1]
    first = [(2, RING), (2, RING, 2)] if relayed else [(2, RING, len(STEPS))]
    return [
        pltpu.VMEM((*lead, half, LANES), BF16)
        for lead in (*first, (2, RING))
        for _ in (0, 1)
    ]


def load_feed_forward(place, gate_hbm, up_hbm, down_hbm, wide, down, sems):
    hidden = gate_hbm.shape[0]
    half = wide.shape[0] // 2
    for at, block in enumerate(ORDER):
        columns = pl.ds(pl.multiple_of(block_of(place, *block) * LANES, LANES), LANES)
        here = pl.ds(at * LANES, LANES)
        pltpu.make_async_copy(
            gate_hbm.at[:, columns], wide.at[pl.ds(0, hidden), here], sems.at[0]
        ).start()
        pltpu.make_async_copy(
            up_hbm.at[:, columns], wide.at[pl.ds(half, hidden), here], sems.at[1]
        ).start()
    for at, (along_0, along_1) in enumerate(CHIP_ORDER):
        for other in (0, 1):
            columns = pl.ds(
                pl.multiple_of(block_of(place, along_0, along_1, other) * LANES, LANES), LANES
            )
            pltpu.make_async_copy(
                down_hbm.at[:, columns],
                down.at[at // 2, :, pl.ds((at % 2 * 2 + other) * LANES, LANES)],
                sems.at[2],
            ).start()


def feed_forward(
    place, wire, held, gain, gate_hbm, up_hbm, down_hbm, wide, down, sems, scratch, buffers
):
    scaled, squares, gains, acc, own, pair_out, pair_in = scratch
    hidden, half = (gate_hbm.shape[0], wide.shape[0] // 2)
    rows, width = scaled.shape
    squares[...] = jnp.zeros_like(squares)
    for at, block in enumerate(ORDER):
        gains[pl.ds(at, 1), :] = gain[pl.ds(block_of(place, *block), 1), :]

    def scale(block, carry):
        entry = held[block].astype(F32)
        squares[...] += entry * entry
        scaled[:, pl.ds(pl.multiple_of(block * LANES, LANES), LANES)] = (
            entry * gains[pl.ds(block, 1), :]
        ).astype(BF16)
        return carry

    def ready(group):
        with jax.named_scope("scale_and_product"):
            first = sum(len(blocks) for blocks in GROUPS[:group])
            last = first + len(GROUPS[group])
            lax.fori_loop(first, last, scale, 0)
            if group == 0:
                pltpu.make_async_copy(gate_hbm, wide.at[pl.ds(0, hidden), :], sems.at[0]).wait()
                pltpu.make_async_copy(up_hbm, wide.at[pl.ds(half, hidden), :], sems.at[1]).wait()
            chunk = pl.ds(first * LANES, (last - first) * LANES)
            part = lax.dot_general(
                scaled[:, chunk],
                wide[:, chunk],
                (((1,), (1,)), ((), ())),
                preferred_element_type=F32,
            )
            acc[...] = part if group == 0 else acc[...] + part

    with jax.named_scope("gather_features"):
        gather(wire, held, ready)
    with jax.named_scope("hidden"):
        row_scale = lax.rsqrt(jnp.sum(squares[...], axis=1, keepdims=True) / width + epsilon)
        gate = row_scale * acc[:, :hidden]
        up = row_scale * acc[:, half : half + hidden]
        units = (gate / (1.0 + jnp.exp(-gate)) * up).astype(BF16)
        pltpu.make_async_copy(down, down, sems.at[2]).wait()
    pairs = CHIPS // 2
    first = wire.take(pairs)

    def pair_copy(at):
        part = pl.ds(2 * at, 2)
        return wire.make(pair_out.at[part], pair_in.at[part], "tp", 1, first + at)

    done = [0]

    def project(until):
        with jax.named_scope("down"):
            for at in range(done[0], until):
                result = jnp.dot(units, down[at], preferred_element_type=F32)
                for which in (0, 1):
                    at_lane = 2 * which * LANES
                    own[2 * at + which] = result[:, at_lane : at_lane + LANES]
                    pair_out[2 * at + which] = result[
                        :, at_lane + LANES : at_lane + 2 * LANES
                    ].astype(BF16)
                pair_copy(at).start()
            done[0] = max(done[0], until)

    arrived = set()

    def term(chip, start, count):
        at = POSITION[chip]
        if at // 2 not in arrived:
            arrived.add(at // 2)
            pair_copy(at // 2).wait_recv()
        return own[at, pl.ds(start, count), :] + pair_in[at, pl.ds(start, count), :].astype(F32)

    project(4)
    with jax.named_scope("scatter_features"):
        sums = scatter_direct(
            wire, rows, term, lambda turn: project((5, 8, 8, 8)[turn]), buffers
        )
    wire.sent += [pair_copy(at) for at in range(pairs)]
    return sums


def feed_forward_scratch(rows, width, hidden):
    half = -(-hidden // LANES) * LANES
    return [
        pltpu.VMEM((BLOCKS, rows, LANES), BF16),
        pltpu.VMEM((2 * half, width), BF16),
        pltpu.VMEM((CHIPS // 2, hidden, 4 * LANES), BF16),
        pltpu.SemaphoreType.DMA((10,)),
        pltpu.VMEM((rows, width), BF16),
        pltpu.VMEM((rows, LANES), F32),
        pltpu.VMEM((BLOCKS, LANES), F32),
        pltpu.VMEM((rows, 2 * half), F32),
        pltpu.VMEM((CHIPS, rows, LANES), F32),
        pltpu.VMEM((CHIPS, rows, LANES), BF16),
        pltpu.VMEM((CHIPS, rows, LANES), BF16),
        *scatter_buffers(rows, False),
    ]


def clear_padding(wide, hidden):
    half = wide.shape[0] // 2
    for start in (hidden, half + hidden):
        wide[pl.ds(start, half - hidden), :] = jnp.zeros((half - hidden, wide.shape[1]), BF16)


def first_kernel(
    tokens,
    gate_hbm,
    up_hbm,
    down_hbm,
    first_gain_hbm,
    mix_gain_hbm,
    query_hbm,
    forget_hbm,
    input_hbm,
    outgate_hbm,
    projected,
    mixer_share,
    send_sems,
    recv_sems,
    held,
    wide,
    down,
    sems,
    scaled,
    squares,
    gains,
    acc,
    own,
    pair_out,
    pair_in,
    *rest,
):
    buffers, own_refs, wide_buffers = (rest[:4], rest[4:13], rest[13:])
    low, high, share, ordered, wide_own, wide_out, wide_in, first_gain, mix_gain = own_refs
    place = own_place()
    wire = Wire(place, send_sems, recv_sems)
    own_tokens = pltpu.make_async_copy(tokens, held.at[0], sems.at[3])
    own_tokens.start()
    gain_loads = [
        pltpu.make_async_copy(first_gain_hbm, first_gain, sems.at[8]),
        pltpu.make_async_copy(mix_gain_hbm, mix_gain, sems.at[9]),
    ]
    for load in gain_loads:
        load.start()
    with jax.named_scope("greet"):
        wire.greet()
    own_tokens.wait()
    with jax.named_scope("issue_loads"):
        load_feed_forward(place, gate_hbm, up_hbm, down_hbm, wide, down, sems)
    width = query_hbm.shape[1]
    loads = [
        pltpu.make_async_copy(source, target.at[:, pl.ds(at, width)], sems.at[4 + index])
        for index, (source, target, at) in enumerate(
            (
                (query_hbm, low, 0),
                (forget_hbm, low, width),
                (input_hbm, high, 0),
                (outgate_hbm, high, width),
            )
        )
    ]
    for load in loads:
        load.start()
    clear_padding(wide, gate_hbm.shape[0])
    for load in gain_loads:
        load.wait()
    sums = feed_forward(
        place,
        wire,
        held,
        first_gain,
        gate_hbm,
        up_hbm,
        down_hbm,
        wide,
        down,
        sems,
        (scaled, squares, gains, acc, own, pair_out, pair_in),
        buffers,
    )
    rows = share.shape[0]
    for (start, count, _), value in zip(halves_of(rows), sums):
        part = pl.ds(start, count)
        mixed = (held[0, part, :].astype(F32) + 0.5 * value).astype(BF16)
        mixer_share[part, :] = mixed
        share[part, :] = mixed.astype(F32)
    seqs = rows // BLOCKS
    for block in range(BLOCKS):
        index = block_of(place, block // (2 * RING), block // 2 % RING, block % 2)
        ordered[pl.ds(block * seqs, seqs), :] = share[
            pl.ds(pl.multiple_of(index * seqs, seqs), seqs), :
        ]
    entry = ordered[...]
    index = block_of(place, 0, 0, 0)
    mix_scaled = (entry * mix_gain[pl.ds(index, 1), :]).astype(BF16)
    square_sum = jnp.broadcast_to(jnp.sum(entry * entry, axis=1, keepdims=True), entry.shape)
    for load in loads:
        load.wait()

    def keep(at, lower, upper):
        pair = jnp.concatenate(
            [lower.reshape(BLOCKS, seqs, LANES), upper.reshape(BLOCKS, seqs, LANES)], axis=1
        ).reshape(CHIPS, 2, 2 * seqs, LANES)
        wide_own[:, pl.ds(at, 2 * seqs), :] = pair[:, 0]
        wide_out[:, pl.ds(at, 2 * seqs), :] = pair[:, 1].astype(BF16)

    tile = 2 * seqs
    heads2 = low.shape[1] // LANES
    groups = (0, 5, 9, 13, heads2 // 2)
    copies = {}

    def project(group):
        with jax.named_scope("project"):
            for step in range(groups[group], groups[group + 1]):
                chunk = slice(2 * step * LANES, 2 * (step + 1) * LANES)
                lower = jnp.dot(mix_scaled, low[:, chunk], preferred_element_type=F32)
                upper = jnp.dot(mix_scaled, high[:, chunk], preferred_element_type=F32)
                for which in (0, 1):
                    lanes = slice(which * LANES, (which + 1) * LANES)
                    keep((2 * step + which) * tile, lower[:, lanes], upper[:, lanes])
            begin = 2 * groups[group] * tile
            end = 2 * groups[group + 1] * tile
            if group + 2 == len(groups):
                keep(end, square_sum, jnp.zeros_like(square_sum))
                end += tile
            part = pl.ds(begin, end - begin)
            copies[group] = wire.send(wide_out.at[:, part, :], wide_in.at[:, part, :], "tp", 1)

    def before(half):
        if half == 0:
            for group in (0, 1, 2):
                project(group)
        else:
            project(3)
        with jax.named_scope("pair"):
            for group in (2 * half, 2 * half + 1):
                copies[group].wait_recv()

    wide_rows = wide_own.shape[1]

    def term(chip, start, count):
        at = chip[0] * RING + chip[1]
        part = pl.ds(start, count)
        return wide_own[at, part, :] + wide_in[at, part, :].astype(F32)

    with jax.named_scope("scatter_wide"):
        sums = scatter_relayed(wire, wide_rows, term, before, wide_buffers)
    for (start, count, _), value in zip(halves_of(wide_rows), sums):
        projected[pl.ds(start, count), :] = value
    with jax.named_scope("finish"):
        wire.finish()


def state_kernel(
    full_width, projected, floor_grid, head_gain, state, next_state, mixer_out, held, sems
):
    seqs, heads, keys, values = state.shape
    tile = 2 * seqs
    writes = [
        pltpu.make_async_copy(held.at[head], next_state.at[:, head], sems.at[head])
        for head in range(heads)
    ]
    squares = projected[pl.ds(2 * heads * tile, seqs), :]
    scale = lax.rsqrt(squares / full_width + epsilon)

    def channels(block, second):
        return scale * projected[pl.ds(block * tile + second * seqs, seqs), :]

    row_seq = lax.broadcasted_iota(jnp.int32, (4 * seqs, seqs * values), 0) % seqs
    lane_seq = lax.broadcasted_iota(jnp.int32, (4 * seqs, seqs * values), 1) // values
    spreader = (row_seq == lane_seq).astype(F32).astype(BF16)

    def pieces(entry):
        first = entry.astype(BF16).astype(F32)
        second = (entry - first).astype(BF16).astype(F32)
        third = entry - first - second
        return jnp.concatenate([first, second, third, jnp.zeros_like(entry)], axis=0)

    for head in range(heads):
        query = channels(head, 0)
        entering = channels(head, 1)
        forget_pre = channels(heads + head, 0)
        gate = channels(heads + head, 1)
        floor = floor_grid[pl.ds(head, 1), :]
        forget = floor + (1.0 - floor) / (1.0 + jnp.exp(-forget_pre))
        query = query / (1.0 + jnp.exp(-query))
        both = jnp.concatenate([pieces(forget), pieces(query)], axis=1).T.astype(BF16)
        spread = jnp.dot(both, spreader, preferred_element_type=F32)
        readouts = []
        for seq in range(seqs):
            kept = spread[:keys, seq * values : (seq + 1) * values]
            asked = spread[keys:, seq * values : (seq + 1) * values]
            after = kept * state[seq, head] + (1.0 - kept) * entering[seq : seq + 1, :]
            held[head, seq] = after
            readouts.append(jnp.sum(after * asked, axis=0, keepdims=True))
        writes[head].start()
        readout = jnp.concatenate(readouts, axis=0)
        normed = (
            readout
            * lax.rsqrt(jnp.mean(readout * readout, axis=-1, keepdims=True) + epsilon)
            * head_gain[...]
        )
        half = heads // 2
        row = head % half * tile + head // half * seqs
        mixer_out[pl.ds(row, seqs), :] = normed * (gate / (1.0 + jnp.exp(-gate)))
    for write in writes:
        write.wait()


def second_kernel(
    mixer_out,
    share_hbm,
    output_hbm,
    gate_hbm,
    up_hbm,
    down_hbm,
    gain_hbm,
    layer_out,
    send_sems,
    recv_sems,
    held,
    wide,
    down,
    sems,
    scaled,
    squares,
    gains,
    acc,
    own,
    pair_out,
    pair_in,
    *rest,
):
    buffers, (mixed, output, update, mixer_share, second_gain) = rest[:4], rest[4:]
    place = own_place()
    wire = Wire(place, send_sems, recv_sems)
    depth = output.shape[0]
    loads = [
        pltpu.make_async_copy(
            output_hbm.at[pl.ds(which * depth, depth), :],
            output.at[:, pl.ds(which * LANES, LANES)],
            sems.at[3 + which],
        )
        for which in (0, 1)
    ] + [
        pltpu.make_async_copy(share_hbm, mixer_share, sems.at[5]),
        pltpu.make_async_copy(gain_hbm, second_gain, sems.at[6]),
    ]
    for load in loads:
        load.start()
    mixed[0] = mixer_out[...].astype(BF16)
    with jax.named_scope("greet"):
        wire.greet()
    with jax.named_scope("issue_loads"):
        load_feed_forward(place, gate_hbm, up_hbm, down_hbm, wide, down, sems)
    clear_padding(wide, gate_hbm.shape[0])
    with jax.named_scope("gather_mixed"):
        gather(wire, mixed)
    for load in loads:
        load.wait()
    rows = update.shape[0]
    seqs = rows // BLOCKS
    tile = 2 * seqs
    total = None
    for step in range(depth // (2 * LANES)):
        pieces = [
            mixed[:, pl.ds((2 * step + which) * tile, tile), :].reshape(
                BLOCKS * tile, LANES
            )
            for which in (0, 1)
        ]
        product = jnp.dot(
            jnp.concatenate(pieces, axis=1),
            output[pl.ds(step * 2 * LANES, 2 * LANES), :],
            preferred_element_type=F32,
        )
        total = product if total is None else total + product
    total = total.reshape(BLOCKS, tile, 2 * LANES)
    total = total[:, :seqs, :LANES] + total[:, seqs:, LANES:]
    for block in range(BLOCKS):
        index = block_of(place, *ORDER[block])
        update[pl.ds(pl.multiple_of(index * seqs, seqs), seqs), :] = total[block]
    held[0] = (mixer_share[...].astype(F32) + update[...]).astype(BF16)
    sums = feed_forward(
        place,
        wire,
        held,
        second_gain,
        gate_hbm,
        up_hbm,
        down_hbm,
        wide,
        down,
        sems,
        (scaled, squares, gains, acc, own, pair_out, pair_in),
        buffers,
    )
    for (start, count, _), value in zip(halves_of(rows), sums):
        part = pl.ds(start, count)
        layer_out[part, :] = (held[0, part, :].astype(F32) + 0.5 * value).astype(BF16)
    with jax.named_scope("finish"):
        wire.finish()


def in_space(*spaces):
    return [pl.BlockSpec(memory_space=space) for space in spaces]


def kernel_params(identity, mebibytes):
    return pltpu.CompilerParams(
        collective_id=identity, has_side_effects=True, vmem_limit_bytes=mebibytes << 20
    )


def per_device(
    tokens,
    carried_state,
    first_gain,
    first_gate,
    first_up,
    first_down,
    mix_gain,
    query_weight,
    forget_weight,
    input_weight,
    outgate_weight,
    forget_floor,
    head_gain,
    output_weight,
    second_gain,
    second_gate,
    second_up,
    second_down,
):
    rows, share = tokens.shape
    full_width, hidden = first_gate.shape
    seqs, heads, keys, values = carried_state.shape
    tile = 2 * seqs
    wide_rows = (2 * heads + 1) * tile
    by_block = (full_width // LANES, LANES)
    projected, mixer_share = pl.pallas_call(
        first_kernel,
        name="first_block",
        out_shape=(
            jax.ShapeDtypeStruct((wide_rows, LANES), F32),
            jax.ShapeDtypeStruct((rows, share), BF16),
        ),
        in_specs=in_space(*(HBM,) * 10),
        out_specs=in_space(VMEM, VMEM),
        scratch_shapes=[
            pltpu.SemaphoreType.DMA((192,)),
            pltpu.SemaphoreType.DMA((192,)),
            *feed_forward_scratch(rows, full_width, hidden),
            pltpu.VMEM((share, 2 * heads * keys), BF16),
            pltpu.VMEM((share, 2 * heads * values), BF16),
            pltpu.VMEM((rows, LANES), F32),
            pltpu.VMEM((rows, LANES), F32),
            pltpu.VMEM((CHIPS, wide_rows, LANES), F32),
            pltpu.VMEM((CHIPS, wide_rows, LANES), BF16),
            pltpu.VMEM((CHIPS, wide_rows, LANES), BF16),
            pltpu.VMEM(by_block, F32),
            pltpu.VMEM(by_block, F32),
            *scatter_buffers(wide_rows, True),
        ],
        compiler_params=kernel_params(0, 54),
    )(
        tokens,
        first_gate.T,
        first_up.T,
        first_down,
        first_gain.reshape(by_block),
        mix_gain.reshape(by_block),
        query_weight,
        forget_weight,
        input_weight,
        outgate_weight,
    )
    next_state, mixer_out = pl.pallas_call(
        lambda *refs: state_kernel(full_width, *refs),
        name="state_update",
        out_shape=(
            jax.ShapeDtypeStruct(carried_state.shape, F32),
            jax.ShapeDtypeStruct((heads * seqs, values), F32),
        ),
        in_specs=in_space(VMEM, VMEM, VMEM, VMEM),
        out_specs=in_space(HBM, VMEM),
        scratch_shapes=[
            pltpu.VMEM((heads, seqs, keys, values), F32),
            pltpu.SemaphoreType.DMA((heads,)),
        ],
        compiler_params=pltpu.CompilerParams(vmem_limit_bytes=12 << 20),
    )(
        projected,
        forget_floor.reshape(heads, keys),
        head_gain.reshape(1, values),
        carried_state,
    )
    layer_out = pl.pallas_call(
        second_kernel,
        name="second_block",
        out_shape=jax.ShapeDtypeStruct((rows, share), BF16),
        in_specs=in_space(VMEM, *(HBM,) * 6),
        out_specs=pl.BlockSpec(memory_space=VMEM),
        scratch_shapes=[
            pltpu.SemaphoreType.DMA((224,)),
            pltpu.SemaphoreType.DMA((224,)),
            *feed_forward_scratch(rows, full_width, hidden),
            pltpu.VMEM((BLOCKS, heads * seqs, LANES), BF16),
            pltpu.VMEM((heads * values // 2, 2 * LANES), BF16),
            pltpu.VMEM((rows, LANES), F32),
            pltpu.VMEM((rows, LANES), BF16),
            pltpu.VMEM(by_block, F32),
        ],
        compiler_params=kernel_params(1, 58),
    )(
        mixer_out,
        mixer_share,
        output_weight,
        second_gate.T,
        second_up.T,
        second_down,
        second_gain.reshape(by_block),
    )
    return (layer_out, next_state)


def solution(mesh):
    split = Mesh(
        mesh.devices.reshape(mesh.shape["dp"], RING, RING, mesh.shape["tp"]), DP_KV_TP
    )
    return jax.shard_map(
        per_device,
        mesh=split,
        in_specs=(
            P("dp", KV_TP),
            P(DP_KV_TP, None, None, None),
            P(),
            P(None, KV_TP),
            P(None, KV_TP),
            P(KV_TP, None),
            P(),
            P(KV_TP, None),
            P(KV_TP, None),
            P(KV_TP, None),
            P(KV_TP, None),
            P(),
            P(),
            P(None, KV_TP),
            P(),
            P(None, KV_TP),
            P(None, KV_TP),
            P(KV_TP, None),
        ),
        out_specs=(P("dp", KV_TP), P(DP_KV_TP, None, None, None)),
        check_vma=False,
    )
```

```python
import jax
import jax.numpy as jnp
from jax import lax
from jax.experimental import pallas as pl
from jax.experimental.pallas import tpu as pltpu
from jax.sharding import Mesh
from jax.sharding import PartitionSpec as P

KV_TP = ("kv_0", "kv_1", "tp")
DP_KV_TP = ("dp", "kv_0", "kv_1", "tp")
MESH = pl.DeviceIdType.MESH
HBM = pltpu.MemorySpace.HBM
VMEM = pltpu.MemorySpace.VMEM
F32 = jnp.float32
BF16 = jnp.bfloat16

epsilon = 1e-06
RING = 4
LANES = 128
CHIPS = RING * RING
BLOCKS = 2 * CHIPS
NEAR = tuple((axis, step) for axis in ("kv_0", "kv_1") for step in (2, 1, 3)) + (("tp", 1),)
HALF_AXES = (("kv_1", "kv_0"), ("kv_0", "kv_1"))
FAR_FIRST = (2, 1, 3, 0)
NEAR_FIRST = (1, 3, 2)
STEPS = (2, 1, 3)
IN_LINE = ((0, 0),) + tuple((0, a) for a in NEAR_FIRST) + tuple((a, 0) for a in NEAR_FIRST)
EARLY = tuple((a, b) for a in (1, 3) for b in (1, 3))
LATE = tuple((a, 2) for a in (1, 3)) + tuple((2, a) for a in NEAR_FIRST)
GROUPS = (
    tuple((*chip, core) for core in (0, 1) for chip in IN_LINE),
    *(tuple((*chip, core) for chip in chips) for chips in (EARLY, LATE) for core in (0, 1)),
)
ORDER = sum(GROUPS, ())
KEPT_AT = {block: at for at, block in enumerate(ORDER)}
FIRST_CHIPS = tuple(
    chip
    for turn in FAR_FIRST
    for step in STEPS
    for chip in ((step, turn), (turn, step))
)
CHIP_ORDER = tuple(dict.fromkeys(FIRST_CHIPS)) + ((0, 0),)
POSITION = {chip: place for place, chip in enumerate(CHIP_ORDER)}


def own_place():
    return (lax.axis_index("kv_0"), lax.axis_index("kv_1"), lax.axis_index("tp"))


def block_of(place, along_0, along_1, other_core):
    at_0, at_1, core = place
    return (
        lax.rem(at_0 + along_0, RING) * (2 * RING)
        + lax.rem(at_1 + along_1, RING) * 2
        + lax.rem(core + other_core, 2)
    )


class Wire:
    def __init__(self, place, send_sems, recv_sems):
        at_0, at_1, core = place
        self.place = {"kv_0": (at_0, RING), "kv_1": (at_1, RING), "tp": (core, 2)}
        self.send_sems, self.recv_sems = send_sems, recv_sems
        self.used = 0
        self.sent = []

    def near(self, axis, step):
        at, size = self.place[axis]
        return {axis: lax.rem(at + step, size)}

    def greet(self, meanwhile):
        barrier = pltpu.get_barrier_semaphore()
        for axis, step in NEAR:
            pl.semaphore_signal(
                barrier, inc=1, device_id=self.near(axis, step), device_id_type=MESH
            )
        meanwhile()
        pl.semaphore_wait(barrier, len(NEAR))

    def take(self, count):
        first = self.used
        self.used += count
        return first

    def make(self, source, target, axis, step, slot):
        return pltpu.make_async_remote_copy(
            src_ref=source,
            dst_ref=target,
            send_sem=self.send_sems.at[slot],
            recv_sem=self.recv_sems.at[slot],
            device_id=self.near(axis, step),
            device_id_type=MESH,
        )

    def send(self, source, target, axis, step):
        copy = self.make(source, target, axis, step, self.take(1))
        copy.start()
        self.sent.append(copy)
        return copy

    def finish(self):
        for copy in self.sent:
            copy.wait_send()
        self.sent = []


def halves_of(rows):
    tiles = rows // 16
    first = (tiles - tiles // 2) * 16
    second = rows - first
    return ((0, first, first // 32 * 16), (first, second, second // 32 * 16))


def gather(wire, held, ready=None):
    halves = halves_of(held.shape[1])
    copies = {}

    def view(half, first, second, core=0):
        start, rows, _ = halves[half]
        along = (second, first) if HALF_AXES[half][0] == "kv_1" else (first, second)
        return held.at[KEPT_AT[(*along, core)], pl.ds(start, rows), :]

    def spread(half, stage, first, steps=STEPS):
        for step in steps:
            there = RING - step
            target = view(half, there, 0) if stage == 0 else view(half, first, there)
            copies[half, stage, first, there] = wire.send(
                view(half, first, 0), target, HALF_AXES[half][stage], step
            )

    def across(half, first, second):
        copies[half, "across", first, second] = wire.send(
            view(half, first, second), view(half, first, second, 1), "tp", 1
        )

    def arrive(half, stage, first, there):
        copies[half, stage, first, there].wait_recv()

    both = (0, 1)
    for half in both:
        spread(half, 0, 0, NEAR_FIRST)
    for half in both:
        spread(half, 1, 0)
    for half in both:
        across(half, 0, 0)
    for there in NEAR_FIRST:
        for half in both:
            arrive(half, 0, 0, there)
            spread(half, 1, there)
            across(half, there, 0)
    for there in NEAR_FIRST:
        for half in both:
            arrive(half, 1, 0, there)
            across(half, 0, there)

    def settle(chips):
        for half in both:
            for chip in chips:
                first, second = chip[::-1] if HALF_AXES[half][0] == "kv_1" else chip
                arrive(half, "across", first, second)

    def pass_on(firsts, theres):
        for first in firsts:
            for there in theres:
                for half in both:
                    arrive(half, 1, first, there)
                    across(half, first, there)

    ready = ready or (lambda group: None)
    settle(IN_LINE)
    ready(0)
    pass_on((1, 3), (1, 3))
    ready(1)
    pass_on((1, 3), (2,))
    pass_on((2,), (1, 3, 2))
    settle(EARLY)
    ready(2)
    ready(3)
    settle(LATE)
    ready(4)


def axes_chip(half, first, second):
    return (second, first) if HALF_AXES[half][0] == "kv_1" else (first, second)


def add_up(wire, halves, value, last_out, last_in):
    copies = {}
    sums = [None, None]
    for turn, second in enumerate(FAR_FIRST):
        for half in (0, 1):
            count = halves[half][1]
            result = value(turn, half)
            if second == 0:
                sums[half] = result
                continue
            last_out[half, turn, pl.ds(0, count), :] = result.astype(BF16)
            copies[half, turn] = wire.send(
                last_out.at[half, turn, pl.ds(0, count), :],
                last_in.at[half, turn, pl.ds(0, count), :],
                HALF_AXES[half][1],
                second,
            )
    for turn in (1, 2, 0):
        for half in (0, 1):
            copies[half, turn].wait_recv()
            sums[half] += last_in[half, turn, pl.ds(0, halves[half][1]), :].astype(F32)
    return sums


def scatter_direct(wire, rows, term, between, buffers):
    halves = halves_of(rows)
    early_out, early_in, last_out, last_in = buffers
    copies = {}
    for turn, second in enumerate(FAR_FIRST):
        for way, step in enumerate(STEPS):
            for half in (0, 1):
                start, count, _ = halves[half]
                early_out[half, turn, way, pl.ds(0, count), :] = term(
                    axes_chip(half, step, second), start, count
                ).astype(BF16)
                copies[half, turn, way] = wire.send(
                    early_out.at[half, turn, way, pl.ds(0, count), :],
                    early_in.at[half, turn, way, pl.ds(0, count), :],
                    HALF_AXES[half][0],
                    step,
                )
        between(turn)

    def value(turn, half):
        start, count, _ = halves[half]
        result = term(axes_chip(half, 0, FAR_FIRST[turn]), start, count)
        for way in range(len(STEPS)):
            copies[half, turn, way].wait_recv()
            result += early_in[half, turn, way, pl.ds(0, count), :].astype(F32)
        return result

    return add_up(wire, halves, value, last_out, last_in)


def scatter_relayed(wire, rows, term, buffers):
    halves = halves_of(rows)
    early_out, early_in, late_out, late_in, last_out, last_in = buffers
    copies = {}

    def parts(half):
        _, count, cut = halves[half]
        return ((0, cut, 1), (cut, count - cut, 3))

    for half in (0, 1):
        for turn, second in enumerate(FAR_FIRST):
            start, count, _ = halves[half]
            early_out[half, turn, pl.ds(0, count), :] = term(
                axes_chip(half, 2, second), start, count
            ).astype(BF16)
            for at, length, step in parts(half):
                copies["early", half, turn, step] = wire.send(
                    early_out.at[half, turn, pl.ds(at, length), :],
                    early_in.at[half, turn, pl.ds(at, length), :],
                    HALF_AXES[half][0],
                    step,
                )
    for turn, second in enumerate(FAR_FIRST):
        for half in (0, 1):
            start, count, _ = halves[half]
            for way, (at, length, step) in enumerate(parts(half)):
                near = axes_chip(half, step, second)
                rest_at, rest = (length, count - length) if at == 0 else (0, at)
                late_out[half, turn, way, pl.ds(rest_at, rest), :] = term(
                    near, start + rest_at, rest
                ).astype(BF16)
                copies["early", half, turn, step].wait_recv()
                late_out[half, turn, way, pl.ds(at, length), :] = (
                    term(near, start + at, length)
                    + early_in[half, turn, pl.ds(at, length), :].astype(F32)
                ).astype(BF16)
                copies["late", half, turn, way] = wire.send(
                    late_out.at[half, turn, way, pl.ds(0, count), :],
                    late_in.at[half, turn, way, pl.ds(0, count), :],
                    HALF_AXES[half][0],
                    step,
                )

    def value(turn, half):
        start, count, _ = halves[half]
        result = term(axes_chip(half, 0, FAR_FIRST[turn]), start, count)
        for way in (0, 1):
            copies["late", half, turn, way].wait_recv()
            result += late_in[half, turn, way, pl.ds(0, count), :].astype(F32)
        return result

    return add_up(wire, halves, value, last_out, last_in)


def scatter_buffers(rows, relayed):
    half = halves_of(rows)[0][1]
    first = [(2, RING), (2, RING, 2)] if relayed else [(2, RING, len(STEPS))]
    return [
        pltpu.VMEM((*lead, half, LANES), BF16)
        for lead in (*first, (2, RING))
        for _ in (0, 1)
    ]


def load_feed_forward(place, gate_hbm, up_hbm, down_hbm, wide, down, sems):
    hidden = gate_hbm.shape[0]
    half = wide.shape[0] // 2
    for at, block in enumerate(ORDER):
        columns = pl.ds(pl.multiple_of(block_of(place, *block) * LANES, LANES), LANES)
        here = pl.ds(at * LANES, LANES)
        pltpu.make_async_copy(
            gate_hbm.at[:, columns], wide.at[pl.ds(0, hidden), here], sems.at[0]
        ).start()
        pltpu.make_async_copy(
            up_hbm.at[:, columns], wide.at[pl.ds(half, hidden), here], sems.at[1]
        ).start()
    for at, (along_0, along_1) in enumerate(CHIP_ORDER):
        for other in (0, 1):
            columns = pl.ds(
                pl.multiple_of(block_of(place, along_0, along_1, other) * LANES, LANES), LANES
            )
            pltpu.make_async_copy(
                down_hbm.at[:, columns],
                down.at[at // 2, :, pl.ds((at % 2 * 2 + other) * LANES, LANES)],
                sems.at[2],
            ).start()


def feed_forward(
    place, wire, held, gain, gate_hbm, up_hbm, down_hbm, wide, down, sems, scratch, buffers
):
    scaled, squares, gains, acc, own, pair_out, pair_in = scratch
    hidden, half = (gate_hbm.shape[0], wide.shape[0] // 2)
    rows, width = scaled.shape
    squares[...] = jnp.zeros_like(squares)
    for at, block in enumerate(ORDER):
        gains[pl.ds(at, 1), :] = gain[pl.ds(block_of(place, *block), 1), :]

    def scale(block, carry):
        entry = held[block].astype(F32)
        squares[...] += entry * entry
        scaled[:, pl.ds(pl.multiple_of(block * LANES, LANES), LANES)] = (
            entry * gains[pl.ds(block, 1), :]
        ).astype(BF16)
        return carry

    def ready(group):
        with jax.named_scope("scale_and_product"):
            first = sum(len(blocks) for blocks in GROUPS[:group])
            last = first + len(GROUPS[group])
            lax.fori_loop(first, last, scale, 0)
            if group == 0:
                pltpu.make_async_copy(gate_hbm, wide.at[pl.ds(0, hidden), :], sems.at[0]).wait()
                pltpu.make_async_copy(up_hbm, wide.at[pl.ds(half, hidden), :], sems.at[1]).wait()
            chunk = pl.ds(first * LANES, (last - first) * LANES)
            part = lax.dot_general(
                scaled[:, chunk],
                wide[:, chunk],
                (((1,), (1,)), ((), ())),
                preferred_element_type=F32,
            )
            acc[...] = part if group == 0 else acc[...] + part

    with jax.named_scope("gather_features"):
        gather(wire, held, ready)
    with jax.named_scope("hidden"):
        row_scale = lax.rsqrt(jnp.sum(squares[...], axis=1, keepdims=True) / width + epsilon)
        gate = row_scale * acc[:, :hidden]
        up = row_scale * acc[:, half : half + hidden]
        units = (gate / (1.0 + jnp.exp(-gate)) * up).astype(BF16)
        pltpu.make_async_copy(down, down, sems.at[2]).wait()
    pairs = CHIPS // 2
    first = wire.take(pairs)

    def pair_copy(at):
        part = pl.ds(2 * at, 2)
        return wire.make(pair_out.at[part], pair_in.at[part], "tp", 1, first + at)

    done = [0]

    def project(until):
        with jax.named_scope("down"):
            for at in range(done[0], until):
                result = jnp.dot(units, down[at], preferred_element_type=F32)
                for which in (0, 1):
                    at_lane = 2 * which * LANES
                    own[2 * at + which] = result[:, at_lane : at_lane + LANES]
                    pair_out[2 * at + which] = result[
                        :, at_lane + LANES : at_lane + 2 * LANES
                    ].astype(BF16)
                pair_copy(at).start()
            done[0] = max(done[0], until)

    arrived = set()

    def term(chip, start, count):
        at = POSITION[chip]
        if at // 2 not in arrived:
            arrived.add(at // 2)
            pair_copy(at // 2).wait_recv()
        return own[at, pl.ds(start, count), :] + pair_in[at, pl.ds(start, count), :].astype(F32)

    project(4)
    with jax.named_scope("scatter_features"):
        sums = scatter_direct(
            wire, rows, term, lambda turn: project((5, 8, 8, 8)[turn]), buffers
        )
    wire.sent += [pair_copy(at) for at in range(pairs)]
    return sums


def feed_forward_scratch(rows, width, hidden):
    half = -(-hidden // LANES) * LANES
    return [
        pltpu.VMEM((BLOCKS, rows, LANES), BF16),
        pltpu.VMEM((2 * half, width), BF16),
        pltpu.VMEM((CHIPS // 2, hidden, 4 * LANES), BF16),
        pltpu.SemaphoreType.DMA((10,)),
        pltpu.VMEM((rows, width), BF16),
        pltpu.VMEM((rows, LANES), F32),
        pltpu.VMEM((BLOCKS, LANES), F32),
        pltpu.VMEM((rows, 2 * half), F32),
        pltpu.VMEM((CHIPS, rows, LANES), F32),
        pltpu.VMEM((CHIPS, rows, LANES), BF16),
        pltpu.VMEM((CHIPS, rows, LANES), BF16),
        *scatter_buffers(rows, False),
    ]


def clear_padding(wide, hidden):
    half = wide.shape[0] // 2
    for start in (hidden, half + hidden):
        wide[pl.ds(start, half - hidden), :] = jnp.zeros((half - hidden, wide.shape[1]), BF16)


def first_kernel(
    tokens,
    gate_hbm,
    up_hbm,
    down_hbm,
    first_gain_hbm,
    mix_gain_hbm,
    query_hbm,
    forget_hbm,
    input_hbm,
    outgate_hbm,
    projected,
    mixer_share,
    send_sems,
    recv_sems,
    held,
    wide,
    down,
    sems,
    scaled,
    squares,
    gains,
    acc,
    own,
    pair_out,
    pair_in,
    *rest,
):
    buffers, own_refs, wide_buffers = (rest[:4], rest[4:13], rest[13:])
    low, high, share, ordered, wide_own, wide_out, wide_in, first_gain, mix_gain = own_refs
    place = own_place()
    wire = Wire(place, send_sems, recv_sems)
    own_tokens = pltpu.make_async_copy(tokens, held.at[0], sems.at[3])
    own_tokens.start()
    gain_loads = [
        pltpu.make_async_copy(first_gain_hbm, first_gain, sems.at[8]),
        pltpu.make_async_copy(mix_gain_hbm, mix_gain, sems.at[9]),
    ]
    for load in gain_loads:
        load.start()
    with jax.named_scope("greet"):
        wire.greet(
            lambda: load_feed_forward(place, gate_hbm, up_hbm, down_hbm, wide, down, sems)
        )
    own_tokens.wait()
    width = query_hbm.shape[1]
    loads = [
        pltpu.make_async_copy(source, target.at[:, pl.ds(at, width)], sems.at[4 + index])
        for index, (source, target, at) in enumerate(
            (
                (query_hbm, low, 0),
                (forget_hbm, low, width),
                (input_hbm, high, 0),
                (outgate_hbm, high, width),
            )
        )
    ]
    for load in loads:
        load.start()
    clear_padding(wide, gate_hbm.shape[0])
    for load in gain_loads:
        load.wait()
    sums = feed_forward(
        place,
        wire,
        held,
        first_gain,
        gate_hbm,
        up_hbm,
        down_hbm,
        wide,
        down,
        sems,
        (scaled, squares, gains, acc, own, pair_out, pair_in),
        buffers,
    )
    rows = share.shape[0]
    for (start, count, _), value in zip(halves_of(rows), sums):
        part = pl.ds(start, count)
        mixed = (held[0, part, :].astype(F32) + 0.5 * value).astype(BF16)
        mixer_share[part, :] = mixed
        share[part, :] = mixed.astype(F32)
    seqs = rows // BLOCKS
    for block in range(BLOCKS):
        index = block_of(place, block // (2 * RING), block // 2 % RING, block % 2)
        ordered[pl.ds(block * seqs, seqs), :] = share[
            pl.ds(pl.multiple_of(index * seqs, seqs), seqs), :
        ]
    entry = ordered[...]
    index = block_of(place, 0, 0, 0)
    mix_scaled = (entry * mix_gain[pl.ds(index, 1), :]).astype(BF16)
    square_sum = jnp.broadcast_to(jnp.sum(entry * entry, axis=1, keepdims=True), entry.shape)
    for load in loads:
        load.wait()

    def keep(at, lower, upper):
        pair = jnp.concatenate(
            [lower.reshape(BLOCKS, seqs, LANES), upper.reshape(BLOCKS, seqs, LANES)], axis=1
        ).reshape(RING, RING, 2, 2 * seqs, LANES)
        wide_own[:, :, pl.ds(at, 2 * seqs), :] = pair[:, :, 0]
        wide_out[:, :, pl.ds(at, 2 * seqs), :] = pair[:, :, 1].astype(BF16)

    tile = 2 * seqs
    wide_rows = wide_own.shape[2]
    wide_halves = halves_of(wide_rows)
    columns = low.shape[1] // LANES
    copies = {}

    def project(steps):
        with jax.named_scope("project"):
            for step in steps:
                chunk = slice(2 * step * LANES, 2 * (step + 1) * LANES)
                lower = jnp.dot(mix_scaled, low[:, chunk], preferred_element_type=F32)
                upper = jnp.dot(mix_scaled, high[:, chunk], preferred_element_type=F32)
                for which in (0, 1):
                    lanes = slice(which * LANES, (which + 1) * LANES)
                    keep((2 * step + which) * tile, lower[:, lanes], upper[:, lanes])

    def across(half, first):
        part = pl.ds(*wide_halves[half][:2])
        chips = (slice(None), first) if HALF_AXES[half][0] == "kv_1" else (first, slice(None))
        copies[half, first] = wire.send(
            wide_out.at[(*chips, part, slice(None))],
            wide_in.at[(*chips, part, slice(None))],
            "tp",
            1,
        )

    first_steps = -(-wide_halves[0][1] // (2 * tile))
    project(range(first_steps))
    across(0, 2)
    project(range(first_steps, columns // 2))
    keep(columns * tile, square_sum, jnp.zeros_like(square_sum))
    across(1, 2)
    for first in (1, 3, 0):
        for half in (0, 1):
            across(half, first)
    arrived = set()

    def term(chip, start, count):
        half = 0 if start < wide_halves[1][0] else 1
        first = chip[1] if HALF_AXES[half][0] == "kv_1" else chip[0]
        if (half, first) not in arrived:
            arrived.add((half, first))
            copies[half, first].wait_recv()
        part = pl.ds(start, count)
        return wide_own[(*chip, part)] + wide_in[(*chip, part)].astype(F32)

    with jax.named_scope("scatter_wide"):
        sums = scatter_relayed(wire, wide_rows, term, wide_buffers)
    for (start, count, _), value in zip(halves_of(wide_rows), sums):
        projected[pl.ds(start, count), :] = value
    with jax.named_scope("finish"):
        wire.finish()


def state_kernel(
    full_width, projected, floor_grid, head_gain, state, next_state, mixer_out, held, sems
):
    seqs, heads, keys, values = state.shape
    tile = 2 * seqs
    writes = [
        pltpu.make_async_copy(held.at[head], next_state.at[:, head], sems.at[head])
        for head in range(heads)
    ]
    squares = projected[pl.ds(2 * heads * tile, seqs), :]
    scale = lax.rsqrt(squares / full_width + epsilon)

    def channels(block, second):
        return scale * projected[pl.ds(block * tile + second * seqs, seqs), :]

    row_seq = lax.broadcasted_iota(jnp.int32, (4 * seqs, seqs * values), 0) % seqs
    lane_seq = lax.broadcasted_iota(jnp.int32, (4 * seqs, seqs * values), 1) // values
    spreader = (row_seq == lane_seq).astype(F32).astype(BF16)

    def pieces(entry):
        first = entry.astype(BF16).astype(F32)
        second = (entry - first).astype(BF16).astype(F32)
        third = entry - first - second
        return jnp.concatenate([first, second, third, jnp.zeros_like(entry)], axis=0)

    for head in range(heads):
        query = channels(head, 0)
        entering = channels(head, 1)
        forget_pre = channels(heads + head, 0)
        gate = channels(heads + head, 1)
        floor = floor_grid[pl.ds(head, 1), :]
        forget = floor + (1.0 - floor) / (1.0 + jnp.exp(-forget_pre))
        query = query / (1.0 + jnp.exp(-query))
        both = jnp.concatenate([pieces(forget), pieces(query)], axis=1).T.astype(BF16)
        spread = jnp.dot(both, spreader, preferred_element_type=F32)
        readouts = []
        for seq in range(seqs):
            kept = spread[:keys, seq * values : (seq + 1) * values]
            asked = spread[keys:, seq * values : (seq + 1) * values]
            after = kept * state[seq, head] + (1.0 - kept) * entering[seq : seq + 1, :]
            held[head, seq] = after
            readouts.append(jnp.sum(after * asked, axis=0, keepdims=True))
        writes[head].start()
        readout = jnp.concatenate(readouts, axis=0)
        normed = (
            readout
            * lax.rsqrt(jnp.mean(readout * readout, axis=-1, keepdims=True) + epsilon)
            * head_gain[...]
        )
        half = heads // 2
        row = head % half * tile + head // half * seqs
        mixer_out[pl.ds(row, seqs), :] = normed * (gate / (1.0 + jnp.exp(-gate)))
    for write in writes:
        write.wait()


def second_kernel(
    mixer_out,
    share_hbm,
    output_hbm,
    gate_hbm,
    up_hbm,
    down_hbm,
    gain_hbm,
    layer_out,
    send_sems,
    recv_sems,
    held,
    wide,
    down,
    sems,
    scaled,
    squares,
    gains,
    acc,
    own,
    pair_out,
    pair_in,
    *rest,
):
    buffers, (mixed, output, update, mixer_share, second_gain) = rest[:4], rest[4:]
    place = own_place()
    wire = Wire(place, send_sems, recv_sems)
    depth = output.shape[0]
    loads = [
        pltpu.make_async_copy(
            output_hbm.at[pl.ds(which * depth, depth), :],
            output.at[:, pl.ds(which * LANES, LANES)],
            sems.at[3 + which],
        )
        for which in (0, 1)
    ] + [
        pltpu.make_async_copy(share_hbm, mixer_share, sems.at[5]),
        pltpu.make_async_copy(gain_hbm, second_gain, sems.at[6]),
    ]
    for load in loads:
        load.start()
    mixed[0] = mixer_out[...].astype(BF16)
    with jax.named_scope("greet"):
        wire.greet(
            lambda: load_feed_forward(place, gate_hbm, up_hbm, down_hbm, wide, down, sems)
        )
    clear_padding(wide, gate_hbm.shape[0])
    with jax.named_scope("gather_mixed"):
        gather(wire, mixed)
    for load in loads:
        load.wait()
    rows = update.shape[0]
    seqs = rows // BLOCKS
    tile = 2 * seqs
    total = None
    for step in range(depth // (2 * LANES)):
        pieces = [
            mixed[:, pl.ds((2 * step + which) * tile, tile), :].reshape(
                BLOCKS * tile, LANES
            )
            for which in (0, 1)
        ]
        product = jnp.dot(
            jnp.concatenate(pieces, axis=1),
            output[pl.ds(step * 2 * LANES, 2 * LANES), :],
            preferred_element_type=F32,
        )
        total = product if total is None else total + product
    total = total.reshape(BLOCKS, tile, 2 * LANES)
    total = total[:, :seqs, :LANES] + total[:, seqs:, LANES:]
    for block in range(BLOCKS):
        index = block_of(place, *ORDER[block])
        update[pl.ds(pl.multiple_of(index * seqs, seqs), seqs), :] = total[block]
    held[0] = (mixer_share[...].astype(F32) + update[...]).astype(BF16)
    sums = feed_forward(
        place,
        wire,
        held,
        second_gain,
        gate_hbm,
        up_hbm,
        down_hbm,
        wide,
        down,
        sems,
        (scaled, squares, gains, acc, own, pair_out, pair_in),
        buffers,
    )
    for (start, count, _), value in zip(halves_of(rows), sums):
        part = pl.ds(start, count)
        layer_out[part, :] = (held[0, part, :].astype(F32) + 0.5 * value).astype(BF16)
    with jax.named_scope("finish"):
        wire.finish()


def in_space(*spaces):
    return [pl.BlockSpec(memory_space=space) for space in spaces]


def kernel_params(identity, mebibytes):
    return pltpu.CompilerParams(
        collective_id=identity, has_side_effects=True, vmem_limit_bytes=mebibytes << 20
    )


def per_device(
    tokens,
    carried_state,
    first_gain,
    first_gate,
    first_up,
    first_down,
    mix_gain,
    query_weight,
    forget_weight,
    input_weight,
    outgate_weight,
    forget_floor,
    head_gain,
    output_weight,
    second_gain,
    second_gate,
    second_up,
    second_down,
):
    rows, share = tokens.shape
    full_width, hidden = first_gate.shape
    in_hbm = lambda array: pltpu.with_memory_space_constraint(array, HBM)
    seqs, heads, keys, values = carried_state.shape
    tile = 2 * seqs
    wide_rows = (2 * heads + 1) * tile
    by_block = (full_width // LANES, LANES)
    projected, mixer_share = pl.pallas_call(
        first_kernel,
        name="first_block",
        out_shape=(
            jax.ShapeDtypeStruct((wide_rows, LANES), F32),
            jax.ShapeDtypeStruct((rows, share), BF16),
        ),
        in_specs=in_space(*(HBM,) * 10),
        out_specs=in_space(VMEM, VMEM),
        scratch_shapes=[
            pltpu.SemaphoreType.DMA((192,)),
            pltpu.SemaphoreType.DMA((192,)),
            *feed_forward_scratch(rows, full_width, hidden),
            pltpu.VMEM((share, 2 * heads * keys), BF16),
            pltpu.VMEM((share, 2 * heads * values), BF16),
            pltpu.VMEM((rows, LANES), F32),
            pltpu.VMEM((rows, LANES), F32),
            pltpu.VMEM((RING, RING, wide_rows, LANES), F32),
            pltpu.VMEM((RING, RING, wide_rows, LANES), BF16),
            pltpu.VMEM((RING, RING, wide_rows, LANES), BF16),
            pltpu.VMEM(by_block, F32),
            pltpu.VMEM(by_block, F32),
            *scatter_buffers(wide_rows, True),
        ],
        compiler_params=kernel_params(0, 44),
    )(
        in_hbm(tokens),
        in_hbm(first_gate.T),
        in_hbm(first_up.T),
        in_hbm(first_down),
        in_hbm(first_gain.reshape(by_block)),
        in_hbm(mix_gain.reshape(by_block)),
        in_hbm(query_weight),
        in_hbm(forget_weight),
        in_hbm(input_weight),
        in_hbm(outgate_weight),
    )
    next_state, mixer_out = pl.pallas_call(
        lambda *refs: state_kernel(full_width, *refs),
        name="state_update",
        out_shape=(
            jax.ShapeDtypeStruct(carried_state.shape, F32),
            jax.ShapeDtypeStruct((heads * seqs, values), F32),
        ),
        in_specs=in_space(VMEM, VMEM, VMEM, VMEM),
        out_specs=in_space(HBM, VMEM),
        scratch_shapes=[
            pltpu.VMEM((heads, seqs, keys, values), F32),
            pltpu.SemaphoreType.DMA((heads,)),
        ],
        compiler_params=pltpu.CompilerParams(vmem_limit_bytes=12 << 20),
    )(
        projected,
        forget_floor.reshape(heads, keys),
        head_gain.reshape(1, values),
        carried_state,
    )
    layer_out = pl.pallas_call(
        second_kernel,
        name="second_block",
        out_shape=jax.ShapeDtypeStruct((rows, share), BF16),
        in_specs=in_space(VMEM, *(HBM,) * 6),
        out_specs=pl.BlockSpec(memory_space=VMEM),
        scratch_shapes=[
            pltpu.SemaphoreType.DMA((224,)),
            pltpu.SemaphoreType.DMA((224,)),
            *feed_forward_scratch(rows, full_width, hidden),
            pltpu.VMEM((BLOCKS, heads * seqs, LANES), BF16),
            pltpu.VMEM((heads * values // 2, 2 * LANES), BF16),
            pltpu.VMEM((rows, LANES), F32),
            pltpu.VMEM((rows, LANES), BF16),
            pltpu.VMEM(by_block, F32),
        ],
        compiler_params=kernel_params(1, 32),
    )(
        mixer_out,
        mixer_share,
        in_hbm(output_weight),
        in_hbm(second_gate.T),
        in_hbm(second_up.T),
        in_hbm(second_down),
        in_hbm(second_gain.reshape(by_block)),
    )
    return (layer_out, next_state)


def solution(mesh):
    split = Mesh(
        mesh.devices.reshape(mesh.shape["dp"], RING, RING, mesh.shape["tp"]), DP_KV_TP
    )
    return jax.shard_map(
        per_device,
        mesh=split,
        in_specs=(
            P("dp", KV_TP),
            P(DP_KV_TP, None, None, None),
            P(),
            P(None, KV_TP),
            P(None, KV_TP),
            P(KV_TP, None),
            P(),
            P(KV_TP, None),
            P(KV_TP, None),
            P(KV_TP, None),
            P(KV_TP, None),
            P(),
            P(),
            P(None, KV_TP),
            P(),
            P(None, KV_TP),
            P(None, KV_TP),
            P(KV_TP, None),
        ),
        out_specs=(P("dp", KV_TP), P(DP_KV_TP, None, None, None)),
        check_vma=False,
    )
```

```python
import jax
import jax.numpy as jnp
from jax import lax
from jax.experimental import pallas as pl
from jax.experimental.pallas import tpu as pltpu
from jax.sharding import Mesh
from jax.sharding import PartitionSpec as P

KV_TP = ("kv_0", "kv_1", "tp")
DP_KV_TP = ("dp", "kv_0", "kv_1", "tp")
MESH = pl.DeviceIdType.MESH
HBM = pltpu.MemorySpace.HBM
VMEM = pltpu.MemorySpace.VMEM
F32 = jnp.float32
BF16 = jnp.bfloat16

epsilon = 1e-06
RING = 4
LANES = 128
CHIPS = RING * RING
WIDE_PIECES = 4
BLOCKS = 2 * CHIPS
NEAR = (
    *((axis, step, 0) for axis in ("kv_0", "kv_1") for step in (2, 1, 3)),
    ("tp", 1, 0),
)
HALF_AXES = (("kv_1", "kv_0"), ("kv_0", "kv_1"))
FAR_FIRST = (2, 1, 3, 0)
NEAR_FIRST = (1, 3, 2)
STEPS = (2, 1, 3)
IN_LINE = ((0, 0),) + tuple((0, a) for a in NEAR_FIRST) + tuple((a, 0) for a in NEAR_FIRST)
EARLY = tuple((a, b) for a in (1, 3) for b in (1, 3))
LATE = tuple((a, 2) for a in (1, 3)) + tuple((2, a) for a in NEAR_FIRST)
GROUPS = (
    tuple((*chip, core) for core in (0, 1) for chip in IN_LINE),
    *(tuple((*chip, core) for chip in chips) for chips in (EARLY, LATE) for core in (0, 1)),
)
ORDER = sum(GROUPS, ())
KEPT_AT = {block: at for at, block in enumerate(ORDER)}
FIRST_CHIPS = tuple(
    chip
    for turn in FAR_FIRST
    for step in STEPS
    for chip in ((step, turn), (turn, step))
)
CHIP_ORDER = tuple(dict.fromkeys(FIRST_CHIPS)) + ((0, 0),)
POSITION = {chip: place for place, chip in enumerate(CHIP_ORDER)}


def crosses(chip):
    return 0


def own_place():
    return (lax.axis_index("kv_0"), lax.axis_index("kv_1"), lax.axis_index("tp"))


def block_of(place, along_0, along_1, other_core):
    at_0, at_1, core = place
    return (
        lax.rem(at_0 + along_0, RING) * (2 * RING)
        + lax.rem(at_1 + along_1, RING) * 2
        + lax.rem(core + other_core, 2)
    )


class Wire:
    def __init__(self, place, send_sems, recv_sems):
        at_0, at_1, core = place
        self.place = {"kv_0": (at_0, RING), "kv_1": (at_1, RING), "tp": (core, 2)}
        self.send_sems, self.recv_sems = send_sems, recv_sems
        self.used = 0
        self.sent = []

    def near(self, axis, step, cross):
        at, size = self.place[axis]
        there = {axis: lax.rem(at + step, size)}
        if cross:
            there["tp"] = 1 - self.place["tp"][0]
        return there

    def greet(self, meanwhile):
        barrier = pltpu.get_barrier_semaphore()
        for axis, step, cross in NEAR:
            pl.semaphore_signal(
                barrier, inc=1, device_id=self.near(axis, step, cross), device_id_type=MESH
            )
        meanwhile()
        pl.semaphore_wait(barrier, len(NEAR))

    def take(self, count):
        first = self.used
        self.used += count
        return first

    def make(self, source, target, axis, step, slot, cross=0):
        return pltpu.make_async_remote_copy(
            src_ref=source,
            dst_ref=target,
            send_sem=self.send_sems.at[slot],
            recv_sem=self.recv_sems.at[slot],
            device_id=self.near(axis, step, cross),
            device_id_type=MESH,
        )

    def send(self, source, target, axis, step, cross=None):
        cross = 0
        copy = self.make(source, target, axis, step, self.take(1), cross)
        copy.start()
        self.sent.append(copy)
        return copy

    def finish(self, count=None):
        for copy in self.sent[:count]:
            copy.wait_send()
        self.sent = self.sent[count:] if count is not None else []


def pieces_of(rows, number=2):
    tiles = rows // 16
    ends = [-(-tiles * piece // number) * 16 for piece in range(number + 1)]
    return tuple((a, b - a, (b - a) // 32 * 16) for a, b in zip(ends, ends[1:]))


def axes_of(piece):
    return HALF_AXES[piece % 2]


def axes_chip(half, first, second):
    return (second, first) if axes_of(half)[0] == "kv_1" else (first, second)


def gather(wire, held, ready, eager, started=lambda: None):
    halves = pieces_of(held.shape[1])
    copies = {}

    def view(half, first, second, core):
        start, rows, _ = halves[half]
        chip = axes_chip(half, first, second)
        return held.at[KEPT_AT[(*chip, core)], pl.ds(start, rows), :]

    def spread(half, stage, first, steps=STEPS):
        for step in steps:
            there = RING - step
            chip = (there, 0) if stage == 0 else (first, there)
            source = (0, 0) if stage == 0 else (first, 0)
            copies[half, stage, first, there] = wire.send(
                view(half, *source, crosses(source)),
                view(half, *chip, crosses(chip)),
                axes_of(half)[stage],
                step,
            )

    def across(half, first, second):
        core = crosses((first, second))
        copies[half, "across", first, second] = wire.send(
            view(half, first, second, core), view(half, first, second, 1 - core), "tp", 1
        )

    def arrive(half, stage, first, there):
        copies[half, stage, first, there].wait_recv()

    both = (0, 1)
    for half in both:
        spread(half, 0, 0, NEAR_FIRST)
    for half in both:
        spread(half, 1, 0)
    for half in both:
        across(half, 0, 0)
    started()
    for there in NEAR_FIRST:
        for half in both:
            arrive(half, 0, 0, there)
            spread(half, 1, there)
            across(half, there, 0)
    for there in NEAR_FIRST:
        for half in both:
            arrive(half, 1, 0, there)
            across(half, 0, there)

    def settle(chips):
        for half in both:
            for chip in chips:
                first, second = chip[::-1] if axes_of(half)[0] == "kv_1" else chip
                arrive(half, "across", first, second)

    def pass_on(firsts, theres):
        for first in firsts:
            for there in theres:
                for half in both:
                    arrive(half, 1, first, there)
                    across(half, first, there)

    if eager:
        settle(IN_LINE)
        ready(0)
    pass_on((1, 3), (1, 3))
    if eager:
        ready(1)
    pass_on((1, 3), (2,))
    pass_on((2,), (1, 3, 2))
    if not eager:
        settle(IN_LINE)
        ready(0)
        ready(1)
    settle(EARLY)
    ready(2)
    ready(3)
    settle(LATE)
    ready(4)


def add_up(wire, halves, value, last_out, last_in):
    copies = {}
    sums = [None] * len(halves)
    for turn, second in enumerate(FAR_FIRST):
        for half in range(len(halves)):
            count = halves[half][1]
            result = value(turn, half)
            if second == 0:
                sums[half] = result
                continue
            last_out[half, turn, pl.ds(0, count), :] = result.astype(BF16)
            copies[half, turn] = wire.send(
                last_out.at[half, turn, pl.ds(0, count), :],
                last_in.at[half, turn, pl.ds(0, count), :],
                axes_of(half)[1],
                second,
            )
    for turn in (1, 2, 0):
        for half in range(len(halves)):
            copies[half, turn].wait_recv()
            sums[half] += last_in[half, turn, pl.ds(0, halves[half][1]), :].astype(F32)
    return sums


def scatter_direct(wire, rows, term, between, buffers):
    halves = pieces_of(rows)
    early_out, early_in, last_out, last_in = buffers
    copies = {}
    keep = len(wire.sent)
    for turn, second in enumerate(FAR_FIRST):
        for way, step in enumerate(STEPS):
            for half in (0, 1):
                start, count, _ = halves[half]
                early_out[half, turn, way, pl.ds(0, count), :] = term(
                    axes_chip(half, step, second), start, count
                ).astype(BF16)
                copies[half, turn, way] = wire.send(
                    early_out.at[half, turn, way, pl.ds(0, count), :],
                    early_in.at[half, turn, way, pl.ds(0, count), :],
                    axes_of(half)[0],
                    step,
                )
        between(turn)

    wire.finish(keep)

    def value(turn, half):
        start, count, _ = halves[half]
        result = term(axes_chip(half, 0, FAR_FIRST[turn]), start, count)
        for way in range(len(STEPS)):
            copies[half, turn, way].wait_recv()
            result += early_in[half, turn, way, pl.ds(0, count), :].astype(F32)
        return result

    return add_up(wire, halves, value, last_out, last_in)


def scatter_relayed(wire, halves, term, before, buffers):
    early_out, early_in, late_out, late_in, last_out, last_in = buffers
    copies = {}
    keep = len(wire.sent)

    def parts(half):
        _, count, cut = halves[half]
        return ((0, cut, 1), (cut, count - cut, 3))

    for half in range(len(halves)):
        before(half)
        for turn, second in enumerate(FAR_FIRST):
            start, count, _ = halves[half]
            early_out[half, turn, pl.ds(0, count), :] = term(
                axes_chip(half, 2, second), start, count
            ).astype(BF16)
            for at, length, step in parts(half):
                copies["early", half, turn, step] = wire.send(
                    early_out.at[half, turn, pl.ds(at, length), :],
                    early_in.at[half, turn, pl.ds(at, length), :],
                    axes_of(half)[0],
                    step,
                    cross=False,
                )
    wire.finish(keep)
    for turn, second in enumerate(FAR_FIRST):
        for half in range(len(halves)):
            start, count, _ = halves[half]
            for way, (at, length, step) in enumerate(parts(half)):
                near = axes_chip(half, step, second)
                rest_at, rest = (length, count - length) if at == 0 else (0, at)
                late_out[half, turn, way, pl.ds(rest_at, rest), :] = term(
                    near, start + rest_at, rest
                ).astype(BF16)
                copies["early", half, turn, step].wait_recv()
                late_out[half, turn, way, pl.ds(at, length), :] = (
                    term(near, start + at, length)
                    + early_in[half, turn, pl.ds(at, length), :].astype(F32)
                ).astype(BF16)
                copies["late", half, turn, way] = wire.send(
                    late_out.at[half, turn, way, pl.ds(0, count), :],
                    late_in.at[half, turn, way, pl.ds(0, count), :],
                    axes_of(half)[0],
                    step,
                )

    def value(turn, half):
        start, count, _ = halves[half]
        result = term(axes_chip(half, 0, FAR_FIRST[turn]), start, count)
        for way in (0, 1):
            copies["late", half, turn, way].wait_recv()
            result += late_in[half, turn, way, pl.ds(0, count), :].astype(F32)
        return result

    return add_up(wire, halves, value, last_out, last_in)


def scatter_buffers(pieces, relayed):
    number, half = len(pieces), pieces[0][1]
    first = [(RING,), (RING, 2)] if relayed else [(RING, len(STEPS))]
    return [
        pltpu.VMEM((number, *lead, half, LANES), BF16)
        for lead in (*first, (RING,))
        for _ in (0, 1)
    ]


def load_feed_forward(place, gate_hbm, up_hbm, down_hbm, wide, down, sems):
    hidden = gate_hbm.shape[0]
    half = wide.shape[0] // 2
    for at, block in enumerate(ORDER):
        columns = pl.ds(pl.multiple_of(block_of(place, *block) * LANES, LANES), LANES)
        here = pl.ds(at * LANES, LANES)
        pltpu.make_async_copy(
            gate_hbm.at[:, columns], wide.at[pl.ds(0, hidden), here], sems.at[0]
        ).start()
        pltpu.make_async_copy(
            up_hbm.at[:, columns], wide.at[pl.ds(half, hidden), here], sems.at[1]
        ).start()
    for at, chip in enumerate(CHIP_ORDER):
        pltpu.make_async_copy(
            down_hbm.at[:, columns_of(place, chip, 0)],
            down.at[pl.ds(0, hidden), pl.ds(at * LANES, LANES)],
            sems.at[2],
        ).start()


def columns_of(place, chip, core):
    return pl.ds(pl.multiple_of(block_of(place, *chip, core) * LANES, LANES), LANES)


def feed_forward(
    place,
    wire,
    held,
    gain,
    gate_hbm,
    up_hbm,
    down_hbm,
    wide,
    down,
    sems,
    scratch,
    buffers,
    after_swap=lambda: None,
):
    scaled, squares, gains, acc, own, units = scratch
    hidden, half = (gate_hbm.shape[0], wide.shape[0] // 2)
    rows, width = scaled.shape
    squares[...] = jnp.zeros_like(squares)
    for at, block in enumerate(ORDER):
        gains[pl.ds(at, 1), :] = gain[pl.ds(block_of(place, *block), 1), :]

    def scale(block, carry):
        entry = held[block].astype(F32)
        scaled[:, pl.ds(pl.multiple_of(block * LANES, LANES), LANES)] = (
            entry * gains[pl.ds(block, 1), :]
        ).astype(BF16)
        return carry + entry * entry

    def ready(group):
        with jax.named_scope("scale_and_product"):
            first = sum(len(blocks) for blocks in GROUPS[:group])
            last = first + len(GROUPS[group])
            squares[...] = lax.fori_loop(first, last, scale, squares[...])
            if group == 0:
                pltpu.make_async_copy(gate_hbm, wide.at[pl.ds(0, hidden), :], sems.at[0]).wait()
                pltpu.make_async_copy(up_hbm, wide.at[pl.ds(half, hidden), :], sems.at[1]).wait()
            chunk = pl.ds(first * LANES, (last - first) * LANES)
            part = lax.dot_general(
                scaled[:, chunk],
                wide[:, chunk],
                (((1,), (1,)), ((), ())),
                preferred_element_type=F32,
            )
            acc[...] = part if group == 0 else acc[...] + part

    def started():
        for at, chip in enumerate(CHIP_ORDER):
            down_copies.append(
                wire.send(
                    down_hbm.at[:, columns_of(place, chip, 1)],
                    down.at[pl.ds(half, hidden), pl.ds(at * LANES, LANES)],
                    "tp",
                    1,
                )
            )

    down_copies = []
    with jax.named_scope("gather_features"):
        gather(wire, held, ready, True, started)
    with jax.named_scope("hidden"):
        row_scale = lax.rsqrt(jnp.sum(squares[...], axis=1, keepdims=True) / width + epsilon)
        gate = row_scale * acc[:, :half]
        up = row_scale * acc[:, half:]
        units[:, pl.ds(0, half)] = (gate / (1.0 + jnp.exp(-gate)) * up).astype(BF16)
        swap = wire.send(
            units.at[:, pl.ds(0, half)], units.at[:, pl.ds(half, half)], "tp", 1
        )
        after_swap()
        arrived = down.at[pl.ds(0, hidden), :]
        pltpu.make_async_copy(arrived, arrived, sems.at[2]).wait()

    def product(first, last, begin, count):
        chips = pl.ds(first * LANES, (last - first) * LANES)
        return jnp.dot(
            units[:, pl.ds(begin, count)],
            down[pl.ds(begin, count), chips],
            preferred_element_type=F32,
        )

    def project(first, last):
        with jax.named_scope("down"):
            result = product(first, last, 0, 2 * half)
            for at in range(first, last):
                own[at] = result[:, (at - first) * LANES : (at - first + 1) * LANES]

    ends = (5, 9, 13, CHIPS)
    with jax.named_scope("down_first"):
        kept = product(0, ends[0], 0, half)
        for at in range(ends[0]):
            own[at] = kept[:, at * LANES : (at + 1) * LANES]
        for copy in down_copies:
            copy.wait_recv()
        swap.wait_recv()
        kept = product(0, ends[0], half, half)
        for at in range(ends[0]):
            own[at] += kept[:, at * LANES : (at + 1) * LANES]

    def term(chip, start, count):
        return own[POSITION[chip], pl.ds(start, count), :]

    def between(turn):
        if turn == 0:
            project(ends[0], ends[1])
        elif turn == 1:
            project(ends[1], ends[2])
            project(ends[2], ends[3])

    with jax.named_scope("scatter_features"):
        sums = scatter_direct(wire, rows, term, between, buffers)
    return sums


def feed_forward_scratch(rows, width, hidden):
    half = -(-hidden // LANES) * LANES
    return [
        pltpu.VMEM((BLOCKS, rows, LANES), BF16),
        pltpu.VMEM((2 * half, width), BF16),
        pltpu.VMEM((2 * half, CHIPS * LANES), BF16),
        pltpu.SemaphoreType.DMA((10,)),
        pltpu.VMEM((rows, width), BF16),
        pltpu.VMEM((rows, LANES), F32),
        pltpu.VMEM((BLOCKS, LANES), F32),
        pltpu.VMEM((rows, 2 * half), F32),
        pltpu.VMEM((CHIPS, rows, LANES), F32),
        pltpu.VMEM((rows, 2 * half), BF16),
        *scatter_buffers(pieces_of(rows), False),
    ]


def clear_padding(wide, down, hidden):
    half = wide.shape[0] // 2
    for array in (wide, down):
        for start in (hidden, half + hidden):
            rest = pl.ds(start, half - hidden)
            array[rest, :] = jnp.zeros((half - hidden, array.shape[1]), BF16)


def first_kernel(
    tokens,
    gate_hbm,
    up_hbm,
    down_hbm,
    first_gain_hbm,
    mix_gain_hbm,
    query_hbm,
    forget_hbm,
    input_hbm,
    outgate_hbm,
    projected,
    mixer_share,
    send_sems,
    recv_sems,
    held,
    wide,
    down,
    sems,
    scaled,
    squares,
    gains,
    acc,
    own,
    units,
    *rest,
):
    buffers, own_refs, wide_buffers = (rest[:4], rest[4:13], rest[13:])
    low, high, share, ordered, rows_out, rows_in, wide_own, first_gain, mix_gain = own_refs
    place = own_place()
    wire = Wire(place, send_sems, recv_sems)
    own_tokens = pltpu.make_async_copy(tokens, held.at[0], sems.at[3])
    own_tokens.start()
    gain_loads = [
        pltpu.make_async_copy(first_gain_hbm, first_gain, sems.at[8]),
        pltpu.make_async_copy(mix_gain_hbm, mix_gain, sems.at[9]),
    ]
    for load in gain_loads:
        load.start()
    with jax.named_scope("greet"):
        wire.greet(
            lambda: load_feed_forward(place, gate_hbm, up_hbm, down_hbm, wide, down, sems)
        )
    own_tokens.wait()
    share_width, width = query_hbm.shape
    weights = (
        (query_hbm, low, 0),
        (forget_hbm, low, width),
        (input_hbm, high, 0),
        (outgate_hbm, high, width),
    )
    loads = [
        pltpu.make_async_copy(
            source, target.at[pl.ds(0, share_width), pl.ds(at, width)], sems.at[4 + index]
        )
        for index, (source, target, at) in enumerate(weights)
    ]
    weight_copies = []

    def share_weights():
        for source, target, at in weights:
            there = target.at[pl.ds(share_width, share_width), pl.ds(at, width)]
            weight_copies.append(wire.send(source, there, "tp", 1))

    for load in loads:
        load.start()
    clear_padding(wide, down, gate_hbm.shape[0])
    for load in gain_loads:
        load.wait()
    sums = feed_forward(
        place,
        wire,
        held,
        first_gain,
        gate_hbm,
        up_hbm,
        down_hbm,
        wide,
        down,
        sems,
        (scaled, squares, gains, acc, own, units),
        buffers,
        share_weights,
    )
    rows = share.shape[0]
    for (start, count, _), value in zip(pieces_of(rows), sums):
        part = pl.ds(start, count)
        mixed = (held[0, part, :].astype(F32) + 0.5 * value).astype(BF16)
        mixer_share[part, :] = mixed
        share[part, :] = mixed.astype(F32)
    seqs = rows // BLOCKS
    for block in range(BLOCKS):
        chip = (block // RING % RING, block % RING)
        index = block_of(place, *chip, block // CHIPS)
        ordered[pl.ds(block * seqs, seqs), :] = share[
            pl.ds(pl.multiple_of(index * seqs, seqs), seqs), :
        ]
    side = rows // 2
    rows_out[...] = ordered[pl.ds(side, side), :].astype(BF16)
    swap = wire.send(rows_out, rows_in, "tp", 1)
    for load in loads:
        load.wait()
    for copy in weight_copies:
        copy.wait_recv()
    swap.wait_recv()
    entries = (ordered[pl.ds(0, side), :], rows_in[...].astype(F32))
    mix_scaled = jnp.concatenate(
        [
            entry * mix_gain[pl.ds(block_of(place, 0, 0, core), 1), :]
            for core, entry in enumerate(entries)
        ],
        axis=1,
    ).astype(BF16)
    square_sum = sum(jnp.sum(entry * entry, axis=1, keepdims=True) for entry in entries)
    square_sum = jnp.broadcast_to(square_sum, entries[0].shape)

    def keep(at, lower, upper):
        both = [part.reshape(RING, RING, seqs, LANES) for part in (lower, upper)]
        wide_own[:, :, pl.ds(at, 2 * seqs), :] = jnp.concatenate(both, axis=2)

    tile = 2 * seqs
    wide_rows = wide_own.shape[2]
    wide_halves = pieces_of(wide_rows, WIDE_PIECES)
    columns = low.shape[1] // LANES

    def project(steps):
        with jax.named_scope("project"):
            for step in steps:
                chunk = slice(2 * step * LANES, 2 * (step + 1) * LANES)
                lower = jnp.dot(mix_scaled, low[:, chunk], preferred_element_type=F32)
                upper = jnp.dot(mix_scaled, high[:, chunk], preferred_element_type=F32)
                for which in (0, 1):
                    lanes = slice(which * LANES, (which + 1) * LANES)
                    keep((2 * step + which) * tile, lower[:, lanes], upper[:, lanes])

    ends = [
        min(-(-(start + count) // (2 * tile)), columns // 2) for start, count, _ in wide_halves
    ]

    def before(piece):
        project(range(ends[piece - 1] if piece else 0, ends[piece]))
        if piece + 1 == len(wide_halves):
            keep(columns * tile, square_sum, jnp.zeros_like(square_sum))

    def term(chip, start, count):
        return wide_own[(*chip, pl.ds(start, count))]

    with jax.named_scope("scatter_wide"):
        sums = scatter_relayed(wire, wide_halves, term, before, wide_buffers)
    for (start, count, _), value in zip(wide_halves, sums):
        projected[pl.ds(start, count), :] = value
    with jax.named_scope("finish"):
        wire.finish()


def state_kernel(
    full_width, projected, floor_grid, head_gain, state, next_state, mixer_out, held, sems
):
    seqs, heads, keys, values = state.shape
    tile = 2 * seqs
    writes = [
        pltpu.make_async_copy(held.at[head], next_state.at[:, head], sems.at[head])
        for head in range(heads)
    ]
    squares = projected[pl.ds(2 * heads * tile, seqs), :]
    scale = lax.rsqrt(squares / full_width + epsilon)

    def channels(block, second):
        return scale * projected[pl.ds(block * tile + second * seqs, seqs), :]

    row_seq = lax.broadcasted_iota(jnp.int32, (4 * seqs, seqs * values), 0) % seqs
    lane_seq = lax.broadcasted_iota(jnp.int32, (4 * seqs, seqs * values), 1) // values
    spreader = (row_seq == lane_seq).astype(F32).astype(BF16)

    def pieces(entry):
        first = entry.astype(BF16).astype(F32)
        second = (entry - first).astype(BF16).astype(F32)
        third = entry - first - second
        return jnp.concatenate([first, second, third, jnp.zeros_like(entry)], axis=0)

    for head in range(heads):
        query = channels(head, 0)
        entering = channels(head, 1)
        forget_pre = channels(heads + head, 0)
        gate = channels(heads + head, 1)
        floor = floor_grid[pl.ds(head, 1), :]
        forget = floor + (1.0 - floor) / (1.0 + jnp.exp(-forget_pre))
        query = query / (1.0 + jnp.exp(-query))
        both = jnp.concatenate([pieces(forget), pieces(query)], axis=1).T.astype(BF16)
        spread = jnp.dot(both, spreader, preferred_element_type=F32)
        readouts = []
        for seq in range(seqs):
            kept = spread[:keys, seq * values : (seq + 1) * values]
            asked = spread[keys:, seq * values : (seq + 1) * values]
            fresh = entering[seq : seq + 1, :]
            after = fresh + kept * (state[seq, head] - fresh)
            held[head, seq] = after
            readouts.append(jnp.sum(after * asked, axis=0, keepdims=True))
        writes[head].start()
        readout = jnp.concatenate(readouts, axis=0)
        normed = (
            readout
            * lax.rsqrt(jnp.mean(readout * readout, axis=-1, keepdims=True) + epsilon)
            * head_gain[...]
        )
        half = heads // 2
        row = head % half * tile + head // half * seqs
        mixer_out[pl.ds(row, seqs), :] = normed * (gate / (1.0 + jnp.exp(-gate)))
    for write in writes:
        write.wait()


def second_kernel(
    mixer_out,
    share_hbm,
    output_hbm,
    gate_hbm,
    up_hbm,
    down_hbm,
    gain_hbm,
    layer_out,
    send_sems,
    recv_sems,
    held,
    wide,
    down,
    sems,
    scaled,
    squares,
    gains,
    acc,
    own,
    units,
    *rest,
):
    buffers, (mixed, output, update, mixer_share, second_gain) = rest[:4], rest[4:]
    place = own_place()
    wire = Wire(place, send_sems, recv_sems)
    depth = output.shape[0]
    loads = [
        pltpu.make_async_copy(
            output_hbm.at[pl.ds(which * depth, depth), :],
            output.at[:, pl.ds(which * LANES, LANES)],
            sems.at[3 + which],
        )
        for which in (0, 1)
    ] + [
        pltpu.make_async_copy(share_hbm, mixer_share, sems.at[5]),
        pltpu.make_async_copy(gain_hbm, second_gain, sems.at[6]),
    ]
    for load in loads:
        load.start()
    mixed[0] = mixer_out[...].astype(BF16)
    with jax.named_scope("greet"):
        wire.greet(
            lambda: load_feed_forward(place, gate_hbm, up_hbm, down_hbm, wide, down, sems)
        )
    clear_padding(wide, down, gate_hbm.shape[0])
    rows = update.shape[0]
    seqs = rows // BLOCKS
    tile = 2 * seqs

    def project(group):
        with jax.named_scope("output"):
            if group == 0:
                for load in loads:
                    load.wait()
            first = sum(len(blocks) for blocks in GROUPS[:group])
            number = len(GROUPS[group])
            total = None
            for step in range(depth // (2 * LANES)):
                pieces = [
                    mixed[
                        pl.ds(first, number), pl.ds((2 * step + which) * tile, tile), :
                    ].reshape(number * tile, LANES)
                    for which in (0, 1)
                ]
                product = jnp.dot(
                    jnp.concatenate(pieces, axis=1),
                    output[pl.ds(step * 2 * LANES, 2 * LANES), :],
                    preferred_element_type=F32,
                )
                total = product if total is None else total + product
            total = total.reshape(number, tile, 2 * LANES)
            total = total[:, :seqs, :LANES] + total[:, seqs:, LANES:]
            for at, block in enumerate(GROUPS[group]):
                index = block_of(place, *block)
                update[pl.ds(pl.multiple_of(index * seqs, seqs), seqs), :] = total[at]

    with jax.named_scope("gather_mixed"):
        gather(wire, mixed, project, False)
    held[0] = (mixer_share[...].astype(F32) + update[...]).astype(BF16)
    sums = feed_forward(
        place,
        wire,
        held,
        second_gain,
        gate_hbm,
        up_hbm,
        down_hbm,
        wide,
        down,
        sems,
        (scaled, squares, gains, acc, own, units),
        buffers,
    )
    for (start, count, _), value in zip(pieces_of(rows), sums):
        part = pl.ds(start, count)
        layer_out[part, :] = (held[0, part, :].astype(F32) + 0.5 * value).astype(BF16)
    with jax.named_scope("finish"):
        wire.finish()


def in_space(*spaces):
    return [pl.BlockSpec(memory_space=space) for space in spaces]


def kernel_params(identity, mebibytes):
    return pltpu.CompilerParams(
        collective_id=identity, has_side_effects=True, vmem_limit_bytes=mebibytes << 20
    )


def per_device(
    tokens,
    carried_state,
    first_gain,
    first_gate,
    first_up,
    first_down,
    mix_gain,
    query_weight,
    forget_weight,
    input_weight,
    outgate_weight,
    forget_floor,
    head_gain,
    output_weight,
    second_gain,
    second_gate,
    second_up,
    second_down,
):
    rows, share = tokens.shape
    full_width, hidden = first_gate.shape
    in_hbm = lambda array: pltpu.with_memory_space_constraint(array, HBM)
    seqs, heads, keys, values = carried_state.shape
    tile = 2 * seqs
    wide_rows = (2 * heads + 1) * tile
    by_block = (full_width // LANES, LANES)
    projected, mixer_share = pl.pallas_call(
        first_kernel,
        name="first_block",
        out_shape=(
            jax.ShapeDtypeStruct((wide_rows, LANES), F32),
            jax.ShapeDtypeStruct((rows, share), BF16),
        ),
        in_specs=in_space(*(HBM,) * 10),
        out_specs=in_space(VMEM, VMEM),
        scratch_shapes=[
            pltpu.SemaphoreType.DMA((208,)),
            pltpu.SemaphoreType.DMA((208,)),
            *feed_forward_scratch(rows, full_width, hidden),
            pltpu.VMEM((2 * share, 2 * heads * keys), BF16),
            pltpu.VMEM((2 * share, 2 * heads * values), BF16),
            pltpu.VMEM((rows, LANES), F32),
            pltpu.VMEM((rows, LANES), F32),
            pltpu.VMEM((rows // 2, LANES), BF16),
            pltpu.VMEM((rows // 2, LANES), BF16),
            pltpu.VMEM((RING, RING, wide_rows, LANES), F32),
            pltpu.VMEM(by_block, F32),
            pltpu.VMEM(by_block, F32),
            *scatter_buffers(pieces_of(wide_rows, WIDE_PIECES), True),
        ],
        compiler_params=kernel_params(0, 44),
    )(
        in_hbm(tokens),
        in_hbm(first_gate.T),
        in_hbm(first_up.T),
        in_hbm(first_down),
        in_hbm(first_gain.reshape(by_block)),
        in_hbm(mix_gain.reshape(by_block)),
        in_hbm(query_weight),
        in_hbm(forget_weight),
        in_hbm(input_weight),
        in_hbm(outgate_weight),
    )
    next_state, mixer_out = pl.pallas_call(
        lambda *refs: state_kernel(full_width, *refs),
        name="state_update",
        out_shape=(
            jax.ShapeDtypeStruct(carried_state.shape, F32),
            jax.ShapeDtypeStruct((heads * seqs, values), F32),
        ),
        in_specs=in_space(VMEM, VMEM, VMEM, VMEM),
        out_specs=in_space(HBM, VMEM),
        scratch_shapes=[
            pltpu.VMEM((heads, seqs, keys, values), F32),
            pltpu.SemaphoreType.DMA((heads,)),
        ],
        compiler_params=pltpu.CompilerParams(vmem_limit_bytes=12 << 20),
    )(
        projected,
        forget_floor.reshape(heads, keys),
        head_gain.reshape(1, values),
        carried_state,
    )
    layer_out = pl.pallas_call(
        second_kernel,
        name="second_block",
        out_shape=jax.ShapeDtypeStruct((rows, share), BF16),
        in_specs=in_space(VMEM, *(HBM,) * 6),
        out_specs=pl.BlockSpec(memory_space=VMEM),
        scratch_shapes=[
            pltpu.SemaphoreType.DMA((176,)),
            pltpu.SemaphoreType.DMA((176,)),
            *feed_forward_scratch(rows, full_width, hidden),
            pltpu.VMEM((BLOCKS, heads * seqs, LANES), BF16),
            pltpu.VMEM((heads * values // 2, 2 * LANES), BF16),
            pltpu.VMEM((rows, LANES), F32),
            pltpu.VMEM((rows, LANES), BF16),
            pltpu.VMEM(by_block, F32),
        ],
        compiler_params=kernel_params(1, 32),
    )(
        mixer_out,
        mixer_share,
        in_hbm(output_weight),
        in_hbm(second_gate.T),
        in_hbm(second_up.T),
        in_hbm(second_down),
        in_hbm(second_gain.reshape(by_block)),
    )
    return (layer_out, next_state)


def solution(mesh):
    split = Mesh(
        mesh.devices.reshape(mesh.shape["dp"], RING, RING, mesh.shape["tp"]), DP_KV_TP
    )
    return jax.shard_map(
        per_device,
        mesh=split,
        in_specs=(
            P("dp", KV_TP),
            P(DP_KV_TP, None, None, None),
            P(),
            P(None, KV_TP),
            P(None, KV_TP),
            P(KV_TP, None),
            P(),
            P(KV_TP, None),
            P(KV_TP, None),
            P(KV_TP, None),
            P(KV_TP, None),
            P(),
            P(),
            P(None, KV_TP),
            P(),
            P(None, KV_TP),
            P(None, KV_TP),
            P(KV_TP, None),
        ),
        out_specs=(P("dp", KV_TP), P(DP_KV_TP, None, None, None)),
        check_vma=False,
    )
```

```python
import jax
import jax.numpy as jnp
from jax import lax
from jax.experimental import pallas as pl
from jax.experimental.pallas import tpu as pltpu
from jax.sharding import Mesh
from jax.sharding import PartitionSpec as P

KV_TP = ("kv_0", "kv_1", "tp")
DP_KV_TP = ("dp", "kv_0", "kv_1", "tp")
MESH = pl.DeviceIdType.MESH
HBM = pltpu.MemorySpace.HBM
VMEM = pltpu.MemorySpace.VMEM
F32 = jnp.float32
BF16 = jnp.bfloat16

epsilon = 1e-06
RING = 4
LANES = 128
CHIPS = RING * RING
WIDE_PIECES = 4
BLOCKS = 2 * CHIPS
NEAR = tuple((axis, step) for axis in ("kv_0", "kv_1") for step in (2, 1, 3)) + (("tp", 1),)
HALF_AXES = (("kv_1", "kv_0"), ("kv_0", "kv_1"))
FAR_FIRST = (2, 1, 3, 0)
NEAR_FIRST = (1, 3, 2)
STEPS = (2, 1, 3)
IN_LINE = ((0, 0),) + tuple((0, a) for a in NEAR_FIRST) + tuple((a, 0) for a in NEAR_FIRST)
EARLY = tuple((a, b) for a in (1, 3) for b in (1, 3))
LATE = tuple((a, 2) for a in (1, 3)) + tuple((2, a) for a in NEAR_FIRST)
GROUPS = (
    tuple((*chip, core) for core in (0, 1) for chip in IN_LINE),
    *(tuple((*chip, core) for chip in chips) for chips in (EARLY, LATE) for core in (0, 1)),
)
ORDER = sum(GROUPS, ())
KEPT_AT = {block: at for at, block in enumerate(ORDER)}
FIRST_CHIPS = tuple(
    chip
    for turn in FAR_FIRST
    for step in STEPS
    for chip in ((step, turn), (turn, step))
)
CHIP_ORDER = tuple(dict.fromkeys(FIRST_CHIPS)) + ((0, 0),)
POSITION = {chip: place for place, chip in enumerate(CHIP_ORDER)}


def own_place():
    return (lax.axis_index("kv_0"), lax.axis_index("kv_1"), lax.axis_index("tp"))


def block_of(place, along_0, along_1, other_core):
    at_0, at_1, core = place
    return (
        lax.rem(at_0 + along_0, RING) * (2 * RING)
        + lax.rem(at_1 + along_1, RING) * 2
        + lax.rem(core + other_core, 2)
    )


class Wire:
    def __init__(self, place, send_sems, recv_sems):
        at_0, at_1, core = place
        self.core = core
        self.place = {"kv_0": (at_0, RING), "kv_1": (at_1, RING), "tp": (core, 2)}
        self.send_sems, self.recv_sems = send_sems, recv_sems
        self.sends = self.receives = 0
        self.owed = []

    def near(self, axis, step):
        at, size = self.place[axis]
        return {axis: lax.rem(at + step, size)}

    def greet(self, meanwhile):
        barrier = pltpu.get_barrier_semaphore()
        for axis, step in NEAR:
            pl.semaphore_signal(
                barrier, inc=1, device_id=self.near(axis, step), device_id_type=MESH
            )
        meanwhile()
        pl.semaphore_wait(barrier, len(NEAR))

    def sender(self, ref):
        self.sends += 1
        self.owed.append((self.sends - 1, ref))
        return self.sends - 1

    def receiver(self):
        self.receives += 1
        return self.receives - 1

    def prepare(self, source, target, axis, step, send, receive):
        return pltpu.make_async_remote_copy(
            src_ref=source,
            dst_ref=target,
            send_sem=self.send_sems.at[send],
            recv_sem=self.recv_sems.at[receive],
            device_id=self.near(axis, step),
            device_id_type=MESH,
        )

    def send(self, source, target, axis, step, send=None, receive=None):
        send = self.sender(source) if send is None else send
        receive = self.receiver() if receive is None else receive
        copy = self.prepare(source, target, axis, step, send, receive)
        copy.start()
        return copy

    def receive(self, receive, ref):
        pltpu.make_async_copy(ref, ref, self.recv_sems.at[receive]).wait()

    def finish(self, count=None):
        for send, ref in self.owed[:count]:
            pltpu.make_async_copy(ref, ref, self.send_sems.at[send]).wait()
        self.owed = self.owed[count:] if count is not None else []


def pieces_of(rows, number=2):
    tiles = rows // 16
    ends = [-(-tiles * piece // number) * 16 for piece in range(number + 1)]
    return tuple((a, b - a, (b - a) // 32 * 16) for a, b in zip(ends, ends[1:]))


def axes_of(piece):
    return HALF_AXES[piece % 2]


def axes_chip(half, first, second):
    return (second, first) if axes_of(half)[0] == "kv_1" else (first, second)


def gather(wire, held, ready, eager, started=lambda: None):
    halves = pieces_of(held.shape[1])
    copies = {}
    send = wire.sender(held.at[pl.ds(0, BLOCKS - 1)])
    crossing = {chips: wire.receiver() for chips in (IN_LINE, EARLY, LATE)}

    def view(half, first, second, core):
        start, rows, _ = halves[half]
        chip = axes_chip(half, first, second)
        return held.at[KEPT_AT[(*chip, core)], pl.ds(start, rows), :]

    def spread(half, stage, first, steps=STEPS):
        for step in steps:
            there = RING - step
            chip = (there, 0) if stage == 0 else (first, there)
            source = (0, 0) if stage == 0 else (first, 0)
            copies[half, stage, first, there] = wire.send(
                view(half, *source, 0),
                view(half, *chip, 0),
                axes_of(half)[stage],
                step,
                send,
            )

    def crossed(half, first, second):
        chip = axes_chip(half, first, second)
        group = next(chips for chips in crossing if chip in chips)
        source, target = (view(half, first, second, core) for core in (0, 1))
        return wire.prepare(source, target, "tp", 1, send, crossing[group])

    def across(half, first, second):
        crossed(half, first, second).start()

    def arrive(half, stage, first, there):
        copies[half, stage, first, there].wait_recv()

    both = (0, 1)
    for half in both:
        spread(half, 0, 0, NEAR_FIRST)
    for half in both:
        spread(half, 1, 0)
    for half in both:
        across(half, 0, 0)
    started()
    for there in NEAR_FIRST:
        for half in both:
            arrive(half, 0, 0, there)
            spread(half, 1, there)
            across(half, there, 0)
    for there in NEAR_FIRST:
        for half in both:
            arrive(half, 1, 0, there)
            across(half, 0, there)

    def settle(chips):
        blocks = held.at[pl.ds(KEPT_AT[(*chips[0], 1)], len(chips))]
        wire.receive(crossing[chips], blocks)

    aside = [
        (half, first, there)
        for firsts, theres in (((1, 3), (1, 3)), ((1, 3), (2,)), ((2,), NEAR_FIRST))
        for first in firsts
        for there in theres
        for half in both
    ]
    for half, first, there in aside:
        copies[half, "across", first, there] = crossed(half, first, there)
    early, late = aside[:8], aside[8:]

    def pass_on(blocks):
        for half, first, there in blocks:
            arrive(half, 1, first, there)
            copies[half, "across", first, there].start()

    if eager:
        @pl.when(wire.core == 1)
        def _():
            pass_on(early)

        settle(IN_LINE)
        ready(0)

        @pl.when(wire.core == 1)
        def _():
            pass_on(late)

        @pl.when(wire.core == 0)
        def _():
            pass_on(early)

        ready(1)
        settle(EARLY)
        ready(2)

        @pl.when(wire.core == 0)
        def _():
            pass_on(late)

    else:
        pass_on(early + late)
        settle(IN_LINE)
        ready(0)
        ready(1)
        settle(EARLY)
        ready(2)
    ready(3)
    settle(LATE)
    ready(4)


def add_up(wire, halves, value, last_out, last_in):
    sums = [None] * len(halves)
    rows = [pl.ds(0, count) for _, count, _ in halves]
    sends = [wire.sender(last_out.at[half, pl.ds(0, 3), part]) for half, part in enumerate(rows)]
    receives = [wire.receiver() for _ in halves]
    for turn, second in enumerate(FAR_FIRST):
        for half in range(len(halves)):
            count = halves[half][1]
            result = value(turn, half)
            if second == 0:
                sums[half] = result
                continue
            last_out[half, turn, pl.ds(0, count), :] = result.astype(BF16)
            wire.send(
                last_out.at[half, turn, pl.ds(0, count), :],
                last_in.at[half, turn, pl.ds(0, count), :],
                axes_of(half)[1],
                second,
                sends[half],
                receives[half],
            )
    for half, part in enumerate(rows):
        wire.receive(receives[half], last_in.at[half, pl.ds(0, 3), part])
        for turn in (1, 2, 0):
            sums[half] += last_in[half, turn, pl.ds(0, halves[half][1]), :].astype(F32)
    return sums


def scatter_direct(wire, rows, term, between, buffers):
    halves = pieces_of(rows)
    early_out, early_in, last_out, last_in = buffers
    keep = len(wire.owed)
    rows = [pl.ds(0, count) for _, count, _ in halves]
    sends = [wire.sender(early_out.at[half, :, :, part]) for half, part in enumerate(rows)]
    receives = [[wire.receiver() for _ in FAR_FIRST] for _ in halves]
    for turn, second in enumerate(FAR_FIRST):
        for way, step in enumerate(STEPS):
            for half in (0, 1):
                start, count, _ = halves[half]
                early_out[half, turn, way, pl.ds(0, count), :] = term(
                    axes_chip(half, step, second), start, count
                ).astype(BF16)
                wire.send(
                    early_out.at[half, turn, way, pl.ds(0, count), :],
                    early_in.at[half, turn, way, pl.ds(0, count), :],
                    axes_of(half)[0],
                    step,
                    sends[half],
                    receives[half][turn],
                )
        between(turn)

    wire.finish(keep)

    def value(turn, half):
        start, count, _ = halves[half]
        result = term(axes_chip(half, 0, FAR_FIRST[turn]), start, count)
        wire.receive(receives[half][turn], early_in.at[half, turn, :, rows[half]])
        for way in range(len(STEPS)):
            result += early_in[half, turn, way, pl.ds(0, count), :].astype(F32)
        return result

    return add_up(wire, halves, value, last_out, last_in)


def scatter_relayed(wire, halves, term, before, buffers):
    early_out, early_in, late_out, late_in, last_out, last_in = buffers
    keep = len(wire.owed)
    rows = [pl.ds(0, count) for _, count, _ in halves]
    early_sends = [wire.sender(early_out.at[half, :, part]) for half, part in enumerate(rows)]
    late_sends = [wire.sender(late_out.at[half, :, :, part]) for half, part in enumerate(rows)]
    early_receives, late_receives = (
        [[wire.receiver() for _ in FAR_FIRST] for _ in halves] for _ in (0, 1)
    )

    def parts(half):
        _, count, cut = halves[half]
        return ((0, cut, 1), (cut, count - cut, 3))

    for half in range(len(halves)):
        before(half)
        for turn, second in enumerate(FAR_FIRST):
            start, count, _ = halves[half]
            early_out[half, turn, pl.ds(0, count), :] = term(
                axes_chip(half, 2, second), start, count
            ).astype(BF16)
            for at, length, step in parts(half):
                wire.send(
                    early_out.at[half, turn, pl.ds(at, length), :],
                    early_in.at[half, turn, pl.ds(at, length), :],
                    axes_of(half)[0],
                    step,
                    early_sends[half],
                    early_receives[half][turn],
                )
    wire.finish(keep)
    for turn, second in enumerate(FAR_FIRST):
        for half in range(len(halves)):
            start, count, _ = halves[half]
            wire.receive(early_receives[half][turn], early_in.at[half, turn, rows[half]])
            for way, (at, length, step) in enumerate(parts(half)):
                near = axes_chip(half, step, second)
                rest_at, rest = (length, count - length) if at == 0 else (0, at)
                late_out[half, turn, way, pl.ds(rest_at, rest), :] = term(
                    near, start + rest_at, rest
                ).astype(BF16)
                late_out[half, turn, way, pl.ds(at, length), :] = (
                    term(near, start + at, length)
                    + early_in[half, turn, pl.ds(at, length), :].astype(F32)
                ).astype(BF16)
                wire.send(
                    late_out.at[half, turn, way, pl.ds(0, count), :],
                    late_in.at[half, turn, way, pl.ds(0, count), :],
                    axes_of(half)[0],
                    step,
                    late_sends[half],
                    late_receives[half][turn],
                )

    def value(turn, half):
        start, count, _ = halves[half]
        result = term(axes_chip(half, 0, FAR_FIRST[turn]), start, count)
        wire.receive(late_receives[half][turn], late_in.at[half, turn, :, rows[half]])
        for way in (0, 1):
            result += late_in[half, turn, way, pl.ds(0, count), :].astype(F32)
        return result

    return add_up(wire, halves, value, last_out, last_in)


def scatter_buffers(pieces, relayed):
    number, half = len(pieces), pieces[0][1]
    first = [(RING,), (RING, 2)] if relayed else [(RING, len(STEPS))]
    return [
        pltpu.VMEM((number, *lead, half, LANES), BF16)
        for lead in (*first, (RING,))
        for _ in (0, 1)
    ]


def load_feed_forward(place, gate_hbm, up_hbm, down_hbm, wide, down, sems):
    hidden = gate_hbm.shape[0]
    half = wide.shape[0] // 2
    for at, block in enumerate(ORDER):
        columns = pl.ds(pl.multiple_of(block_of(place, *block) * LANES, LANES), LANES)
        here = pl.ds(at * LANES, LANES)
        pltpu.make_async_copy(
            gate_hbm.at[:, columns], wide.at[pl.ds(0, hidden), here], sems.at[0]
        ).start()
        pltpu.make_async_copy(
            up_hbm.at[:, columns], wide.at[pl.ds(half, hidden), here], sems.at[1]
        ).start()
    for at, chip in enumerate(CHIP_ORDER):
        pltpu.make_async_copy(
            down_hbm.at[:, columns_of(place, chip, 0)],
            down.at[pl.ds(0, hidden), pl.ds(at * LANES, LANES)],
            sems.at[2],
        ).start()


def columns_of(place, chip, core):
    return pl.ds(pl.multiple_of(block_of(place, *chip, core) * LANES, LANES), LANES)


def feed_forward(
    place,
    wire,
    held,
    gain,
    gate_hbm,
    up_hbm,
    down_hbm,
    wide,
    down,
    sems,
    scratch,
    buffers,
    after_swap=lambda: None,
):
    scaled, squares, gains, acc, own, units = scratch
    hidden, half = (gate_hbm.shape[0], wide.shape[0] // 2)
    rows, width = scaled.shape
    squares[...] = jnp.zeros_like(squares)
    for at, block in enumerate(ORDER):
        gains[pl.ds(at, 1), :] = gain[pl.ds(block_of(place, *block), 1), :]

    def scale(block, carry):
        entry = held[block].astype(F32)
        scaled[:, pl.ds(pl.multiple_of(block * LANES, LANES), LANES)] = (
            entry * gains[pl.ds(block, 1), :]
        ).astype(BF16)
        return carry + entry * entry

    def ready(group):
        with jax.named_scope("scale_and_product"):
            first = sum(len(blocks) for blocks in GROUPS[:group])
            last = first + len(GROUPS[group])
            squares[...] = lax.fori_loop(first, last, scale, squares[...])
            if group == 0:
                pltpu.make_async_copy(gate_hbm, wide.at[pl.ds(0, hidden), :], sems.at[0]).wait()
                pltpu.make_async_copy(up_hbm, wide.at[pl.ds(half, hidden), :], sems.at[1]).wait()
            chunk = pl.ds(first * LANES, (last - first) * LANES)
            part = lax.dot_general(
                scaled[:, chunk],
                wide[:, chunk],
                (((1,), (1,)), ((), ())),
                preferred_element_type=F32,
            )
            acc[...] = part if group == 0 else acc[...] + part

    def started():
        send = wire.sender(others)
        for at, chip in enumerate(CHIP_ORDER):
            wire.send(
                down_hbm.at[:, columns_of(place, chip, 1)],
                down.at[pl.ds(half, hidden), pl.ds(at * LANES, LANES)],
                "tp",
                1,
                send,
                others_receive,
            )

    others, others_receive = down.at[pl.ds(half, hidden), :], wire.receiver()
    with jax.named_scope("gather_features"):
        gather(wire, held, ready, True, started)
    with jax.named_scope("hidden"):
        row_scale = lax.rsqrt(jnp.sum(squares[...], axis=1, keepdims=True) / width + epsilon)
        gate = row_scale * acc[:, :half]
        up = row_scale * acc[:, half:]
        units[:, pl.ds(0, half)] = (gate / (1.0 + jnp.exp(-gate)) * up).astype(BF16)
        swap = wire.send(
            units.at[:, pl.ds(0, half)], units.at[:, pl.ds(half, half)], "tp", 1
        )
        after_swap()
        arrived = down.at[pl.ds(0, hidden), :]
        pltpu.make_async_copy(arrived, arrived, sems.at[2]).wait()

    def product(first, last, begin, count):
        chips = pl.ds(first * LANES, (last - first) * LANES)
        return jnp.dot(
            units[:, pl.ds(begin, count)],
            down[pl.ds(begin, count), chips],
            preferred_element_type=F32,
        )

    def project(first, last):
        with jax.named_scope("down"):
            result = product(first, last, 0, 2 * half)
            for at in range(first, last):
                own[at] = result[:, (at - first) * LANES : (at - first + 1) * LANES]

    ends = (5, 9, 13, CHIPS)
    with jax.named_scope("down_first"):
        kept = product(0, ends[0], 0, half)
        for at in range(ends[0]):
            own[at] = kept[:, at * LANES : (at + 1) * LANES]
        wire.receive(others_receive, others)
        swap.wait_recv()
        kept = product(0, ends[0], half, half)
        for at in range(ends[0]):
            own[at] += kept[:, at * LANES : (at + 1) * LANES]

    def term(chip, start, count):
        return own[POSITION[chip], pl.ds(start, count), :]

    def between(turn):
        if turn == 0:
            project(ends[0], ends[1])
        elif turn == 1:
            project(ends[1], ends[2])
            project(ends[2], ends[3])

    with jax.named_scope("scatter_features"):
        sums = scatter_direct(wire, rows, term, between, buffers)
    return sums


def feed_forward_scratch(rows, width, hidden):
    half = -(-hidden // LANES) * LANES
    return [
        pltpu.VMEM((BLOCKS, rows, LANES), BF16),
        pltpu.VMEM((2 * half, width), BF16),
        pltpu.VMEM((2 * half, CHIPS * LANES), BF16),
        pltpu.SemaphoreType.DMA((10,)),
        pltpu.VMEM((rows, width), BF16),
        pltpu.VMEM((rows, LANES), F32),
        pltpu.VMEM((BLOCKS, LANES), F32),
        pltpu.VMEM((rows, 2 * half), F32),
        pltpu.VMEM((CHIPS, rows, LANES), F32),
        pltpu.VMEM((rows, 2 * half), BF16),
        *scatter_buffers(pieces_of(rows), False),
    ]


def clear_padding(wide, down, hidden):
    half = wide.shape[0] // 2
    for array in (wide, down):
        for start in (hidden, half + hidden):
            rest = pl.ds(start, half - hidden)
            array[rest, :] = jnp.zeros((half - hidden, array.shape[1]), BF16)


def first_kernel(
    tokens,
    gate_hbm,
    up_hbm,
    down_hbm,
    first_gain_hbm,
    mix_gain_hbm,
    query_hbm,
    forget_hbm,
    input_hbm,
    outgate_hbm,
    projected,
    mixer_share,
    send_sems,
    recv_sems,
    held,
    wide,
    down,
    sems,
    scaled,
    squares,
    gains,
    acc,
    own,
    units,
    *rest,
):
    buffers, own_refs, wide_buffers = (rest[:4], rest[4:13], rest[13:])
    low, high, share, ordered, rows_out, rows_in, wide_own, first_gain, mix_gain = own_refs
    place = own_place()
    wire = Wire(place, send_sems, recv_sems)
    own_tokens = pltpu.make_async_copy(tokens, held.at[0], sems.at[3])
    own_tokens.start()
    gain_loads = [
        pltpu.make_async_copy(first_gain_hbm, first_gain, sems.at[8]),
        pltpu.make_async_copy(mix_gain_hbm, mix_gain, sems.at[9]),
    ]
    for load in gain_loads:
        load.start()
    with jax.named_scope("greet"):
        wire.greet(
            lambda: load_feed_forward(place, gate_hbm, up_hbm, down_hbm, wide, down, sems)
        )
    own_tokens.wait()
    share_width, width = query_hbm.shape
    weights = (
        (query_hbm, low, 0),
        (forget_hbm, low, width),
        (input_hbm, high, 0),
        (outgate_hbm, high, width),
    )
    loads = [
        pltpu.make_async_copy(
            source, target.at[pl.ds(0, share_width), pl.ds(at, width)], sems.at[4 + index]
        )
        for index, (source, target, at) in enumerate(weights)
    ]
    weight_copies = []

    def share_weights():
        send = wire.sender(low)
        for source, target, at in weights:
            there = target.at[pl.ds(share_width, share_width), pl.ds(at, width)]
            weight_copies.append(wire.send(source, there, "tp", 1, send))

    for load in loads:
        load.start()
    clear_padding(wide, down, gate_hbm.shape[0])
    for load in gain_loads:
        load.wait()
    sums = feed_forward(
        place,
        wire,
        held,
        first_gain,
        gate_hbm,
        up_hbm,
        down_hbm,
        wide,
        down,
        sems,
        (scaled, squares, gains, acc, own, units),
        buffers,
        share_weights,
    )
    rows = share.shape[0]
    for (start, count, _), value in zip(pieces_of(rows), sums):
        part = pl.ds(start, count)
        mixed = (held[0, part, :].astype(F32) + 0.5 * value).astype(BF16)
        mixer_share[part, :] = mixed
        share[part, :] = mixed.astype(F32)
    seqs = rows // BLOCKS
    for block in range(BLOCKS):
        chip = (block // RING % RING, block % RING)
        index = block_of(place, *chip, block // CHIPS)
        ordered[pl.ds(block * seqs, seqs), :] = share[
            pl.ds(pl.multiple_of(index * seqs, seqs), seqs), :
        ]
    side = rows // 2
    rows_out[...] = ordered[pl.ds(side, side), :].astype(BF16)
    swap = wire.send(rows_out, rows_in, "tp", 1)
    for load in loads:
        load.wait()
    for copy in weight_copies:
        copy.wait_recv()
    swap.wait_recv()
    entries = (ordered[pl.ds(0, side), :], rows_in[...].astype(F32))
    mix_scaled = jnp.concatenate(
        [
            entry * mix_gain[pl.ds(block_of(place, 0, 0, core), 1), :]
            for core, entry in enumerate(entries)
        ],
        axis=1,
    ).astype(BF16)
    square_sum = sum(jnp.sum(entry * entry, axis=1, keepdims=True) for entry in entries)
    square_sum = jnp.broadcast_to(square_sum, entries[0].shape)

    def keep(at, lower, upper):
        both = [part.reshape(RING, RING, seqs, LANES) for part in (lower, upper)]
        wide_own[:, :, pl.ds(at, 2 * seqs), :] = jnp.concatenate(both, axis=2)

    tile = 2 * seqs
    wide_rows = wide_own.shape[2]
    wide_halves = pieces_of(wide_rows, WIDE_PIECES)
    columns = low.shape[1] // LANES

    def project(steps):
        with jax.named_scope("project"):
            for step in steps:
                chunk = slice(2 * step * LANES, 2 * (step + 1) * LANES)
                lower = jnp.dot(mix_scaled, low[:, chunk], preferred_element_type=F32)
                upper = jnp.dot(mix_scaled, high[:, chunk], preferred_element_type=F32)
                for which in (0, 1):
                    lanes = slice(which * LANES, (which + 1) * LANES)
                    keep((2 * step + which) * tile, lower[:, lanes], upper[:, lanes])

    ends = [
        min(-(-(start + count) // (2 * tile)), columns // 2) for start, count, _ in wide_halves
    ]

    def before(piece):
        project(range(ends[piece - 1] if piece else 0, ends[piece]))
        if piece + 1 == len(wide_halves):
            keep(columns * tile, square_sum, jnp.zeros_like(square_sum))

    def term(chip, start, count):
        return wide_own[(*chip, pl.ds(start, count))]

    with jax.named_scope("scatter_wide"):
        sums = scatter_relayed(wire, wide_halves, term, before, wide_buffers)
    for (start, count, _), value in zip(wide_halves, sums):
        projected[pl.ds(start, count), :] = value
    with jax.named_scope("finish"):
        wire.finish()
    assert (wire.sends, wire.receives) == (send_sems.shape[0], recv_sems.shape[0]), (wire.sends, wire.receives)


def state_kernel(
    full_width, projected, floor_grid, head_gain, state, next_state, mixer_out, held, sems
):
    seqs, heads, keys, values = state.shape
    tile = 2 * seqs
    writes = [
        pltpu.make_async_copy(held.at[head], next_state.at[:, head], sems.at[head])
        for head in range(heads)
    ]
    squares = projected[pl.ds(2 * heads * tile, seqs), :]
    scale = lax.rsqrt(squares / full_width + epsilon)

    def channels(block, second):
        return scale * projected[pl.ds(block * tile + second * seqs, seqs), :]

    row_seq = lax.broadcasted_iota(jnp.int32, (4 * seqs, seqs * values), 0) % seqs
    lane_seq = lax.broadcasted_iota(jnp.int32, (4 * seqs, seqs * values), 1) // values
    spreader = (row_seq == lane_seq).astype(F32).astype(BF16)

    def pieces(entry):
        first = entry.astype(BF16).astype(F32)
        second = (entry - first).astype(BF16).astype(F32)
        third = entry - first - second
        return jnp.concatenate([first, second, third, jnp.zeros_like(entry)], axis=0)

    for head in range(heads):
        query = channels(head, 0)
        entering = channels(head, 1)
        forget_pre = channels(heads + head, 0)
        gate = channels(heads + head, 1)
        floor = floor_grid[pl.ds(head, 1), :]
        forget = floor + (1.0 - floor) / (1.0 + jnp.exp(-forget_pre))
        query = query / (1.0 + jnp.exp(-query))
        both = jnp.concatenate([pieces(forget), pieces(query)], axis=1).T.astype(BF16)
        spread = jnp.dot(both, spreader, preferred_element_type=F32)
        readouts = []
        for seq in range(seqs):
            kept = spread[:keys, seq * values : (seq + 1) * values]
            asked = spread[keys:, seq * values : (seq + 1) * values]
            fresh = entering[seq : seq + 1, :]
            after = fresh + kept * (state[seq, head] - fresh)
            held[head, seq] = after
            readouts.append(jnp.sum(after * asked, axis=0, keepdims=True))
        writes[head].start()
        readout = jnp.concatenate(readouts, axis=0)
        normed = (
            readout
            * lax.rsqrt(jnp.mean(readout * readout, axis=-1, keepdims=True) + epsilon)
            * head_gain[...]
        )
        half = heads // 2
        row = head % half * tile + head // half * seqs
        mixer_out[pl.ds(row, seqs), :] = normed * (gate / (1.0 + jnp.exp(-gate)))
    for write in writes:
        write.wait()


def second_kernel(
    mixer_out,
    share_hbm,
    output_hbm,
    gate_hbm,
    up_hbm,
    down_hbm,
    gain_hbm,
    layer_out,
    send_sems,
    recv_sems,
    held,
    wide,
    down,
    sems,
    scaled,
    squares,
    gains,
    acc,
    own,
    units,
    *rest,
):
    buffers, (mixed, output, update, mixer_share, second_gain) = rest[:4], rest[4:]
    place = own_place()
    wire = Wire(place, send_sems, recv_sems)
    depth = output.shape[0]
    loads = [
        pltpu.make_async_copy(
            output_hbm.at[pl.ds(which * depth, depth), :],
            output.at[:, pl.ds(which * LANES, LANES)],
            sems.at[3 + which],
        )
        for which in (0, 1)
    ] + [
        pltpu.make_async_copy(share_hbm, mixer_share, sems.at[5]),
        pltpu.make_async_copy(gain_hbm, second_gain, sems.at[6]),
    ]
    for load in loads:
        load.start()
    mixed[0] = mixer_out[...].astype(BF16)
    with jax.named_scope("greet"):
        wire.greet(
            lambda: load_feed_forward(place, gate_hbm, up_hbm, down_hbm, wide, down, sems)
        )
    clear_padding(wide, down, gate_hbm.shape[0])
    rows = update.shape[0]
    seqs = rows // BLOCKS
    tile = 2 * seqs

    def project(group):
        with jax.named_scope("output"):
            if group == 0:
                for load in loads:
                    load.wait()
            first = sum(len(blocks) for blocks in GROUPS[:group])
            number = len(GROUPS[group])
            total = None
            for step in range(depth // (2 * LANES)):
                pieces = [
                    mixed[
                        pl.ds(first, number), pl.ds((2 * step + which) * tile, tile), :
                    ].reshape(number * tile, LANES)
                    for which in (0, 1)
                ]
                product = jnp.dot(
                    jnp.concatenate(pieces, axis=1),
                    output[pl.ds(step * 2 * LANES, 2 * LANES), :],
                    preferred_element_type=F32,
                )
                total = product if total is None else total + product
            total = total.reshape(number, tile, 2 * LANES)
            total = total[:, :seqs, :LANES] + total[:, seqs:, LANES:]
            for at, block in enumerate(GROUPS[group]):
                index = block_of(place, *block)
                update[pl.ds(pl.multiple_of(index * seqs, seqs), seqs), :] = total[at]

    with jax.named_scope("gather_mixed"):
        gather(wire, mixed, project, False)
    held[0] = (mixer_share[...].astype(F32) + update[...]).astype(BF16)
    sums = feed_forward(
        place,
        wire,
        held,
        second_gain,
        gate_hbm,
        up_hbm,
        down_hbm,
        wide,
        down,
        sems,
        (scaled, squares, gains, acc, own, units),
        buffers,
    )
    for (start, count, _), value in zip(pieces_of(rows), sums):
        part = pl.ds(start, count)
        layer_out[part, :] = (held[0, part, :].astype(F32) + 0.5 * value).astype(BF16)
    with jax.named_scope("finish"):
        wire.finish()
    assert (wire.sends, wire.receives) == (send_sems.shape[0], recv_sems.shape[0]), (wire.sends, wire.receives)


def in_space(*spaces):
    return [pl.BlockSpec(memory_space=space) for space in spaces]


def kernel_params(identity, mebibytes):
    return pltpu.CompilerParams(
        collective_id=identity, has_side_effects=True, vmem_limit_bytes=mebibytes << 20
    )


def per_device(
    tokens,
    carried_state,
    first_gain,
    first_gate,
    first_up,
    first_down,
    mix_gain,
    query_weight,
    forget_weight,
    input_weight,
    outgate_weight,
    forget_floor,
    head_gain,
    output_weight,
    second_gain,
    second_gate,
    second_up,
    second_down,
):
    rows, share = tokens.shape
    full_width, hidden = first_gate.shape
    in_hbm = lambda array: pltpu.with_memory_space_constraint(array, HBM)
    seqs, heads, keys, values = carried_state.shape
    tile = 2 * seqs
    wide_rows = (2 * heads + 1) * tile
    by_block = (full_width // LANES, LANES)
    projected, mixer_share = pl.pallas_call(
        first_kernel,
        name="first_block",
        out_shape=(
            jax.ShapeDtypeStruct((wide_rows, LANES), F32),
            jax.ShapeDtypeStruct((rows, share), BF16),
        ),
        in_specs=in_space(*(HBM,) * 10),
        out_specs=in_space(VMEM, VMEM),
        scratch_shapes=[
            pltpu.SemaphoreType.DMA((21,)),
            pltpu.SemaphoreType.DMA((86,)),
            *feed_forward_scratch(rows, full_width, hidden),
            pltpu.VMEM((2 * share, 2 * heads * keys), BF16),
            pltpu.VMEM((2 * share, 2 * heads * values), BF16),
            pltpu.VMEM((rows, LANES), F32),
            pltpu.VMEM((rows, LANES), F32),
            pltpu.VMEM((rows // 2, LANES), BF16),
            pltpu.VMEM((rows // 2, LANES), BF16),
            pltpu.VMEM((RING, RING, wide_rows, LANES), F32),
            pltpu.VMEM(by_block, F32),
            pltpu.VMEM(by_block, F32),
            *scatter_buffers(pieces_of(wide_rows, WIDE_PIECES), True),
        ],
        compiler_params=kernel_params(0, 44),
    )(
        in_hbm(tokens),
        in_hbm(first_gate.T),
        in_hbm(first_up.T),
        in_hbm(first_down),
        in_hbm(first_gain.reshape(by_block)),
        in_hbm(mix_gain.reshape(by_block)),
        in_hbm(query_weight),
        in_hbm(forget_weight),
        in_hbm(input_weight),
        in_hbm(outgate_weight),
    )
    next_state, mixer_out = pl.pallas_call(
        lambda *refs: state_kernel(full_width, *refs),
        name="state_update",
        out_shape=(
            jax.ShapeDtypeStruct(carried_state.shape, F32),
            jax.ShapeDtypeStruct((heads * seqs, values), F32),
        ),
        in_specs=in_space(VMEM, VMEM, VMEM, VMEM),
        out_specs=in_space(HBM, VMEM),
        scratch_shapes=[
            pltpu.VMEM((heads, seqs, keys, values), F32),
            pltpu.SemaphoreType.DMA((heads,)),
        ],
        compiler_params=pltpu.CompilerParams(vmem_limit_bytes=12 << 20),
    )(
        projected,
        forget_floor.reshape(heads, keys),
        head_gain.reshape(1, values),
        carried_state,
    )
    layer_out = pl.pallas_call(
        second_kernel,
        name="second_block",
        out_shape=jax.ShapeDtypeStruct((rows, share), BF16),
        in_specs=in_space(VMEM, *(HBM,) * 6),
        out_specs=pl.BlockSpec(memory_space=VMEM),
        scratch_shapes=[
            pltpu.SemaphoreType.DMA((8,)),
            pltpu.SemaphoreType.DMA((78,)),
            *feed_forward_scratch(rows, full_width, hidden),
            pltpu.VMEM((BLOCKS, heads * seqs, LANES), BF16),
            pltpu.VMEM((heads * values // 2, 2 * LANES), BF16),
            pltpu.VMEM((rows, LANES), F32),
            pltpu.VMEM((rows, LANES), BF16),
            pltpu.VMEM(by_block, F32),
        ],
        compiler_params=kernel_params(1, 32),
    )(
        mixer_out,
        mixer_share,
        in_hbm(output_weight),
        in_hbm(second_gate.T),
        in_hbm(second_up.T),
        in_hbm(second_down),
        in_hbm(second_gain.reshape(by_block)),
    )
    return (layer_out, next_state)


def solution(mesh):
    split = Mesh(
        mesh.devices.reshape(mesh.shape["dp"], RING, RING, mesh.shape["tp"]), DP_KV_TP
    )
    return jax.shard_map(
        per_device,
        mesh=split,
        in_specs=(
            P("dp", KV_TP),
            P(DP_KV_TP, None, None, None),
            P(),
            P(None, KV_TP),
            P(None, KV_TP),
            P(KV_TP, None),
            P(),
            P(KV_TP, None),
            P(KV_TP, None),
            P(KV_TP, None),
            P(KV_TP, None),
            P(),
            P(),
            P(None, KV_TP),
            P(),
            P(None, KV_TP),
            P(None, KV_TP),
            P(KV_TP, None),
        ),
        out_specs=(P("dp", KV_TP), P(DP_KV_TP, None, None, None)),
        check_vma=False,
    )
```

```python
import jax
import jax.numpy as jnp
from jax import lax
from jax.experimental import pallas as pl
from jax.experimental.pallas import tpu as pltpu
from jax.sharding import Mesh
from jax.sharding import PartitionSpec as P

KV_TP = ("kv_0", "kv_1", "tp")
DP_KV_TP = ("dp", "kv_0", "kv_1", "tp")
MESH = pl.DeviceIdType.MESH
HBM = pltpu.MemorySpace.HBM
VMEM = pltpu.MemorySpace.VMEM
F32 = jnp.float32
BF16 = jnp.bfloat16

epsilon = 1e-06
RING = 4
LANES = 128
CHIPS = RING * RING
WIDE_PIECES = 4
BLOCKS = 2 * CHIPS
NEAR = tuple((axis, step) for axis in ("kv_0", "kv_1") for step in (2, 1, 3)) + (("tp", 1),)
HALF_AXES = (("kv_1", "kv_0"), ("kv_0", "kv_1"))
FAR_FIRST = (2, 1, 3, 0)
NEAR_FIRST = (1, 3, 2)
STEPS = (2, 1, 3)
IN_LINE = ((0, 0),) + tuple((0, a) for a in NEAR_FIRST) + tuple((a, 0) for a in NEAR_FIRST)
EARLY = tuple((a, b) for a in (1, 3) for b in (1, 3))
LATE = tuple((a, 2) for a in (1, 3)) + tuple((2, a) for a in NEAR_FIRST)
GROUPS = (
    tuple((*chip, core) for core in (0, 1) for chip in IN_LINE),
    *(tuple((*chip, core) for chip in chips) for chips in (EARLY, LATE) for core in (0, 1)),
)
ORDER = sum(GROUPS, ())
KEPT_AT = {block: at for at, block in enumerate(ORDER)}
FIRST_CHIPS = tuple(
    chip
    for turn in FAR_FIRST
    for step in STEPS
    for chip in ((step, turn), (turn, step))
)
CHIP_ORDER = tuple(dict.fromkeys(FIRST_CHIPS)) + ((0, 0),)
POSITION = {chip: place for place, chip in enumerate(CHIP_ORDER)}


def own_place():
    return (lax.axis_index("kv_0"), lax.axis_index("kv_1"), lax.axis_index("tp"))


def block_of(place, along_0, along_1, other_core):
    at_0, at_1, core = place
    return (
        lax.rem(at_0 + along_0, RING) * (2 * RING)
        + lax.rem(at_1 + along_1, RING) * 2
        + lax.rem(core + other_core, 2)
    )


class Wire:
    def __init__(self, place, send_sems, recv_sems):
        at_0, at_1, core = place
        self.core = core
        self.place = {"kv_0": (at_0, RING), "kv_1": (at_1, RING), "tp": (core, 2)}
        self.send_sems, self.recv_sems = send_sems, recv_sems
        self.sends = self.receives = 0
        self.owed = []

    def near(self, axis, step):
        at, size = self.place[axis]
        return {axis: lax.rem(at + step, size)}

    def greet(self, meanwhile):
        barrier = pltpu.get_barrier_semaphore()
        for axis, step in NEAR:
            pl.semaphore_signal(
                barrier, inc=1, device_id=self.near(axis, step), device_id_type=MESH
            )
        meanwhile()
        pl.semaphore_wait(barrier, len(NEAR))

    def sender(self, ref):
        self.sends += 1
        self.owed.append((self.sends - 1, ref))
        return self.sends - 1

    def receiver(self):
        self.receives += 1
        return self.receives - 1

    def prepare(self, source, target, axis, step, send, receive):
        return pltpu.make_async_remote_copy(
            src_ref=source,
            dst_ref=target,
            send_sem=self.send_sems.at[send],
            recv_sem=self.recv_sems.at[receive],
            device_id=self.near(axis, step),
            device_id_type=MESH,
        )

    def send(self, source, target, axis, step, send=None, receive=None):
        send = self.sender(source) if send is None else send
        receive = self.receiver() if receive is None else receive
        copy = self.prepare(source, target, axis, step, send, receive)
        copy.start()
        return copy

    def receive(self, receive, ref):
        pltpu.make_async_copy(ref, ref, self.recv_sems.at[receive]).wait()

    def finish(self, count=None):
        for send, ref in self.owed[:count]:
            pltpu.make_async_copy(ref, ref, self.send_sems.at[send]).wait()
        self.owed = self.owed[count:] if count is not None else []


def pieces_of(rows, number=2):
    tiles = rows // 16
    ends = [-(-tiles * piece // number) * 16 for piece in range(number + 1)]
    return tuple((a, b - a, (b - a) // 32 * 16) for a, b in zip(ends, ends[1:]))


def axes_of(piece):
    return HALF_AXES[piece % 2]


def axes_chip(half, first, second):
    return (second, first) if axes_of(half)[0] == "kv_1" else (first, second)


def gather(wire, held, ready, eager, started=lambda: None):
    halves = pieces_of(held.shape[1])
    copies = {}
    send = wire.sender(held.at[pl.ds(0, BLOCKS - 1)])
    crossing = {chips: wire.receiver() for chips in (IN_LINE, EARLY, LATE)}
    aside = {chip: wire.receiver() for chip in EARLY + LATE}

    def view(half, first, second, core):
        start, rows, _ = halves[half]
        chip = axes_chip(half, first, second)
        return held.at[KEPT_AT[(*chip, core)], pl.ds(start, rows), :]

    def spread(half, stage, first, steps=STEPS):
        for step in steps:
            there = RING - step
            chip = (there, 0) if stage == 0 else (first, there)
            source = (0, 0) if stage == 0 else (first, 0)
            copies[half, stage, first, there] = wire.send(
                view(half, *source, 0),
                view(half, *chip, 0),
                axes_of(half)[stage],
                step,
                send,
                aside.get(axes_chip(half, *chip)),
            )

    def crossed(half, first, second):
        chip = axes_chip(half, first, second)
        group = next(chips for chips in crossing if chip in chips)
        source, target = (view(half, first, second, core) for core in (0, 1))
        return wire.prepare(source, target, "tp", 1, send, crossing[group])

    def across(half, first, second):
        crossed(half, first, second).start()

    def arrive(half, stage, first, there):
        copies[half, stage, first, there].wait_recv()

    both = (0, 1)
    for half in both:
        spread(half, 0, 0, NEAR_FIRST)
    for half in both:
        spread(half, 1, 0)
    for half in both:
        across(half, 0, 0)
    started()
    for there in NEAR_FIRST:
        for half in both:
            arrive(half, 0, 0, there)
            spread(half, 1, there)
            across(half, there, 0)
    for there in NEAR_FIRST:
        for half in both:
            arrive(half, 1, 0, there)
            across(half, 0, there)

    def settle(chips):
        blocks = held.at[pl.ds(KEPT_AT[(*chips[0], 1)], len(chips))]
        wire.receive(crossing[chips], blocks)

    onward = {
        chip: wire.prepare(
            held.at[KEPT_AT[(*chip, 0)]],
            held.at[KEPT_AT[(*chip, 1)]],
            "tp",
            1,
            send,
            crossing[EARLY if chip in EARLY else LATE],
        )
        for chip in aside
    }

    def pass_on(chips):
        for chip in chips:
            wire.receive(aside[chip], held.at[KEPT_AT[(*chip, 0)]])
            onward[chip].start()

    if eager:
        @pl.when(wire.core == 1)
        def _():
            pass_on(EARLY)

        settle(IN_LINE)
        ready(0)

        @pl.when(wire.core == 1)
        def _():
            pass_on(LATE)

        @pl.when(wire.core == 0)
        def _():
            pass_on(EARLY)

        ready(1)
        settle(EARLY)
        ready(2)

        @pl.when(wire.core == 0)
        def _():
            pass_on(LATE)

    else:
        pass_on(EARLY + LATE)
        settle(IN_LINE)
        ready(0)
        ready(1)
        settle(EARLY)
        ready(2)
    ready(3)
    settle(LATE)
    ready(4)


def add_up(wire, halves, value, last_out, last_in):
    sums = [None] * len(halves)
    rows = [pl.ds(0, count) for _, count, _ in halves]
    sends = [wire.sender(last_out.at[half, pl.ds(0, 3), part]) for half, part in enumerate(rows)]
    receives = [wire.receiver() for _ in halves]
    for turn, second in enumerate(FAR_FIRST):
        for half in range(len(halves)):
            count = halves[half][1]
            result = value(turn, half)
            if second == 0:
                sums[half] = result
                continue
            last_out[half, turn, pl.ds(0, count), :] = result.astype(BF16)
            wire.send(
                last_out.at[half, turn, pl.ds(0, count), :],
                last_in.at[half, turn, pl.ds(0, count), :],
                axes_of(half)[1],
                second,
                sends[half],
                receives[half],
            )
    for half, part in enumerate(rows):
        wire.receive(receives[half], last_in.at[half, pl.ds(0, 3), part])
        for turn in (1, 2, 0):
            sums[half] += last_in[half, turn, pl.ds(0, halves[half][1]), :].astype(F32)
    return sums


def scatter_direct(wire, rows, term, between, buffers):
    halves = pieces_of(rows)
    early_out, early_in, last_out, last_in = buffers
    keep = len(wire.owed)
    rows = [pl.ds(0, count) for _, count, _ in halves]
    sends = [wire.sender(early_out.at[half, :, :, part]) for half, part in enumerate(rows)]
    receives = [[wire.receiver() for _ in FAR_FIRST] for _ in halves]
    for turn, second in enumerate(FAR_FIRST):
        for way, step in enumerate(STEPS):
            for half in (0, 1):
                start, count, _ = halves[half]
                early_out[half, turn, way, pl.ds(0, count), :] = term(
                    axes_chip(half, step, second), start, count
                ).astype(BF16)
                wire.send(
                    early_out.at[half, turn, way, pl.ds(0, count), :],
                    early_in.at[half, turn, way, pl.ds(0, count), :],
                    axes_of(half)[0],
                    step,
                    sends[half],
                    receives[half][turn],
                )
        between(turn)

    wire.finish(keep)

    def value(turn, half):
        start, count, _ = halves[half]
        result = term(axes_chip(half, 0, FAR_FIRST[turn]), start, count)
        wire.receive(receives[half][turn], early_in.at[half, turn, :, rows[half]])
        for way in range(len(STEPS)):
            result += early_in[half, turn, way, pl.ds(0, count), :].astype(F32)
        return result

    return add_up(wire, halves, value, last_out, last_in)


def scatter_relayed(wire, halves, term, before, buffers):
    early_out, early_in, late_out, late_in, last_out, last_in = buffers
    keep = len(wire.owed)
    rows = [pl.ds(0, count) for _, count, _ in halves]
    early_sends = [wire.sender(early_out.at[half, :, part]) for half, part in enumerate(rows)]
    late_sends = [wire.sender(late_out.at[half, :, :, part]) for half, part in enumerate(rows)]
    early_receives, late_receives = (
        [[wire.receiver() for _ in FAR_FIRST] for _ in halves] for _ in (0, 1)
    )

    def parts(half):
        _, count, cut = halves[half]
        return ((0, cut, 1), (cut, count - cut, 3))

    for half in range(len(halves)):
        before(half)
        for turn, second in enumerate(FAR_FIRST):
            start, count, _ = halves[half]
            early_out[half, turn, pl.ds(0, count), :] = term(
                axes_chip(half, 2, second), start, count
            ).astype(BF16)
            for at, length, step in parts(half):
                wire.send(
                    early_out.at[half, turn, pl.ds(at, length), :],
                    early_in.at[half, turn, pl.ds(at, length), :],
                    axes_of(half)[0],
                    step,
                    early_sends[half],
                    early_receives[half][turn],
                )
    wire.finish(keep)
    for turn, second in enumerate(FAR_FIRST):
        for half in range(len(halves)):
            start, count, _ = halves[half]
            wire.receive(early_receives[half][turn], early_in.at[half, turn, rows[half]])
            for way, (at, length, step) in enumerate(parts(half)):
                near = axes_chip(half, step, second)
                rest_at, rest = (length, count - length) if at == 0 else (0, at)
                late_out[half, turn, way, pl.ds(rest_at, rest), :] = term(
                    near, start + rest_at, rest
                ).astype(BF16)
                late_out[half, turn, way, pl.ds(at, length), :] = (
                    term(near, start + at, length)
                    + early_in[half, turn, pl.ds(at, length), :].astype(F32)
                ).astype(BF16)
                wire.send(
                    late_out.at[half, turn, way, pl.ds(0, count), :],
                    late_in.at[half, turn, way, pl.ds(0, count), :],
                    axes_of(half)[0],
                    step,
                    late_sends[half],
                    late_receives[half][turn],
                )

    def value(turn, half):
        start, count, _ = halves[half]
        result = term(axes_chip(half, 0, FAR_FIRST[turn]), start, count)
        wire.receive(late_receives[half][turn], late_in.at[half, turn, :, rows[half]])
        for way in (0, 1):
            result += late_in[half, turn, way, pl.ds(0, count), :].astype(F32)
        return result

    return add_up(wire, halves, value, last_out, last_in)


def scatter_buffers(pieces, relayed):
    number, half = len(pieces), pieces[0][1]
    first = [(RING,), (RING, 2)] if relayed else [(RING, len(STEPS))]
    return [
        pltpu.VMEM((number, *lead, half, LANES), BF16)
        for lead in (*first, (RING,))
        for _ in (0, 1)
    ]


def load_feed_forward(place, gate_hbm, up_hbm, down_hbm, wide, down, sems):
    hidden = gate_hbm.shape[0]
    half = wide.shape[0] // 2
    for at, block in enumerate(ORDER):
        columns = pl.ds(pl.multiple_of(block_of(place, *block) * LANES, LANES), LANES)
        here = pl.ds(at * LANES, LANES)
        pltpu.make_async_copy(
            gate_hbm.at[:, columns], wide.at[pl.ds(0, hidden), here], sems.at[0]
        ).start()
        pltpu.make_async_copy(
            up_hbm.at[:, columns], wide.at[pl.ds(half, hidden), here], sems.at[1]
        ).start()
    for at, chip in enumerate(CHIP_ORDER):
        pltpu.make_async_copy(
            down_hbm.at[:, columns_of(place, chip, 0)],
            down.at[pl.ds(0, hidden), pl.ds(at * LANES, LANES)],
            sems.at[2],
        ).start()


def columns_of(place, chip, core):
    return pl.ds(pl.multiple_of(block_of(place, *chip, core) * LANES, LANES), LANES)


def feed_forward(
    place,
    wire,
    held,
    gain,
    gate_hbm,
    up_hbm,
    down_hbm,
    wide,
    down,
    sems,
    scratch,
    buffers,
    after_swap=lambda: None,
):
    scaled, squares, gains, acc, own, units = scratch
    hidden, half = (gate_hbm.shape[0], wide.shape[0] // 2)
    rows, width = scaled.shape
    squares[...] = jnp.zeros_like(squares)
    for at, block in enumerate(ORDER):
        gains[pl.ds(at, 1), :] = gain[pl.ds(block_of(place, *block), 1), :]

    def scale(block, carry):
        entry = held[block].astype(F32)
        scaled[:, pl.ds(pl.multiple_of(block * LANES, LANES), LANES)] = (
            entry * gains[pl.ds(block, 1), :]
        ).astype(BF16)
        return carry + entry * entry

    def ready(group):
        with jax.named_scope("scale_and_product"):
            first = sum(len(blocks) for blocks in GROUPS[:group])
            last = first + len(GROUPS[group])
            squares[...] = lax.fori_loop(first, last, scale, squares[...])
            if group == 0:
                pltpu.make_async_copy(gate_hbm, wide.at[pl.ds(0, hidden), :], sems.at[0]).wait()
                pltpu.make_async_copy(up_hbm, wide.at[pl.ds(half, hidden), :], sems.at[1]).wait()
            chunk = pl.ds(first * LANES, (last - first) * LANES)
            part = lax.dot_general(
                scaled[:, chunk],
                wide[:, chunk],
                (((1,), (1,)), ((), ())),
                preferred_element_type=F32,
            )
            acc[...] = part if group == 0 else acc[...] + part

    def started():
        send = wire.sender(others)
        for at, chip in enumerate(CHIP_ORDER):
            wire.send(
                down_hbm.at[:, columns_of(place, chip, 1)],
                down.at[pl.ds(half, hidden), pl.ds(at * LANES, LANES)],
                "tp",
                1,
                send,
                others_receive,
            )

    others, others_receive = down.at[pl.ds(half, hidden), :], wire.receiver()
    with jax.named_scope("gather_features"):
        gather(wire, held, ready, True, started)
    with jax.named_scope("hidden"):
        row_scale = lax.rsqrt(jnp.sum(squares[...], axis=1, keepdims=True) / width + epsilon)
        gate = row_scale * acc[:, :half]
        up = row_scale * acc[:, half:]
        units[:, pl.ds(0, half)] = (gate / (1.0 + jnp.exp(-gate)) * up).astype(BF16)
        swap = wire.send(
            units.at[:, pl.ds(0, half)], units.at[:, pl.ds(half, half)], "tp", 1
        )
        after_swap()
        arrived = down.at[pl.ds(0, hidden), :]
        pltpu.make_async_copy(arrived, arrived, sems.at[2]).wait()

    def product(first, last, begin, count):
        chips = pl.ds(first * LANES, (last - first) * LANES)
        return jnp.dot(
            units[:, pl.ds(begin, count)],
            down[pl.ds(begin, count), chips],
            preferred_element_type=F32,
        )

    def project(first, last):
        with jax.named_scope("down"):
            result = product(first, last, 0, 2 * half)
            for at in range(first, last):
                own[at] = result[:, (at - first) * LANES : (at - first + 1) * LANES]

    ends = (5, 9, 13, CHIPS)
    with jax.named_scope("down_first"):
        kept = product(0, ends[0], 0, half)
        for at in range(ends[0]):
            own[at] = kept[:, at * LANES : (at + 1) * LANES]
        wire.receive(others_receive, others)
        swap.wait_recv()
        kept = product(0, ends[0], half, half)
        for at in range(ends[0]):
            own[at] += kept[:, at * LANES : (at + 1) * LANES]

    def term(chip, start, count):
        return own[POSITION[chip], pl.ds(start, count), :]

    def between(turn):
        if turn == 0:
            project(ends[0], ends[1])
        elif turn == 1:
            project(ends[1], ends[2])
            project(ends[2], ends[3])

    with jax.named_scope("scatter_features"):
        sums = scatter_direct(wire, rows, term, between, buffers)
    return sums


def feed_forward_scratch(rows, width, hidden):
    half = -(-hidden // LANES) * LANES
    return [
        pltpu.VMEM((BLOCKS, rows, LANES), BF16),
        pltpu.VMEM((2 * half, width), BF16),
        pltpu.VMEM((2 * half, CHIPS * LANES), BF16),
        pltpu.SemaphoreType.DMA((10,)),
        pltpu.VMEM((rows, width), BF16),
        pltpu.VMEM((rows, LANES), F32),
        pltpu.VMEM((BLOCKS, LANES), F32),
        pltpu.VMEM((rows, 2 * half), F32),
        pltpu.VMEM((CHIPS, rows, LANES), F32),
        pltpu.VMEM((rows, 2 * half), BF16),
        *scatter_buffers(pieces_of(rows), False),
    ]


def clear_padding(wide, down, hidden):
    half = wide.shape[0] // 2
    for array in (wide, down):
        for start in (hidden, half + hidden):
            rest = pl.ds(start, half - hidden)
            array[rest, :] = jnp.zeros((half - hidden, array.shape[1]), BF16)


def first_kernel(
    tokens,
    gate_hbm,
    up_hbm,
    down_hbm,
    first_gain_hbm,
    mix_gain_hbm,
    query_hbm,
    forget_hbm,
    input_hbm,
    outgate_hbm,
    projected,
    mixer_share,
    send_sems,
    recv_sems,
    held,
    wide,
    down,
    sems,
    scaled,
    squares,
    gains,
    acc,
    own,
    units,
    *rest,
):
    buffers, own_refs, wide_buffers = (rest[:4], rest[4:13], rest[13:])
    low, high, share, ordered, rows_out, rows_in, wide_own, first_gain, mix_gain = own_refs
    place = own_place()
    wire = Wire(place, send_sems, recv_sems)
    own_tokens = pltpu.make_async_copy(tokens, held.at[0], sems.at[3])
    own_tokens.start()
    gain_loads = [
        pltpu.make_async_copy(first_gain_hbm, first_gain, sems.at[8]),
        pltpu.make_async_copy(mix_gain_hbm, mix_gain, sems.at[9]),
    ]
    for load in gain_loads:
        load.start()
    with jax.named_scope("greet"):
        wire.greet(
            lambda: load_feed_forward(place, gate_hbm, up_hbm, down_hbm, wide, down, sems)
        )
    own_tokens.wait()
    share_width, width = query_hbm.shape
    weights = (
        (query_hbm, low, 0),
        (forget_hbm, low, width),
        (input_hbm, high, 0),
        (outgate_hbm, high, width),
    )
    loads = [
        pltpu.make_async_copy(
            source, target.at[pl.ds(0, share_width), pl.ds(at, width)], sems.at[4 + index]
        )
        for index, (source, target, at) in enumerate(weights)
    ]
    weight_copies = []

    def share_weights():
        send = wire.sender(low)
        for source, target, at in weights:
            there = target.at[pl.ds(share_width, share_width), pl.ds(at, width)]
            weight_copies.append(wire.send(source, there, "tp", 1, send))

    for load in loads:
        load.start()
    clear_padding(wide, down, gate_hbm.shape[0])
    for load in gain_loads:
        load.wait()
    sums = feed_forward(
        place,
        wire,
        held,
        first_gain,
        gate_hbm,
        up_hbm,
        down_hbm,
        wide,
        down,
        sems,
        (scaled, squares, gains, acc, own, units),
        buffers,
        share_weights,
    )
    rows = share.shape[0]
    for (start, count, _), value in zip(pieces_of(rows), sums):
        part = pl.ds(start, count)
        mixed = (held[0, part, :].astype(F32) + 0.5 * value).astype(BF16)
        mixer_share[part, :] = mixed
        share[part, :] = mixed.astype(F32)
    seqs = rows // BLOCKS
    for block in range(BLOCKS):
        chip = (block // RING % RING, block % RING)
        index = block_of(place, *chip, block // CHIPS)
        ordered[pl.ds(block * seqs, seqs), :] = share[
            pl.ds(pl.multiple_of(index * seqs, seqs), seqs), :
        ]
    side = rows // 2
    rows_out[...] = ordered[pl.ds(side, side), :].astype(BF16)
    swap = wire.send(rows_out, rows_in, "tp", 1)
    for load in loads:
        load.wait()
    for copy in weight_copies:
        copy.wait_recv()
    swap.wait_recv()
    entries = (ordered[pl.ds(0, side), :], rows_in[...].astype(F32))
    mix_scaled = jnp.concatenate(
        [
            entry * mix_gain[pl.ds(block_of(place, 0, 0, core), 1), :]
            for core, entry in enumerate(entries)
        ],
        axis=1,
    ).astype(BF16)
    square_sum = sum(jnp.sum(entry * entry, axis=1, keepdims=True) for entry in entries)
    square_sum = jnp.broadcast_to(square_sum, entries[0].shape)

    def keep(at, lower, upper):
        both = [part.reshape(RING, RING, seqs, LANES) for part in (lower, upper)]
        wide_own[:, :, pl.ds(at, 2 * seqs), :] = jnp.concatenate(both, axis=2)

    tile = 2 * seqs
    wide_rows = wide_own.shape[2]
    wide_halves = pieces_of(wide_rows, WIDE_PIECES)
    columns = low.shape[1] // LANES

    def project(steps):
        with jax.named_scope("project"):
            for step in steps:
                chunk = slice(2 * step * LANES, 2 * (step + 1) * LANES)
                lower = jnp.dot(mix_scaled, low[:, chunk], preferred_element_type=F32)
                upper = jnp.dot(mix_scaled, high[:, chunk], preferred_element_type=F32)
                for which in (0, 1):
                    lanes = slice(which * LANES, (which + 1) * LANES)
                    keep((2 * step + which) * tile, lower[:, lanes], upper[:, lanes])

    ends = [
        min(-(-(start + count) // (2 * tile)), columns // 2) for start, count, _ in wide_halves
    ]

    def before(piece):
        project(range(ends[piece - 1] if piece else 0, ends[piece]))
        if piece + 1 == len(wide_halves):
            keep(columns * tile, square_sum, jnp.zeros_like(square_sum))

    def term(chip, start, count):
        return wide_own[(*chip, pl.ds(start, count))]

    with jax.named_scope("scatter_wide"):
        sums = scatter_relayed(wire, wide_halves, term, before, wide_buffers)
    for (start, count, _), value in zip(wide_halves, sums):
        projected[pl.ds(start, count), :] = value
    with jax.named_scope("finish"):
        wire.finish()
    assert (wire.sends, wire.receives) == (send_sems.shape[0], recv_sems.shape[0]), (wire.sends, wire.receives)


def state_kernel(
    full_width, projected, floor_grid, head_gain, state, next_state, mixer_out, held, sems
):
    seqs, heads, keys, values = state.shape
    tile = 2 * seqs
    writes = [
        pltpu.make_async_copy(held.at[head], next_state.at[:, head], sems.at[head])
        for head in range(heads)
    ]
    squares = projected[pl.ds(2 * heads * tile, seqs), :]
    scale = lax.rsqrt(squares / full_width + epsilon)

    def channels(block, second):
        return scale * projected[pl.ds(block * tile + second * seqs, seqs), :]

    row_seq = lax.broadcasted_iota(jnp.int32, (4 * seqs, seqs * values), 0) % seqs
    lane_seq = lax.broadcasted_iota(jnp.int32, (4 * seqs, seqs * values), 1) // values
    spreader = (row_seq == lane_seq).astype(F32).astype(BF16)

    def pieces(entry):
        first = entry.astype(BF16).astype(F32)
        second = (entry - first).astype(BF16).astype(F32)
        third = entry - first - second
        return jnp.concatenate([first, second, third, jnp.zeros_like(entry)], axis=0)

    for head in range(heads):
        query = channels(head, 0)
        entering = channels(head, 1)
        forget_pre = channels(heads + head, 0)
        gate = channels(heads + head, 1)
        floor = floor_grid[pl.ds(head, 1), :]
        forget = floor + (1.0 - floor) / (1.0 + jnp.exp(-forget_pre))
        query = query / (1.0 + jnp.exp(-query))
        both = jnp.concatenate([pieces(forget), pieces(query)], axis=1).T.astype(BF16)
        spread = jnp.dot(both, spreader, preferred_element_type=F32)
        readouts = []
        for seq in range(seqs):
            kept = spread[:keys, seq * values : (seq + 1) * values]
            asked = spread[keys:, seq * values : (seq + 1) * values]
            fresh = entering[seq : seq + 1, :]
            after = fresh + kept * (state[seq, head] - fresh)
            held[head, seq] = after
            readouts.append(jnp.sum(after * asked, axis=0, keepdims=True))
        writes[head].start()
        readout = jnp.concatenate(readouts, axis=0)
        normed = (
            readout
            * lax.rsqrt(jnp.mean(readout * readout, axis=-1, keepdims=True) + epsilon)
            * head_gain[...]
        )
        half = heads // 2
        row = head % half * tile + head // half * seqs
        mixer_out[pl.ds(row, seqs), :] = normed * (gate / (1.0 + jnp.exp(-gate)))
    for write in writes:
        write.wait()


def second_kernel(
    mixer_out,
    share_hbm,
    output_hbm,
    gate_hbm,
    up_hbm,
    down_hbm,
    gain_hbm,
    layer_out,
    send_sems,
    recv_sems,
    held,
    wide,
    down,
    sems,
    scaled,
    squares,
    gains,
    acc,
    own,
    units,
    *rest,
):
    buffers, (mixed, output, update, mixer_share, second_gain) = rest[:4], rest[4:]
    place = own_place()
    wire = Wire(place, send_sems, recv_sems)
    depth = output.shape[0]
    loads = [
        pltpu.make_async_copy(
            output_hbm.at[pl.ds(which * depth, depth), :],
            output.at[:, pl.ds(which * LANES, LANES)],
            sems.at[3 + which],
        )
        for which in (0, 1)
    ] + [
        pltpu.make_async_copy(share_hbm, mixer_share, sems.at[5]),
        pltpu.make_async_copy(gain_hbm, second_gain, sems.at[6]),
    ]
    for load in loads:
        load.start()
    mixed[0] = mixer_out[...].astype(BF16)
    with jax.named_scope("greet"):
        wire.greet(
            lambda: load_feed_forward(place, gate_hbm, up_hbm, down_hbm, wide, down, sems)
        )
    clear_padding(wide, down, gate_hbm.shape[0])
    rows = update.shape[0]
    seqs = rows // BLOCKS
    tile = 2 * seqs

    def project(group):
        with jax.named_scope("output"):
            if group == 0:
                for load in loads:
                    load.wait()
            first = sum(len(blocks) for blocks in GROUPS[:group])
            number = len(GROUPS[group])
            total = None
            for step in range(depth // (2 * LANES)):
                pieces = [
                    mixed[
                        pl.ds(first, number), pl.ds((2 * step + which) * tile, tile), :
                    ].reshape(number * tile, LANES)
                    for which in (0, 1)
                ]
                product = jnp.dot(
                    jnp.concatenate(pieces, axis=1),
                    output[pl.ds(step * 2 * LANES, 2 * LANES), :],
                    preferred_element_type=F32,
                )
                total = product if total is None else total + product
            total = total.reshape(number, tile, 2 * LANES)
            total = total[:, :seqs, :LANES] + total[:, seqs:, LANES:]
            for at, block in enumerate(GROUPS[group]):
                index = block_of(place, *block)
                update[pl.ds(pl.multiple_of(index * seqs, seqs), seqs), :] = total[at]

    with jax.named_scope("gather_mixed"):
        gather(wire, mixed, project, False)
    held[0] = (mixer_share[...].astype(F32) + update[...]).astype(BF16)
    sums = feed_forward(
        place,
        wire,
        held,
        second_gain,
        gate_hbm,
        up_hbm,
        down_hbm,
        wide,
        down,
        sems,
        (scaled, squares, gains, acc, own, units),
        buffers,
    )
    for (start, count, _), value in zip(pieces_of(rows), sums):
        part = pl.ds(start, count)
        layer_out[part, :] = (held[0, part, :].astype(F32) + 0.5 * value).astype(BF16)
    with jax.named_scope("finish"):
        wire.finish()
    assert (wire.sends, wire.receives) == (send_sems.shape[0], recv_sems.shape[0]), (wire.sends, wire.receives)


def in_space(*spaces):
    return [pl.BlockSpec(memory_space=space) for space in spaces]


def kernel_params(identity, mebibytes):
    return pltpu.CompilerParams(
        collective_id=identity, has_side_effects=True, vmem_limit_bytes=mebibytes << 20
    )


def per_device(
    tokens,
    carried_state,
    first_gain,
    first_gate,
    first_up,
    first_down,
    mix_gain,
    query_weight,
    forget_weight,
    input_weight,
    outgate_weight,
    forget_floor,
    head_gain,
    output_weight,
    second_gain,
    second_gate,
    second_up,
    second_down,
):
    rows, share = tokens.shape
    full_width, hidden = first_gate.shape
    in_hbm = lambda array: pltpu.with_memory_space_constraint(array, HBM)
    seqs, heads, keys, values = carried_state.shape
    tile = 2 * seqs
    wide_rows = (2 * heads + 1) * tile
    by_block = (full_width // LANES, LANES)
    projected, mixer_share = pl.pallas_call(
        first_kernel,
        name="first_block",
        out_shape=(
            jax.ShapeDtypeStruct((wide_rows, LANES), F32),
            jax.ShapeDtypeStruct((rows, share), BF16),
        ),
        in_specs=in_space(*(HBM,) * 10),
        out_specs=in_space(VMEM, VMEM),
        scratch_shapes=[
            pltpu.SemaphoreType.DMA((21,)),
            pltpu.SemaphoreType.DMA((77,)),
            *feed_forward_scratch(rows, full_width, hidden),
            pltpu.VMEM((2 * share, 2 * heads * keys), BF16),
            pltpu.VMEM((2 * share, 2 * heads * values), BF16),
            pltpu.VMEM((rows, LANES), F32),
            pltpu.VMEM((rows, LANES), F32),
            pltpu.VMEM((rows // 2, LANES), BF16),
            pltpu.VMEM((rows // 2, LANES), BF16),
            pltpu.VMEM((RING, RING, wide_rows, LANES), F32),
            pltpu.VMEM(by_block, F32),
            pltpu.VMEM(by_block, F32),
            *scatter_buffers(pieces_of(wide_rows, WIDE_PIECES), True),
        ],
        compiler_params=kernel_params(0, 44),
    )(
        in_hbm(tokens),
        in_hbm(first_gate.T),
        in_hbm(first_up.T),
        in_hbm(first_down),
        in_hbm(first_gain.reshape(by_block)),
        in_hbm(mix_gain.reshape(by_block)),
        in_hbm(query_weight),
        in_hbm(forget_weight),
        in_hbm(input_weight),
        in_hbm(outgate_weight),
    )
    next_state, mixer_out = pl.pallas_call(
        lambda *refs: state_kernel(full_width, *refs),
        name="state_update",
        out_shape=(
            jax.ShapeDtypeStruct(carried_state.shape, F32),
            jax.ShapeDtypeStruct((heads * seqs, values), F32),
        ),
        in_specs=in_space(VMEM, VMEM, VMEM, VMEM),
        out_specs=in_space(HBM, VMEM),
        scratch_shapes=[
            pltpu.VMEM((heads, seqs, keys, values), F32),
            pltpu.SemaphoreType.DMA((heads,)),
        ],
        compiler_params=pltpu.CompilerParams(vmem_limit_bytes=12 << 20),
    )(
        projected,
        forget_floor.reshape(heads, keys),
        head_gain.reshape(1, values),
        carried_state,
    )
    layer_out = pl.pallas_call(
        second_kernel,
        name="second_block",
        out_shape=jax.ShapeDtypeStruct((rows, share), BF16),
        in_specs=in_space(VMEM, *(HBM,) * 6),
        out_specs=pl.BlockSpec(memory_space=VMEM),
        scratch_shapes=[
            pltpu.SemaphoreType.DMA((8,)),
            pltpu.SemaphoreType.DMA((60,)),
            *feed_forward_scratch(rows, full_width, hidden),
            pltpu.VMEM((BLOCKS, heads * seqs, LANES), BF16),
            pltpu.VMEM((heads * values // 2, 2 * LANES), BF16),
            pltpu.VMEM((rows, LANES), F32),
            pltpu.VMEM((rows, LANES), BF16),
            pltpu.VMEM(by_block, F32),
        ],
        compiler_params=kernel_params(1, 32),
    )(
        mixer_out,
        mixer_share,
        in_hbm(output_weight),
        in_hbm(second_gate.T),
        in_hbm(second_up.T),
        in_hbm(second_down),
        in_hbm(second_gain.reshape(by_block)),
    )
    return (layer_out, next_state)


def solution(mesh):
    split = Mesh(
        mesh.devices.reshape(mesh.shape["dp"], RING, RING, mesh.shape["tp"]), DP_KV_TP
    )
    return jax.shard_map(
        per_device,
        mesh=split,
        in_specs=(
            P("dp", KV_TP),
            P(DP_KV_TP, None, None, None),
            P(),
            P(None, KV_TP),
            P(None, KV_TP),
            P(KV_TP, None),
            P(),
            P(KV_TP, None),
            P(KV_TP, None),
            P(KV_TP, None),
            P(KV_TP, None),
            P(),
            P(),
            P(None, KV_TP),
            P(),
            P(None, KV_TP),
            P(None, KV_TP),
            P(KV_TP, None),
        ),
        out_specs=(P("dp", KV_TP), P(DP_KV_TP, None, None, None)),
        check_vma=False,
    )
```
